256 devices in a mesh: sp: 64 (over z, x, core), tp: 4 (over y).
Axes of the slice: x: 4, y: 4, z: 8, core: 2. Of those that a mesh axis runs over, the one named last changes fastest.
Arguments:
- wide_query: bfloat16 [32768, 1536], P('sp', 'tp'), may hold values from -6 to 6
- wide_key: bfloat16 [32768, 1536], P('sp', 'tp'), may hold values from -6 to 6
- wide_value: bfloat16 [32768, 1536], P('sp', 'tp'), may hold values from -6 to 6
- wide_gate: bfloat16 [32768, 1536], P('sp', 'tp'), may hold values from -6 to 6
- narrow_query: bfloat16 [32768, 512], P('sp', 'tp'), may hold values from -6 to 6
- narrow_key: bfloat16 [32768, 512], P('sp', 'tp'), may hold values from -6 to 6
- narrow_value: bfloat16 [32768, 512], P('sp', 'tp'), may hold values from -6 to 6
- narrow_gate: bfloat16 [32768, 512], P('sp', 'tp'), may hold values from -6 to 6
- wide_decay: float32 [12, 32768], P('tp', 'sp'), may hold values from -1 to 0
- narrow_decay: float32 [8, 32768], P('tp', 'sp'), may hold values from -1 to 0
- residual: bfloat16 [32768, 2048], P(('sp', 'tp')), may hold values from -6 to 6
- wide_out: bfloat16 [1536, 2048], P('tp'), may hold values from -0.125 to 0.125
- narrow_out: bfloat16 [512, 2048], P('tp'), may hold values from -0.125 to 0.125
- up_weight: bfloat16 [2048, 8192], P('sp', 'tp'), may hold values from -0.125 to 0.125
- down_weight: bfloat16 [8192, 2048], P('tp', 'sp'), may hold values from -0.0625 to 0.0625
- gain_mix: float32 [2048], replicated, may hold values from 0.1 to 1.9
- gain_pre: float32 [2048], replicated, may hold values from 0.1 to 1.9
- gain_mlp: float32 [2048], replicated, may hold values from 0.1 to 1.9
Outputs:
- result: bfloat16 [32768, 2048], P(('sp', 'tp'))
The draws below stay inside these ranges and needn't reach their ends.
All inputs are finite; a program needn't handle non-finite values.
Results may differ from the reference program's by a relative error of at most 0.02.
Values may be sent and summed in bfloat16 or wider, within the bound.
No kernel may reach another device: no remote copies, remote signals or barrier semaphores. Data moves between devices by JAX's collectives and lax.ppermute only.
A program may use at most 128 MiB of HBM per device.

```python
import math
import jax
import jax.numpy as jnp
from jax import lax

D = 2048
FF = 8192
WIDE_HEADS = 12
WIDE_DIM = 128
NARROW_HEADS = 8
NARROW_DIM = 64
SPAN = 128
TOK_DEV = 512
TOKEN_POSITIONS = 32768


def decay_law(source, count_of_heads):
    key_sequences = jax.random.split(source, 7)
    order = jax.random.permutation(key_sequences[0], count_of_heads)
    quick = order < count_of_heads // 2
    quick_rate = jnp.exp(jax.random.uniform(key_sequences[1], (count_of_heads,), jnp.float32, math.log(1.0 / 50.0), math.log(1.0 / 30.0)))
    slow_rate = jnp.exp(jax.random.uniform(key_sequences[2], (count_of_heads,), jnp.float32, math.log(0.12), math.log(0.35))) / TOKEN_POSITIONS
    base_rate = jnp.where(quick, quick_rate, slow_rate)
    block_count = TOKEN_POSITIONS // TOK_DEV
    factor = jnp.exp(jax.random.uniform(key_sequences[3], (count_of_heads, block_count), jnp.float32, math.log(0.5), math.log(2.0)))
    factor = jnp.repeat(factor, TOK_DEV, axis=1)
    jitter = jnp.exp(jax.random.uniform(key_sequences[4], (count_of_heads, TOKEN_POSITIONS), jnp.float32, math.log(0.6), math.log(1.4)))
    decay_rates = base_rate[:, None] * factor * jitter
    group_start_index = jax.random.randint(key_sequences[5], (count_of_heads, 2), 0, TOKEN_POSITIONS)
    group_length = jax.random.uniform(key_sequences[6], (count_of_heads, 2), jnp.float32, math.log(0.6), math.log(0.8))
    token_positions = jnp.arange(TOKEN_POSITIONS, dtype=jnp.int32)
    token_groups = jnp.sum(jnp.where(token_positions[None, None, :] == group_start_index[:, :, None], group_length[:, :, None], 0.0), axis=1)
    return (token_groups - decay_rates).astype(jnp.float32)


def draw_wide_decay(key, part):
    return decay_law(jax.random.fold_in(key, 11), WIDE_HEADS)


def draw_narrow_decay(key, part):
    return decay_law(jax.random.fold_in(key, 12), NARROW_HEADS)


def shard_levels(key, dims, shards, least, largest):
    def one(position, blocks):
        steps = jax.random.uniform(jax.random.fold_in(jax.random.fold_in(key, 6), position), (blocks,), jnp.float32, least / len(shards), largest / len(shards))
        return jnp.repeat(jnp.exp(steps), dims[position] // blocks).reshape((-1,) + (1,) * (len(dims) - position - 1))

    factor_of = one(*shards[0])
    for cut in shards[1:]:
        factor_of = factor_of * one(*cut)
    return factor_of


def gaussian(own_key, shape, deviation, reach, pieces=(), held_as=jnp.bfloat16):
    array = jax.random.normal(own_key, shape, jnp.float32) * deviation
    if len(pieces) > 0:
        array = shard_levels(own_key, shape, pieces, -0.22, 0.18) * array
    return jnp.clip(array, min=-reach, max=reach).astype(held_as)


def setup_inputs(seed: int = 0) -> dict:
    arg_keys = jax.random.split(jax.random.key(seed), 19)
    wide_query = gaussian(arg_keys[0], (TOKEN_POSITIONS, WIDE_HEADS * WIDE_DIM), 1.0, 6.0, ((0, 64), (1, 4)))
    wide_key = gaussian(arg_keys[1], (TOKEN_POSITIONS, WIDE_HEADS * WIDE_DIM), 1.0, 6.0, ((0, 64), (1, 4)))
    wide_value = gaussian(arg_keys[2], (TOKEN_POSITIONS, WIDE_HEADS * WIDE_DIM), 1.0, 6.0, ((0, 64), (1, 4)))
    wide_gate = gaussian(arg_keys[3], (TOKEN_POSITIONS, WIDE_HEADS * WIDE_DIM), 1.0, 6.0, ((0, 64), (1, 4)))
    narrow_query = gaussian(arg_keys[4], (TOKEN_POSITIONS, NARROW_HEADS * NARROW_DIM), 1.0, 6.0, ((0, 64), (1, 4)))
    narrow_key = gaussian(arg_keys[5], (TOKEN_POSITIONS, NARROW_HEADS * NARROW_DIM), 1.0, 6.0, ((0, 64), (1, 4)))
    narrow_value = gaussian(arg_keys[6], (TOKEN_POSITIONS, NARROW_HEADS * NARROW_DIM), 1.0, 6.0, ((0, 64), (1, 4)))
    narrow_gate = gaussian(arg_keys[7], (TOKEN_POSITIONS, NARROW_HEADS * NARROW_DIM), 1.0, 6.0, ((0, 64), (1, 4)))
    wide_decay = draw_wide_decay(jax.random.fold_in(arg_keys[18], 71), 0)
    narrow_decay = draw_narrow_decay(jax.random.fold_in(arg_keys[18], 71), 0)
    residual = gaussian(arg_keys[10], (TOKEN_POSITIONS, D), 1.0, 6.0, ((0, 256),))
    wide_out = gaussian(arg_keys[11], (WIDE_HEADS * WIDE_DIM, D), D ** -0.5, 0.125, ((0, 4),))
    narrow_out = gaussian(arg_keys[12], (NARROW_HEADS * NARROW_DIM, D), D ** -0.5, 0.125, ((0, 4),))
    up_weight = gaussian(arg_keys[13], (D, FF), D ** -0.5, 0.125, ((0, 64), (1, 4)))
    down_weight = gaussian(arg_keys[14], (FF, D), FF ** -0.5, 0.0625, ((0, 4), (1, 64)))
    gain_mix = jnp.clip(1.0 + 0.18 * jax.random.normal(arg_keys[15], (D,), jnp.float32), 0.1, 1.9)
    gain_pre = jnp.clip(1.0 + 0.18 * jax.random.normal(arg_keys[16], (D,), jnp.float32), 0.1, 1.9)
    gain_mlp = jnp.clip(1.0 + 0.18 * jax.random.normal(arg_keys[17], (D,), jnp.float32), 0.1, 1.9)
    return {"wide_query": wide_query, "wide_key": wide_key, "wide_value": wide_value, "wide_gate": wide_gate, "narrow_query": narrow_query, "narrow_key": narrow_key, "narrow_value": narrow_value, "narrow_gate": narrow_gate, "wide_decay": wide_decay, "narrow_decay": narrow_decay, "residual": residual, "wide_out": wide_out, "narrow_out": narrow_out, "up_weight": up_weight, "down_weight": down_weight, "gain_mix": gain_mix, "gain_pre": gain_pre, "gain_mlp": gain_mlp}


epsilon = 1e-06

def rotate(packed, head_dim, positions):
    length = packed.shape[0]
    grouped = packed.astype(jnp.float32).reshape(length, -1, head_dim)
    halfway = head_dim // 2
    inverse = 10000.0 ** (-jnp.arange(0, head_dim, 2, dtype=jnp.float32) / head_dim)
    angles = positions.astype(jnp.float32)[:, None] * inverse[None, :]
    cosine_table = jnp.cos(angles)[:, None, :]
    sine_table = jnp.sin(angles)[:, None, :]
    leading = grouped[..., :halfway]
    trailing = grouped[..., halfway:]
    return jnp.concatenate([leading * cosine_table - trailing * sine_table, leading * sine_table + trailing * cosine_table], axis=-1)

def rms_scale(values, gain_vector):
    return values * lax.rsqrt(lax.optimization_barrier(jnp.mean(values * values, axis=-1, keepdims=True)) + epsilon) * gain_vector.astype(jnp.float32)

def retention(query, key, value, gate, log_decay, head_dim):
    length = query.shape[0]
    count_of_heads = query.shape[1] // head_dim
    span_count = length // SPAN
    positions = jnp.arange(length, dtype=jnp.int32)
    queries = lax.optimization_barrier(rotate(query, head_dim, positions).astype(jnp.bfloat16))
    keys_full = rotate(key, head_dim, positions) * head_dim ** (-0.5)
    keys_half = lax.optimization_barrier(keys_full.astype(jnp.bfloat16))
    shaped = (span_count, SPAN, count_of_heads, head_dim)
    cumulative = jnp.cumsum(log_decay.T.reshape(span_count, SPAN, count_of_heads), axis=1)
    causal = jnp.arange(SPAN)[:, None] >= jnp.arange(SPAN)[None, :]

    def advance(carried, inputs):
        span_queries, span_keys, span_full, span_values, span_decay = inputs
        scores = jnp.einsum('ihd,jhd->hij', span_queries.astype(jnp.float32), span_keys.astype(jnp.float32), precision=lax.Precision.HIGHEST)
        decay_rows = span_decay.T
        log_gaps = jnp.where(causal[None], decay_rows[:, :, None] - decay_rows[:, None, :], -jnp.inf)
        weights = lax.optimization_barrier((scores * jnp.exp(log_gaps)).astype(jnp.bfloat16))
        within = jnp.einsum('hij,jhd->ihd', weights.astype(jnp.float32), span_values.astype(jnp.float32), precision=lax.Precision.HIGHEST)
        entering = lax.optimization_barrier(carried.astype(jnp.bfloat16)).astype(jnp.float32)
        across = jnp.einsum('ihd,hde->ihe', span_queries.astype(jnp.float32), entering, precision=lax.Precision.HIGHEST) * jnp.exp(span_decay)[:, :, None]
        span_total = span_decay[-1]
        scaled = lax.optimization_barrier((span_full * jnp.exp(span_total[None, :] - span_decay)[:, :, None]).astype(jnp.bfloat16))
        update = jnp.einsum('jhd,jhe->hde', scaled.astype(jnp.float32), span_values.astype(jnp.float32), precision=lax.Precision.HIGHEST)
        carried = carried * jnp.exp(span_total)[:, None, None] + update
        return (carried, within + across)
    initial = jnp.zeros((count_of_heads, head_dim, head_dim), jnp.float32)
    inputs = (queries.reshape(shaped), keys_half.reshape(shaped), keys_full.reshape(shaped), value.reshape(shaped), cumulative)
    closing, output = lax.scan(advance, initial, inputs)
    output = output.reshape(length, count_of_heads, head_dim)
    normed = output * lax.rsqrt(lax.optimization_barrier(jnp.mean(output * output, axis=-1, keepdims=True)) + epsilon)
    return (normed.reshape(length, -1) * jax.nn.silu(gate.astype(jnp.float32))).astype(jnp.bfloat16)

def reference(wide_query, wide_key, wide_value, wide_gate, narrow_query, narrow_key, narrow_value, narrow_gate, wide_decay, narrow_decay, residual, wide_out, narrow_out, up_weight, down_weight, gain_mix, gain_pre, gain_mlp):
    wide_mixed = retention(wide_query, wide_key, wide_value, wide_gate, wide_decay, WIDE_DIM)
    narrow_mixed = retention(narrow_query, narrow_key, narrow_value, narrow_gate, narrow_decay, NARROW_DIM)
    projected = jnp.dot(wide_mixed, wide_out, preferred_element_type=jnp.float32) + jnp.dot(narrow_mixed, narrow_out, preferred_element_type=jnp.float32)
    updated = (residual.astype(jnp.float32) + rms_scale(projected, gain_mix)).astype(jnp.bfloat16)
    normed = rms_scale(updated.astype(jnp.float32), gain_pre).astype(jnp.bfloat16)
    rectified = jax.nn.relu(jnp.dot(normed, up_weight, preferred_element_type=jnp.float32))
    hidden = (rectified * rectified).astype(jnp.bfloat16)
    lowered = jnp.dot(hidden, down_weight, preferred_element_type=jnp.float32)
    return (updated.astype(jnp.float32) + rms_scale(lowered, gain_mlp)).astype(jnp.bfloat16)
```

```python
import functools

import jax
import jax.numpy as jnp
import numpy as np
from jax import lax
from jax.experimental import pallas as pl
from jax.experimental.pallas import tpu as pltpu
from jax.sharding import Mesh
from jax.sharding import PartitionSpec as P

SPAN = 128
LANES = 128
SPANS = 4
SP = ("sp_0", "sp_1", "sp_2")
SP_TP = ("sp_0", "sp_1", "sp_2", "tp")
EPS = 1e-06
WIDE_SCALE = 128 ** (-0.5)
NARROW_SCALE = 64 ** (-0.5)
F32 = jnp.float32
BF16 = jnp.bfloat16


def position_tables(devices):
    lane = np.arange(LANES)

    def inverse(head_dim):
        half = head_dim // 2
        return 10000.0 ** (-2.0 * (lane % half) / head_dim), np.where(
            lane % head_dim < half, -1.0, 1.0
        )

    row = np.arange(SPAN)[:, None]
    first = (np.arange(devices * SPANS) * SPAN)[:, None]
    inside, starts = [], []
    for head_dim in (128, 64):
        rate, sign = inverse(head_dim)
        inside += [np.cos(row * rate), np.sin(row * rate) * sign]
        starts += [
            np.cos(first * rate).reshape(devices, SPANS, LANES),
            (np.sin(first * rate) * sign).reshape(devices, SPANS, LANES),
        ]
    return (
        np.stack(inside).astype(np.float32),
        np.concatenate(starts, axis=1).astype(np.float32),
    )


def span_tables(inside_ref, start_ref, span, group):
    cos_row, sin_row = inside_ref[2 * group], inside_ref[2 * group + 1]
    cos_start = start_ref[0, pl.ds(2 * group * SPANS + span, 1), :]
    sin_start = start_ref[0, pl.ds((2 * group + 1) * SPANS + span, 1), :]
    return (
        cos_row * cos_start - sin_row * sin_start,
        sin_row * cos_start + cos_row * sin_start,
    )


def rotated_wide(x, tables):
    x = x.astype(F32)
    return x * tables[0] + pltpu.roll(x, 64, 1) * tables[1]


def rotated_narrow(x, tables):
    x = x.astype(F32)
    lane = lax.broadcasted_iota(jnp.int32, x.shape, 1)
    partner = jnp.where((lane & 32) == 0, pltpu.roll(x, 96, 1), pltpu.roll(x, 32, 1))
    return x * tables[0] + partner * tables[1]


def running_decay(wide_decay_ref, narrow_decay_ref, rows_ref):
    rows_ref[...] = jnp.zeros_like(rows_ref)
    rows_ref[0:3, :] = wide_decay_ref[...]
    rows_ref[3:5, :] = narrow_decay_ref[...]
    x = rows_ref[...]
    lane = lax.broadcasted_iota(jnp.int32, x.shape, 1)
    step = 1
    while step < SPAN:
        x = x + jnp.where(lane >= step, pltpu.roll(x, step, 1), 0.0)
        step *= 2
    return x


def low_rows(shape):
    return lax.broadcasted_iota(jnp.int32, shape, 0) < 64


def low_lanes(shape):
    return lax.broadcasted_iota(jnp.int32, shape, 1) < 64


def mm(a, b):
    return jnp.dot(a, b, preferred_element_type=F32)


def mm_nt(a, b):
    return lax.dot_general(a, b, (((1,), (1,)), ((), ())), preferred_element_type=F32)


def mm_tn(a, b):
    return lax.dot_general(a, b, (((0,), (0,)), ((), ())), preferred_element_type=F32)


def states_kernel(
    _, wk_ref, wv_ref, nk_ref, nv_ref, wd_ref, nd_ref, inside_ref, start_ref,
    before_ref, message_ref, rows_ref, state_ref, decay_ref,
):
    span = pl.program_id(0)

    @pl.when(span == 0)
    def _():
        state_ref[...] = jnp.zeros_like(state_ref)
        decay_ref[...] = jnp.zeros_like(decay_ref)

    total = running_decay(wd_ref, nd_ref, rows_ref)
    last = total[:, SPAN - 1 : SPAN]
    tail = jnp.exp(last - total).T
    kept = jnp.exp(last)
    before_ref[0] = state_ref[...]
    tables = span_tables(inside_ref, start_ref, span, 0)
    for head in range(3):
        cut = slice(head * 128, head * 128 + 128)
        keys = rotated_wide(wk_ref[:, cut], tables) * WIDE_SCALE
        scaled = (keys * tail[:, head : head + 1]).astype(BF16)
        state_ref[cut, :] = state_ref[cut, :] * kept[head : head + 1, :] + mm_tn(scaled, wv_ref[:, cut])
    tables = span_tables(inside_ref, start_ref, span, 1)
    keys = rotated_narrow(nk_ref[...], tables) * NARROW_SCALE
    tails = jnp.where(low_lanes((SPAN, LANES)), tail[:, 3:4], tail[:, 4:5])
    own = mm_tn((keys * tails).astype(BF16), nv_ref[...])
    square = (LANES, LANES)
    own = jnp.where(low_rows(square) == low_lanes(square), own, 0.0)
    keeps = jnp.where(low_rows(square), kept[3:4, :], kept[4:5, :])
    state_ref[384:512, :] = state_ref[384:512, :] * keeps + own
    decay_ref[...] += jnp.broadcast_to(last, decay_ref.shape)

    @pl.when(span == SPANS - 1)
    def _():
        sums = decay_ref[...]
        high = sums.astype(BF16).astype(F32)
        low = sums - high
        sub = lax.broadcasted_iota(jnp.int32, (8, LANES), 0)
        at = 0
        for head, count in enumerate((16, 16, 16, 8, 8)):
            pair = jnp.where(
                sub == 0,
                high[head : head + 1, :],
                jnp.where(sub == 1, low[head : head + 1, :], 0.0),
            )
            body = state_ref[at * 8 : (at + count) * 8, :].reshape(count, 8, LANES)
            ends = jnp.broadcast_to(pair[None], (count, 8, LANES))
            message_ref[at : at + count] = jnp.concatenate([body, ends], axis=1).astype(BF16)
            at += count


def prefix_kernel(message_ref, out_ref):
    devices = message_ref.shape[0]
    carried = jnp.zeros((8, LANES), F32)
    for k in range(devices):
        out_ref[k] = carried.astype(BF16)
        if k + 1 < devices:
            piece = message_ref[k].astype(F32)
            kept = jnp.exp(piece[8:9, :] + piece[9:10, :])
            carried = carried * kept + piece[0:8, :]


def gated(output, gate, scale):
    gate = gate.astype(F32)
    return (output * scale * (gate / (1.0 + jnp.exp(-gate)))).astype(BF16)


def finish_kernel(
    _, wq_ref, wk_ref, wv_ref, wg_ref, nq_ref, nk_ref, nv_ref, ng_ref, wd_ref, nd_ref,
    inside_ref, start_ref, before_ref, prefix_ref, wide_out_ref, narrow_out_ref,
    out_ref, rows_ref, decay_ref, mixed_ref,
):
    span = pl.program_id(0)

    @pl.when(span == 0)
    def _():
        decay_ref[...] = jnp.zeros_like(decay_ref)

    total = running_decay(wd_ref, nd_ref, rows_ref)
    columns = total.T
    grown = jnp.exp(columns)
    earlier = jnp.exp(decay_ref[...])
    square = (SPAN, SPAN)
    causal = lax.broadcasted_iota(jnp.int32, square, 0) >= lax.broadcasted_iota(jnp.int32, square, 1)

    def weights(scores, head):
        gaps = columns[:, head : head + 1] - total[head : head + 1, :]
        return (scores * jnp.exp(jnp.where(causal, gaps, -jnp.inf))).astype(BF16)

    tables = span_tables(inside_ref, start_ref, span, 0)
    for head in range(3):
        cut = slice(head * 128, head * 128 + 128)
        queries = rotated_wide(wq_ref[:, cut], tables).astype(BF16)
        keys = (rotated_wide(wk_ref[:, cut], tables) * WIDE_SCALE).astype(BF16)
        within = mm(weights(mm_nt(queries, keys), head), wv_ref[:, cut])
        entering = (
            prefix_ref[cut, :].astype(F32) * earlier[head : head + 1, :] + before_ref[0, cut, :]
        ).astype(BF16)
        output = within + mm(queries, entering) * grown[:, head : head + 1]
        scale = lax.rsqrt(jnp.mean(output * output, axis=-1, keepdims=True) + EPS)
        mixed_ref[:, cut] = gated(output, wg_ref[:, cut], scale)

    tables = span_tables(inside_ref, start_ref, span, 1)
    queries = rotated_narrow(nq_ref[...], tables).astype(BF16)
    keys = (rotated_narrow(nk_ref[...], tables) * NARROW_SCALE).astype(BF16)
    values = nv_ref[...]
    low = low_lanes(square)
    none = jnp.zeros_like(queries)
    within = jnp.where(
        low,
        mm(weights(mm_nt(jnp.where(low, queries, none), keys), 3), values),
        mm(weights(mm_nt(jnp.where(low, none, queries), keys), 4), values),
    )
    fades = jnp.where(low_rows(square), earlier[3:4, :], earlier[4:5, :])
    entering = (prefix_ref[384:512, :].astype(F32) * fades + before_ref[0, 384:512, :]).astype(BF16)
    output = within + mm(queries, entering) * jnp.where(low, grown[:, 3:4], grown[:, 4:5])
    squares = output * output
    first = jnp.sum(jnp.where(low, squares, 0.0), axis=-1, keepdims=True)
    second = jnp.sum(jnp.where(low, 0.0, squares), axis=-1, keepdims=True)
    scale = lax.rsqrt(jnp.where(low, first, second) * (1.0 / 64.0) + EPS)
    mixed_ref[:, 384:512] = gated(output, ng_ref[...], scale)
    decay_ref[...] += jnp.broadcast_to(total[:, SPAN - 1 : SPAN], decay_ref.shape)

    out_ref[0] = (
        mm(mixed_ref[:, 0:384], wide_out_ref[...]) + mm(mixed_ref[:, 384:512], narrow_out_ref[...])
    ).astype(BF16)


def rms(values, gain):
    return values * lax.rsqrt(jnp.mean(values * values, axis=-1, keepdims=True) + EPS) * gain


def norms_kernel(tiles_ref, residual_ref, mix_ref, pre_ref, updated_ref, normed_ref):
    projected = tiles_ref[0].astype(F32)
    for k in range(1, tiles_ref.shape[0]):
        projected = projected + tiles_ref[k].astype(F32)
    updated = (residual_ref[...].astype(F32) + rms(projected, mix_ref[...])).astype(BF16)
    updated_ref[...] = updated
    normed = rms(updated.astype(F32), pre_ref[...]).astype(BF16)
    for k in range(normed_ref.shape[0]):
        normed_ref[k] = normed


def mixer_kernel(x_ref, up_ref, down_ref, out_ref, hidden_ref, *, steps, block):
    step = pl.program_id(0)

    @pl.when(step < steps)
    def _():
        weight = up_ref[...].reshape(x_ref.shape[1], block)
        rectified = jnp.maximum(mm(x_ref[...], weight), 0.0)
        at = pl.multiple_of(step * block, block)
        hidden_ref[:, pl.ds(at, block)] = (rectified * rectified).astype(BF16)

    @pl.when(step >= steps)
    def _():
        weight = down_ref[...].reshape(block, hidden_ref.shape[1])
        out_ref[...] = mm_nt(hidden_ref[...], weight).astype(BF16)


def local(
    wide_query, wide_key, wide_value, wide_gate,
    narrow_query, narrow_key, narrow_value, narrow_gate,
    wide_decay, narrow_decay, residual, wide_out, narrow_out,
    up_weight, down_weight, gain_mix, gain_pre, gain_mlp,
):
    devices = lax.axis_size(SP)
    ranks = lax.axis_size("tp")
    length, width = wide_query.shape[0], residual.shape[1]
    rows = residual.shape[0]
    share = up_weight.shape[0]
    units = up_weight.shape[1]

    both = lax.all_gather(
        jnp.concatenate([up_weight, down_weight.T], axis=0), SP, axis=0, tiled=True
    ).reshape(devices, 2, share, units)

    inside, starts = (jnp.asarray(t) for t in position_tables(devices))
    index = lax.axis_index(SP).astype(jnp.int32).reshape(1)
    wide_block = pl.BlockSpec((SPAN, 384), lambda s, i: (s, 0))
    narrow_block = pl.BlockSpec((SPAN, 128), lambda s, i: (s, 0))
    decay_blocks = [
        pl.BlockSpec((3, SPAN), lambda s, i: (0, s)),
        pl.BlockSpec((2, SPAN), lambda s, i: (0, s)),
    ]
    table_blocks = [
        pl.BlockSpec((4, SPAN, LANES), lambda s, i: (0, 0, 0)),
        pl.BlockSpec((1, 4 * SPANS, LANES), lambda s, i: (i[0], 0, 0)),
    ]
    before_block = pl.BlockSpec((1, 512, LANES), lambda s, i: (s, 0, 0))
    before, message = pl.pallas_call(
        states_kernel,
        out_shape=(
            jax.ShapeDtypeStruct((SPANS, 512, LANES), F32),
            jax.ShapeDtypeStruct((devices, 16, LANES), BF16),
        ),
        grid_spec=pltpu.PrefetchScalarGridSpec(
            num_scalar_prefetch=1,
            grid=(SPANS,),
            in_specs=[wide_block, wide_block, narrow_block, narrow_block, *decay_blocks, *table_blocks],
            out_specs=[
                before_block,
                pl.BlockSpec((devices, 16, LANES), lambda s, i: (0, 0, 0)),
            ],
            scratch_shapes=[
                pltpu.VMEM((8, LANES), F32),
                pltpu.VMEM((512, LANES), F32),
                pltpu.VMEM((8, LANES), F32),
            ],
        ),
        name="states",
        cost_estimate=pl.CostEstimate(flops=60_000_000, bytes_accessed=2_500_000, transcendentals=20_000),
    )(index, wide_key, wide_value, narrow_key, narrow_value, wide_decay, narrow_decay, inside, starts)

    arrived = lax.all_to_all(message, SP, 0, 0, tiled=True)
    prefixes = pl.pallas_call(
        prefix_kernel,
        out_shape=jax.ShapeDtypeStruct((devices, 8, LANES), BF16),
        name="prefix",
        cost_estimate=pl.CostEstimate(flops=2_000_000, bytes_accessed=400_000, transcendentals=8_000),
    )(arrived)
    prefix = lax.all_to_all(prefixes, SP, 0, 0, tiled=True).reshape(512, LANES)

    partial = pl.pallas_call(
        finish_kernel,
        out_shape=jax.ShapeDtypeStruct((SPANS, SPAN, width), BF16),
        grid_spec=pltpu.PrefetchScalarGridSpec(
            num_scalar_prefetch=1,
            grid=(SPANS,),
            in_specs=[
                wide_block, wide_block, wide_block, wide_block,
                narrow_block, narrow_block, narrow_block, narrow_block,
                *decay_blocks, *table_blocks, before_block,
                pl.BlockSpec((512, LANES), lambda s, i: (0, 0)),
                pl.BlockSpec((384, width), lambda s, i: (0, 0)),
                pl.BlockSpec((128, width), lambda s, i: (0, 0)),
            ],
            out_specs=pl.BlockSpec((1, SPAN, width), lambda s, i: (s, 0, 0)),
            scratch_shapes=[
                pltpu.VMEM((8, LANES), F32),
                pltpu.VMEM((8, LANES), F32),
                pltpu.VMEM((SPAN, 512), BF16),
            ],
        ),
        name="finish",
        cost_estimate=pl.CostEstimate(flops=1_400_000_000, bytes_accessed=9_000_000, transcendentals=600_000),
    )(
        index, wide_query, wide_key, wide_value, wide_gate,
        narrow_query, narrow_key, narrow_value, narrow_gate,
        wide_decay, narrow_decay, inside, starts, before, prefix, wide_out, narrow_out,
    )

    tiles = lax.all_to_all(partial.reshape(ranks, rows, width), "tp", 0, 0, tiled=True)
    updated, normed = pl.pallas_call(
        norms_kernel,
        out_shape=(
            jax.ShapeDtypeStruct((rows, width), BF16),
            jax.ShapeDtypeStruct((ranks, rows, width), BF16),
        ),
        name="norms",
        cost_estimate=pl.CostEstimate(flops=4_000_000, bytes_accessed=6_000_000, transcendentals=300),
    )(tiles, residual, gain_mix.reshape(1, width), gain_pre.reshape(1, width))
    block_rows = lax.all_to_all(normed, "tp", 0, 0, tiled=True).reshape(length, width)

    block = 256
    steps = units // block
    lowered = pl.pallas_call(
        functools.partial(mixer_kernel, steps=steps, block=block),
        out_shape=jax.ShapeDtypeStruct((length, width), BF16),
        grid=(2 * steps,),
        in_specs=[
            pl.BlockSpec((length, width), lambda i: (0, 0)),
            pl.BlockSpec((devices, 1, share, block), lambda i: (0, 0, 0, jnp.minimum(i, steps - 1))),
            pl.BlockSpec(
                (block // share, 1, share, units), lambda i: (jnp.maximum(i - steps, 0), 1, 0, 0)
            ),
        ],
        out_specs=pl.BlockSpec((length, block), lambda i: (0, jnp.maximum(i - steps, 0))),
        scratch_shapes=[pltpu.VMEM((length, units), BF16)],
        compiler_params=pltpu.CompilerParams(vmem_limit_bytes=32 * 1024 * 1024),
        name="mixer",
        cost_estimate=pl.CostEstimate(
            flops=4 * length * width * units, bytes_accessed=22_000_000, transcendentals=0
        ),
    )(block_rows, both, both)
    lowered = lax.all_to_all(lowered.reshape(ranks, rows, width), "tp", 0, 0, tiled=True)
    lowered = jnp.sum(lowered.astype(F32), axis=0)
    return (updated.astype(F32) + rms(lowered, gain_mlp)).astype(BF16)


def solution(mesh):
    finer = Mesh(mesh.devices.reshape(8, 4, 2, mesh.shape["tp"]), ("sp_0", "sp_1", "sp_2", "tp"))
    in_specs = (
        *([P(SP, "tp")] * 8),
        P("tp", SP),
        P("tp", SP),
        P(SP_TP, None),
        P("tp", None),
        P("tp", None),
        P(SP, "tp"),
        P("tp", SP),
        P(),
        P(),
        P(),
    )
    return jax.shard_map(
        local, mesh=finer, in_specs=in_specs, out_specs=P(SP_TP, None), check_vma=False
    )
```

```python
import functools

import jax
import jax.numpy as jnp
import numpy as np
from jax import lax
from jax.experimental import pallas as pl
from jax.experimental.pallas import tpu as pltpu
from jax.sharding import Mesh
from jax.sharding import PartitionSpec as P

SPAN = 128
LANES = 128
SPANS = 4
SP = ("sp_0", "sp_1", "sp_2")
SP_TP = ("sp_0", "sp_1", "sp_2", "tp")
EPS = 1e-06
WIDE_SCALE = 128 ** (-0.5)
NARROW_SCALE = 64 ** (-0.5)
F32 = jnp.float32
BF16 = jnp.bfloat16


def position_tables(devices):
    lane = np.arange(LANES)

    def inverse(head_dim):
        half = head_dim // 2
        return 10000.0 ** (-2.0 * (lane % half) / head_dim), np.where(
            lane % head_dim < half, -1.0, 1.0
        )

    row = np.arange(SPAN)[:, None]
    first = (np.arange(devices * SPANS) * SPAN)[:, None]
    inside, starts = [], []
    for head_dim in (128, 64):
        rate, sign = inverse(head_dim)
        inside += [np.cos(row * rate), np.sin(row * rate) * sign]
        starts += [
            np.cos(first * rate).reshape(devices, SPANS, LANES),
            (np.sin(first * rate) * sign).reshape(devices, SPANS, LANES),
        ]
    return (
        np.stack(inside).astype(np.float32),
        np.concatenate(starts, axis=1).astype(np.float32),
    )


def span_tables(inside_ref, start_ref, span, group):
    cos_row, sin_row = inside_ref[2 * group], inside_ref[2 * group + 1]
    cos_start = start_ref[0, pl.ds(2 * group * SPANS + span, 1), :]
    sin_start = start_ref[0, pl.ds((2 * group + 1) * SPANS + span, 1), :]
    return (
        cos_row * cos_start - sin_row * sin_start,
        sin_row * cos_start + cos_row * sin_start,
    )


def rotated_wide(x, tables):
    x = x.astype(F32)
    return x * tables[0] + pltpu.roll(x, 64, 1) * tables[1]


def rotated_narrow(x, tables):
    x = x.astype(F32)
    lane = lax.broadcasted_iota(jnp.int32, x.shape, 1)
    partner = jnp.where((lane & 32) == 0, pltpu.roll(x, 96, 1), pltpu.roll(x, 32, 1))
    return x * tables[0] + partner * tables[1]


def running_decay(wide_decay_ref, narrow_decay_ref, rows_ref):
    rows_ref[...] = jnp.zeros_like(rows_ref)
    rows_ref[0:3, :] = wide_decay_ref[...]
    rows_ref[3:5, :] = narrow_decay_ref[...]
    x = rows_ref[...]
    lane = lax.broadcasted_iota(jnp.int32, x.shape, 1)
    step = 1
    while step < SPAN:
        x = x + jnp.where(lane >= step, pltpu.roll(x, step, 1), 0.0)
        step *= 2
    return x


def low_rows(shape):
    return lax.broadcasted_iota(jnp.int32, shape, 0) < 64


def low_lanes(shape):
    return lax.broadcasted_iota(jnp.int32, shape, 1) < 64


def mm(a, b):
    return jnp.dot(a, b, preferred_element_type=F32)


def mm_nt(a, b):
    return lax.dot_general(a, b, (((1,), (1,)), ((), ())), preferred_element_type=F32)


def mm_tn(a, b):
    return lax.dot_general(a, b, (((0,), (0,)), ((), ())), preferred_element_type=F32)


def states_kernel(
    _, wk_ref, wv_ref, nk_ref, nv_ref, wd_ref, nd_ref, inside_ref, start_ref,
    before_ref, earlier_ref, message_ref, rows_ref, state_ref, decay_ref,
):
    span = pl.program_id(0)

    @pl.when(span == 0)
    def _():
        state_ref[...] = jnp.zeros_like(state_ref)
        decay_ref[...] = jnp.zeros_like(decay_ref)

    total = running_decay(wd_ref, nd_ref, rows_ref)
    last = total[:, SPAN - 1 : SPAN]
    tail = jnp.exp(last - total).T
    kept = jnp.exp(last)
    before_ref[0] = state_ref[...]
    earlier_ref[0] = decay_ref[...]
    tables = span_tables(inside_ref, start_ref, span, 0)
    for head in range(3):
        cut = slice(head * 128, head * 128 + 128)
        keys = rotated_wide(wk_ref[:, cut], tables) * WIDE_SCALE
        scaled = (keys * tail[:, head : head + 1]).astype(BF16)
        state_ref[cut, :] = state_ref[cut, :] * kept[head : head + 1, :] + mm_tn(scaled, wv_ref[:, cut])
    tables = span_tables(inside_ref, start_ref, span, 1)
    keys = rotated_narrow(nk_ref[...], tables) * NARROW_SCALE
    tails = jnp.where(low_lanes((SPAN, LANES)), tail[:, 3:4], tail[:, 4:5])
    own = mm_tn((keys * tails).astype(BF16), nv_ref[...])
    square = (LANES, LANES)
    own = jnp.where(low_rows(square) == low_lanes(square), own, 0.0)
    keeps = jnp.where(low_rows(square), kept[3:4, :], kept[4:5, :])
    state_ref[384:512, :] = state_ref[384:512, :] * keeps + own
    decay_ref[...] += jnp.broadcast_to(last, decay_ref.shape)

    @pl.when(span == SPANS - 1)
    def _():
        sums = decay_ref[...]
        high = sums.astype(BF16).astype(F32)
        low = sums - high
        sub = lax.broadcasted_iota(jnp.int32, (8, LANES), 0)
        at = 0
        for head, count in enumerate((16, 16, 16, 8, 8)):
            pair = jnp.where(
                sub == 0,
                high[head : head + 1, :],
                jnp.where(sub == 1, low[head : head + 1, :], 0.0),
            )
            body = state_ref[at * 8 : (at + count) * 8, :].reshape(count, 8, LANES)
            ends = jnp.broadcast_to(pair[None], (count, 8, LANES))
            message_ref[at : at + count] = jnp.concatenate([body, ends], axis=1).astype(BF16)
            at += count


def prefix_kernel(message_ref, out_ref):
    devices = message_ref.shape[0]
    carried = jnp.zeros((8, LANES), F32)
    for k in range(devices):
        out_ref[k] = carried.astype(BF16)
        if k + 1 < devices:
            piece = message_ref[k].astype(F32)
            kept = jnp.exp(piece[8:9, :] + piece[9:10, :])
            carried = carried * kept + piece[0:8, :]


def gated(output, gate, scale):
    gate = gate.astype(F32)
    return (output * scale * (gate / (1.0 + jnp.exp(-gate)))).astype(BF16)


def finish_kernel(
    order_ref, wq_ref, wk_ref, wv_ref, wg_ref, nq_ref, nk_ref, nv_ref, ng_ref, wd_ref, nd_ref,
    inside_ref, start_ref, before_ref, earlier_ref, prefix_ref, wide_out_ref, narrow_out_ref,
    *out_refs, first,
):
    *out_refs, rows_ref, mixed_ref = out_refs
    span = order_ref[1 + first + pl.program_id(0)]
    total = running_decay(wd_ref, nd_ref, rows_ref)
    columns = total.T
    grown = jnp.exp(columns)
    earlier = jnp.exp(earlier_ref[0])
    square = (SPAN, SPAN)
    causal = lax.broadcasted_iota(jnp.int32, square, 0) >= lax.broadcasted_iota(jnp.int32, square, 1)

    def weights(scores, head):
        gaps = columns[:, head : head + 1] - total[head : head + 1, :]
        return (scores * jnp.exp(jnp.where(causal, gaps, -jnp.inf))).astype(BF16)

    tables = span_tables(inside_ref, start_ref, span, 0)
    for head in range(3):
        cut = slice(head * 128, head * 128 + 128)
        queries = rotated_wide(wq_ref[:, cut], tables).astype(BF16)
        keys = (rotated_wide(wk_ref[:, cut], tables) * WIDE_SCALE).astype(BF16)
        within = mm(weights(mm_nt(queries, keys), head), wv_ref[:, cut])
        entering = (
            prefix_ref[cut, :].astype(F32) * earlier[head : head + 1, :] + before_ref[0, cut, :]
        ).astype(BF16)
        output = within + mm(queries, entering) * grown[:, head : head + 1]
        scale = lax.rsqrt(jnp.mean(output * output, axis=-1, keepdims=True) + EPS)
        mixed_ref[:, cut] = gated(output, wg_ref[:, cut], scale)

    tables = span_tables(inside_ref, start_ref, span, 1)
    queries = rotated_narrow(nq_ref[...], tables).astype(BF16)
    keys = (rotated_narrow(nk_ref[...], tables) * NARROW_SCALE).astype(BF16)
    values = nv_ref[...]
    low = low_lanes(square)
    none = jnp.zeros_like(queries)
    within = jnp.where(
        low,
        mm(weights(mm_nt(jnp.where(low, queries, none), keys), 3), values),
        mm(weights(mm_nt(jnp.where(low, none, queries), keys), 4), values),
    )
    fades = jnp.where(low_rows(square), earlier[3:4, :], earlier[4:5, :])
    entering = (prefix_ref[384:512, :].astype(F32) * fades + before_ref[0, 384:512, :]).astype(BF16)
    output = within + mm(queries, entering) * jnp.where(low, grown[:, 3:4], grown[:, 4:5])
    squares = output * output
    left = jnp.sum(jnp.where(low, squares, 0.0), axis=-1, keepdims=True)
    right = jnp.sum(jnp.where(low, 0.0, squares), axis=-1, keepdims=True)
    scale = lax.rsqrt(jnp.where(low, left, right) * (1.0 / 64.0) + EPS)
    mixed_ref[:, 384:512] = gated(output, ng_ref[...], scale)

    projected = (
        mm(mixed_ref[:, 0:384], wide_out_ref[...]) + mm(mixed_ref[:, 384:512], narrow_out_ref[...])
    ).astype(BF16)
    if len(out_refs) == 2:
        half = SPAN // 2
        out_refs[0][...] = projected[:half]
        out_refs[1][...] = projected[half:]
    else:
        out_refs[0][0] = projected


def join_kernel(minus_ref, plus_ref, from_below_ref, from_above_ref, minus_out_ref, plus_out_ref):
    part = pl.program_id(0)

    @pl.when(part == 0)
    def _():
        minus_out_ref[...] = minus_ref[...]
        plus_out_ref[...] = (plus_ref[...].astype(F32) + from_below_ref[...].astype(F32)).astype(BF16)

    @pl.when(part == 1)
    def _():
        minus_out_ref[...] = (minus_ref[...].astype(F32) + from_above_ref[...].astype(F32)).astype(BF16)
        plus_out_ref[...] = plus_ref[...]


def rms(values, gain):
    return values * lax.rsqrt(jnp.mean(values * values, axis=-1, keepdims=True) + EPS) * gain


def norms_kernel(own_ref, below_ref, above_ref, residual_ref, mix_ref, pre_ref, updated_ref, normed_ref):
    projected = own_ref[...].astype(F32) + below_ref[...].astype(F32) + above_ref[...].astype(F32)
    updated = (residual_ref[...].astype(F32) + rms(projected, mix_ref[...])).astype(BF16)
    updated_ref[...] = updated
    normed_ref[...] = rms(updated.astype(F32), pre_ref[...]).astype(BF16)


def result_kernel(own_ref, below_ref, above_ref, updated_ref, gain_ref, out_ref):
    lowered = own_ref[...].astype(F32) + below_ref[...].astype(F32) + above_ref[...].astype(F32)
    out_ref[...] = (updated_ref[...].astype(F32) + rms(lowered.T, gain_ref[...])).astype(BF16)


def far_mixer_kernel(
    own_ref, far_low_ref, far_high_ref, below_ref, above_ref, up_ref, down_ref,
    hidden_ref, out_ref, low_ref, high_ref, x_ref, now_ref, *, steps, block,
):
    step = pl.program_id(0)
    rows = own_ref.shape[0]
    half = rows // 2

    @pl.when(step == 0)
    def _():
        x_ref[0:rows] = own_ref[...]
        x_ref[rows : rows + half] = far_low_ref[...]
        x_ref[rows + half : 2 * rows] = far_high_ref[...]
        x_ref[2 * rows : 3 * rows] = below_ref[...]
        x_ref[3 * rows :] = above_ref[...]

    @pl.when(step < steps)
    def _():
        rectified = jnp.maximum(mm(x_ref[...], up_ref[...].reshape(x_ref.shape[1], block)), 0.0)
        hidden = (rectified * rectified).astype(BF16).T
        hidden_ref[...] = hidden[:, 2 * rows :]
        now_ref[pl.ds(pl.multiple_of(step * block, block), block), :] = hidden[:, : 2 * rows]

    @pl.when(step >= steps)
    def _():
        lowered = mm(down_ref[...].reshape(block, now_ref.shape[0]), now_ref[...]).astype(BF16)
        out_ref[...] = lowered[:, :rows]

        @pl.when(step < steps + steps // 2)
        def _():
            low_ref[...] = lowered[:, rows:]

        @pl.when(step >= steps + steps // 2)
        def _():
            high_ref[...] = lowered[:, rows:]


def near_mixer_kernel(hidden_ref, down_ref, minus_ref, plus_ref):
    lowered = mm(down_ref[...].reshape(-1, hidden_ref.shape[0]), hidden_ref[...]).astype(BF16)
    rows = minus_ref.shape[1]
    minus_ref[...] = lowered[:, :rows]
    plus_ref[...] = lowered[:, rows:]


SMALL = pltpu.CompilerParams(vmem_limit_bytes=16 * 1024 * 1024)
LARGE = pltpu.CompilerParams(vmem_limit_bytes=50 * 1024 * 1024)


def shifted(array, axis, by):
    size = lax.axis_size(axis)
    return lax.ppermute(array, axis, [(k, (k + by) % size) for k in range(size)])


def joined(minus, plus, from_below, from_above, picks=(None, None)):
    half, width = from_below.shape
    flat = pl.BlockSpec((half, width), lambda i: (i, 0))
    kept = pl.BlockSpec((half, width), lambda i: (0, 0))
    out = jax.ShapeDtypeStruct((2 * half, width), BF16)

    def source(pick):
        if pick is None:
            return flat
        return pl.BlockSpec((None, half, width), lambda i: (pick, i, 0))

    return pl.pallas_call(
        join_kernel,
        out_shape=(out, out),
        grid=(2,),
        in_specs=[source(picks[0]), source(picks[1]), kept, kept],
        out_specs=[flat, flat],
        compiler_params=SMALL,
        name="join",
        cost_estimate=pl.CostEstimate(flops=1_000_000, bytes_accessed=3_500_000, transcendentals=0),
    )(minus, plus, from_below, from_above)


def local(
    wide_query, wide_key, wide_value, wide_gate,
    narrow_query, narrow_key, narrow_value, narrow_gate,
    wide_decay, narrow_decay, residual, wide_out, narrow_out,
    up_weight, down_weight, gain_mix, gain_pre, gain_mlp,
):
    devices = lax.axis_size(SP)
    ranks = lax.axis_size("tp")
    length, width = wide_query.shape[0], residual.shape[1]
    rows = residual.shape[0]
    share = up_weight.shape[0]
    units = up_weight.shape[1]

    both = lax.all_gather(
        jnp.concatenate([up_weight, down_weight.T], axis=0), SP, axis=0, tiled=True
    ).reshape(devices, 2, share, units)

    inside, starts = (jnp.asarray(t) for t in position_tables(devices))
    turn = lax.axis_index("tp")
    order = jnp.stack(
        [lax.axis_index(SP), (turn + 2) % ranks, turn, (turn + ranks - 1) % ranks, (turn + 1) % ranks]
    ).astype(jnp.int32)
    table_blocks = [
        pl.BlockSpec((4, SPAN, LANES), lambda s, i: (0, 0, 0)),
        pl.BlockSpec((1, 4 * SPANS, LANES), lambda s, i: (i[0], 0, 0)),
    ]

    def span_blocks(at):
        return (
            pl.BlockSpec((SPAN, 384), lambda s, i: (at(s, i), 0)),
            pl.BlockSpec((SPAN, 128), lambda s, i: (at(s, i), 0)),
            [
                pl.BlockSpec((3, SPAN), lambda s, i: (0, at(s, i))),
                pl.BlockSpec((2, SPAN), lambda s, i: (0, at(s, i))),
            ],
            [
                pl.BlockSpec((1, 512, LANES), lambda s, i: (at(s, i), 0, 0)),
                pl.BlockSpec((1, 8, LANES), lambda s, i: (at(s, i), 0, 0)),
            ],
        )

    wide_block, narrow_block, decay_blocks, state_blocks = span_blocks(lambda s, i: s)
    before, earlier, message = pl.pallas_call(
        states_kernel,
        out_shape=(
            jax.ShapeDtypeStruct((SPANS, 512, LANES), F32),
            jax.ShapeDtypeStruct((SPANS, 8, LANES), F32),
            jax.ShapeDtypeStruct((devices, 16, LANES), BF16),
        ),
        grid_spec=pltpu.PrefetchScalarGridSpec(
            num_scalar_prefetch=1,
            grid=(SPANS,),
            in_specs=[wide_block, wide_block, narrow_block, narrow_block, *decay_blocks, *table_blocks],
            out_specs=[*state_blocks, pl.BlockSpec((devices, 16, LANES), lambda s, i: (0, 0, 0))],
            scratch_shapes=[
                pltpu.VMEM((8, LANES), F32),
                pltpu.VMEM((512, LANES), F32),
                pltpu.VMEM((8, LANES), F32),
            ],
        ),
        name="states",
        cost_estimate=pl.CostEstimate(flops=60_000_000, bytes_accessed=2_500_000, transcendentals=20_000),
    )(order, wide_key, wide_value, narrow_key, narrow_value, wide_decay, narrow_decay, inside, starts)

    arrived = lax.all_to_all(message, SP, 0, 0, tiled=True)
    prefixes = pl.pallas_call(
        prefix_kernel,
        out_shape=jax.ShapeDtypeStruct((devices, 8, LANES), BF16),
        compiler_params=SMALL,
        name="prefix",
        cost_estimate=pl.CostEstimate(flops=2_000_000, bytes_accessed=400_000, transcendentals=8_000),
    )(arrived)
    prefix = lax.all_to_all(prefixes, SP, 0, 0, tiled=True).reshape(512, LANES)

    def finish(first, count, out_shape, out_specs):
        wide, narrow, decays, states = span_blocks(lambda s, i: i[1 + first + s])
        return pl.pallas_call(
            functools.partial(finish_kernel, first=first),
            out_shape=out_shape,
            grid_spec=pltpu.PrefetchScalarGridSpec(
                num_scalar_prefetch=1,
                grid=(count,),
                in_specs=[
                    wide, wide, wide, wide, narrow, narrow, narrow, narrow,
                    *decays, *table_blocks, *states,
                    pl.BlockSpec((512, LANES), lambda s, i: (0, 0)),
                    pl.BlockSpec((384, width), lambda s, i: (0, 0)),
                    pl.BlockSpec((128, width), lambda s, i: (0, 0)),
                ],
                out_specs=out_specs,
                scratch_shapes=[pltpu.VMEM((8, LANES), F32), pltpu.VMEM((SPAN, 512), BF16)],
            ),
            compiler_params=SMALL,
            name="finish" if first else "finish_far",
            cost_estimate=pl.CostEstimate(
                flops=350_000_000 * count,
                bytes_accessed=3_000_000 + 1_500_000 * count,
                transcendentals=150_000 * count,
            ),
        )(
            order, wide_query, wide_key, wide_value, wide_gate,
            narrow_query, narrow_key, narrow_value, narrow_gate,
            wide_decay, narrow_decay, inside, starts, before, earlier, prefix, wide_out, narrow_out,
        )

    half = rows // 2
    half_out = jax.ShapeDtypeStruct((half, width), BF16)
    near_out = jax.ShapeDtypeStruct((3, rows, width), BF16)
    low, high = finish(
        0, 1, (half_out, half_out), [pl.BlockSpec((half, width), lambda s, i: (0, 0))] * 2
    )
    low, high = shifted(low, "tp", 1), shifted(high, "tp", -1)
    (near,) = finish(
        1, 3, (near_out,), [pl.BlockSpec((1, rows, width), lambda s, i: (s, 0, 0))]
    )
    minus, plus = joined(near, near, low, high, (1, 2))
    below, above = shifted(plus, "tp", 1), shifted(minus, "tp", -1)
    lines = 32
    flat = pl.BlockSpec((lines, width), lambda i: (i, 0))
    gain = pl.BlockSpec((1, width), lambda i: (0, 0))
    updated, normed = pl.pallas_call(
        norms_kernel,
        out_shape=[jax.ShapeDtypeStruct((rows, width), BF16)] * 2,
        grid=(rows // lines,),
        in_specs=[
            pl.BlockSpec((None, lines, width), lambda i: (0, i, 0)), flat, flat, flat, gain, gain,
        ],
        out_specs=[flat, flat],
        compiler_params=SMALL,
        name="norms",
        cost_estimate=pl.CostEstimate(flops=4_000_000, bytes_accessed=3_500_000, transcendentals=300),
    )(near, below, above, residual, gain_mix.reshape(1, width), gain_pre.reshape(1, width))
    below, above = shifted(normed, "tp", 1), shifted(normed, "tp", -1)
    low, high = shifted(below[:half], "tp", 1), shifted(above[half:], "tp", -1)

    block = min(1024, units // 2)
    steps, halves = units // block, units // block // 2
    resident = pl.BlockSpec((rows, width), lambda i: (0, 0))
    resident_half = pl.BlockSpec((half, width), lambda i: (0, 0))
    turned = jax.ShapeDtypeStruct((width, rows), BF16)
    turned_half = jax.ShapeDtypeStruct((width // 2, rows), BF16)
    hidden, own, low, high = pl.pallas_call(
        functools.partial(far_mixer_kernel, steps=steps, block=block),
        out_shape=(
            jax.ShapeDtypeStruct((units, 2 * rows), BF16), turned, turned_half, turned_half,
        ),
        grid=(2 * steps,),
        in_specs=[
            resident, resident_half, resident_half, resident, resident,
            pl.BlockSpec((devices, 1, share, block), lambda i: (0, 0, 0, jnp.minimum(i, steps - 1))),
            pl.BlockSpec(
                (block // share, 1, share, units), lambda i: (jnp.maximum(i - steps, 0), 1, 0, 0)
            ),
        ],
        out_specs=[
            pl.BlockSpec((block, 2 * rows), lambda i: (jnp.minimum(i, steps - 1), 0)),
            pl.BlockSpec((block, rows), lambda i: (jnp.maximum(i - steps, 0), 0)),
            pl.BlockSpec((block, rows), lambda i: (jnp.clip(i - steps, 0, halves - 1), 0)),
            pl.BlockSpec((block, rows), lambda i: (jnp.clip(i - steps - halves, 0, halves - 1), 0)),
        ],
        scratch_shapes=[pltpu.VMEM((4 * rows, width), BF16), pltpu.VMEM((units, 2 * rows), BF16)],
        compiler_params=LARGE,
        name="mixer_far",
        cost_estimate=pl.CostEstimate(
            flops=12 * rows * width * units, bytes_accessed=20_000_000, transcendentals=0
        ),
    )(normed, low, high, below, above, both, both)
    low, high = shifted(low, "tp", 1), shifted(high, "tp", -1)
    lasts = pl.BlockSpec((block, rows), lambda i: (i, 0))
    minus, plus = pl.pallas_call(
        near_mixer_kernel,
        out_shape=(turned, turned),
        grid=(width // block,),
        in_specs=[
            pl.BlockSpec((units, 2 * rows), lambda i: (0, 0)),
            pl.BlockSpec((block // share, 1, share, units), lambda i: (i, 1, 0, 0)),
        ],
        out_specs=[lasts, lasts],
        compiler_params=LARGE,
        name="mixer_near",
        cost_estimate=pl.CostEstimate(
            flops=4 * rows * width * units, bytes_accessed=12_000_000, transcendentals=0
        ),
    )(hidden, both)
    minus, plus = joined(minus, plus, low, high)
    below, above = shifted(plus, "tp", 1), shifted(minus, "tp", -1)
    return pl.pallas_call(
        result_kernel,
        out_shape=jax.ShapeDtypeStruct((rows, width), BF16),
        compiler_params=SMALL,
        name="result",
        cost_estimate=pl.CostEstimate(flops=4_000_000, bytes_accessed=3_500_000, transcendentals=300),
    )(own, below, above, updated, gain_mlp.reshape(1, width))


def solution(mesh):
    finer = Mesh(mesh.devices.reshape(8, 4, 2, mesh.shape["tp"]), ("sp_0", "sp_1", "sp_2", "tp"))
    in_specs = (
        *([P(SP, "tp")] * 8),
        P("tp", SP),
        P("tp", SP),
        P(SP_TP, None),
        P("tp", None),
        P("tp", None),
        P(SP, "tp"),
        P("tp", SP),
        P(),
        P(),
        P(),
    )
    return jax.shard_map(
        local, mesh=finer, in_specs=in_specs, out_specs=P(SP_TP, None), check_vma=False
    )
```

```python
import functools

import jax
import jax.numpy as jnp
import numpy as np
from jax import lax
from jax.experimental import pallas as pl
from jax.experimental.pallas import tpu as pltpu
from jax.sharding import Mesh
from jax.sharding import PartitionSpec as P

SPAN = 128
LANES = 128
SPANS = 4
SP = ("sp_0", "sp_1", "sp_2")
SP_TP = ("sp_0", "sp_1", "sp_2", "tp")
EPS = 1e-06
WIDE_SCALE = 128 ** (-0.5)
NARROW_SCALE = 64 ** (-0.5)
F32 = jnp.float32
BF16 = jnp.bfloat16


def position_tables(devices):
    lane = np.arange(LANES)

    def inverse(head_dim):
        half = head_dim // 2
        return 10000.0 ** (-2.0 * (lane % half) / head_dim), np.where(
            lane % head_dim < half, -1.0, 1.0
        )

    row = np.arange(SPAN)[:, None]
    first = (np.arange(devices * SPANS) * SPAN)[:, None]
    inside, starts = [], []
    for head_dim in (128, 64):
        rate, sign = inverse(head_dim)
        inside += [np.cos(row * rate), np.sin(row * rate) * sign]
        starts += [
            np.cos(first * rate).reshape(devices, SPANS, LANES),
            (np.sin(first * rate) * sign).reshape(devices, SPANS, LANES),
        ]
    return (
        np.stack(inside).astype(np.float32),
        np.concatenate(starts, axis=1).astype(np.float32),
    )


def span_tables(inside_ref, start_ref, span, group):
    cos_row, sin_row = inside_ref[2 * group], inside_ref[2 * group + 1]
    cos_start = start_ref[0, pl.ds(2 * group * SPANS + span, 1), :]
    sin_start = start_ref[0, pl.ds((2 * group + 1) * SPANS + span, 1), :]
    return (
        cos_row * cos_start - sin_row * sin_start,
        sin_row * cos_start + cos_row * sin_start,
    )


def rotated_wide(x, tables):
    x = x.astype(F32)
    return x * tables[0] + pltpu.roll(x, 64, 1) * tables[1]


def rotated_narrow(x, tables):
    x = x.astype(F32)
    lane = lax.broadcasted_iota(jnp.int32, x.shape, 1)
    partner = jnp.where((lane & 32) == 0, pltpu.roll(x, 96, 1), pltpu.roll(x, 32, 1))
    return x * tables[0] + partner * tables[1]


def running_decay(wide_decay_ref, narrow_decay_ref, rows_ref):
    rows_ref[...] = jnp.zeros_like(rows_ref)
    rows_ref[0:3, :] = wide_decay_ref[...]
    rows_ref[3:5, :] = narrow_decay_ref[...]
    x = rows_ref[...]
    lane = lax.broadcasted_iota(jnp.int32, x.shape, 1)
    step = 1
    while step < SPAN:
        x = x + jnp.where(lane >= step, pltpu.roll(x, step, 1), 0.0)
        step *= 2
    return x


def low_rows(shape):
    return lax.broadcasted_iota(jnp.int32, shape, 0) < 64


def low_lanes(shape):
    return lax.broadcasted_iota(jnp.int32, shape, 1) < 64


def mm(a, b):
    return jnp.dot(a, b, preferred_element_type=F32)


def mm_nt(a, b):
    return lax.dot_general(a, b, (((1,), (1,)), ((), ())), preferred_element_type=F32)


def mm_tn(a, b):
    return lax.dot_general(a, b, (((0,), (0,)), ((), ())), preferred_element_type=F32)


def turned_span(place, turn):
    return (turn + jnp.where(place == 0, 2, jnp.where(place == 3, 1, jnp.where(place == 2, 3, 0)))) & 3


def states_kernel(
    _, __, wk_ref, wv_ref, nk_ref, nv_ref, wd_ref, nd_ref, inside_ref, start_ref, *refs, staged,
):
    sources, refs = refs[:staged], refs[staged:]
    before_ref, earlier_ref, message_ref = refs[:3]
    targets, refs = refs[3 : 3 + staged], refs[3 + staged :]
    rows_ref, state_ref, decay_ref, sems = refs
    span = pl.program_id(0)
    copies = [pltpu.make_async_copy(a, b, sems.at[k]) for k, (a, b) in enumerate(zip(sources, targets))]

    @pl.when(span == 0)
    def _():
        for copy in copies:
            copy.start()
        state_ref[...] = jnp.zeros_like(state_ref)
        decay_ref[...] = jnp.zeros_like(decay_ref)

    total = running_decay(wd_ref, nd_ref, rows_ref)
    last = total[:, SPAN - 1 : SPAN]
    tail = jnp.exp(last - total).T
    kept = jnp.exp(last)
    before_ref[0] = state_ref[...]
    earlier_ref[0] = decay_ref[...]
    tables = span_tables(inside_ref, start_ref, span, 0)
    for head in range(3):
        cut = slice(head * 128, head * 128 + 128)
        keys = rotated_wide(wk_ref[:, cut], tables) * WIDE_SCALE
        scaled = (keys * tail[:, head : head + 1]).astype(BF16)
        state_ref[cut, :] = state_ref[cut, :] * kept[head : head + 1, :] + mm_tn(scaled, wv_ref[:, cut])
    tables = span_tables(inside_ref, start_ref, span, 1)
    keys = rotated_narrow(nk_ref[...], tables) * NARROW_SCALE
    tails = jnp.where(low_lanes((SPAN, LANES)), tail[:, 3:4], tail[:, 4:5])
    own = mm_tn((keys * tails).astype(BF16), nv_ref[...])
    square = (LANES, LANES)
    own = jnp.where(low_rows(square) == low_lanes(square), own, 0.0)
    keeps = jnp.where(low_rows(square), kept[3:4, :], kept[4:5, :])
    state_ref[384:512, :] = state_ref[384:512, :] * keeps + own
    decay_ref[...] += jnp.broadcast_to(last, decay_ref.shape)

    @pl.when(span == SPANS - 1)
    def _():
        sums = decay_ref[...]
        high = sums.astype(BF16).astype(F32)
        low = sums - high
        sub = lax.broadcasted_iota(jnp.int32, (8, LANES), 0)
        at = 0
        for head, count in enumerate((16, 16, 16, 8, 8)):
            pair = jnp.where(
                sub == 0,
                high[head : head + 1, :],
                jnp.where(sub == 1, low[head : head + 1, :], 0.0),
            )
            body = state_ref[at * 8 : (at + count) * 8, :].reshape(count, 8, LANES)
            ends = jnp.broadcast_to(pair[None], (count, 8, LANES))
            message_ref[at : at + count] = jnp.concatenate([body, ends], axis=1).astype(BF16)
            at += count
        for copy in copies:
            copy.wait()


def prefix_kernel(message_ref, out_ref):
    devices = message_ref.shape[0]
    carried = jnp.zeros((8, LANES), F32)
    for k in range(devices):
        out_ref[k] = carried.astype(BF16)
        if k + 1 < devices:
            piece = message_ref[k].astype(F32)
            kept = jnp.exp(piece[8:9, :] + piece[9:10, :])
            carried = carried * kept + piece[0:8, :]


def gated(output, gate, scale):
    gate = gate.astype(F32)
    return (output * scale * (gate / (1.0 + jnp.exp(-gate)))).astype(BF16)


def finish_kernel(
    index_ref, turn_ref, wq_ref, wk_ref, wv_ref, wg_ref, nq_ref, nk_ref, nv_ref, ng_ref, wd_ref, nd_ref,
    inside_ref, start_ref, before_ref, earlier_ref, prefix_ref, wide_out_ref, narrow_out_ref,
    *out_refs, first,
):
    *out_refs, rows_ref, mixed_ref = out_refs
    span = turned_span(first + pl.program_id(0), turn_ref[0])
    total = running_decay(wd_ref, nd_ref, rows_ref)
    columns = total.T
    grown = jnp.exp(columns)
    earlier = jnp.exp(earlier_ref[0])
    square = (SPAN, SPAN)
    causal = lax.broadcasted_iota(jnp.int32, square, 0) >= lax.broadcasted_iota(jnp.int32, square, 1)

    def weights(scores, head):
        gaps = columns[:, head : head + 1] - total[head : head + 1, :]
        return (scores * jnp.exp(jnp.where(causal, gaps, -jnp.inf))).astype(BF16)

    tables = span_tables(inside_ref, start_ref, span, 0)
    for head in range(3):
        cut = slice(head * 128, head * 128 + 128)
        queries = rotated_wide(wq_ref[:, cut], tables).astype(BF16)
        keys = (rotated_wide(wk_ref[:, cut], tables) * WIDE_SCALE).astype(BF16)
        within = mm(weights(mm_nt(queries, keys), head), wv_ref[:, cut])
        entering = (
            prefix_ref[cut, :].astype(F32) * earlier[head : head + 1, :] + before_ref[0, cut, :]
        ).astype(BF16)
        output = within + mm(queries, entering) * grown[:, head : head + 1]
        scale = lax.rsqrt(jnp.mean(output * output, axis=-1, keepdims=True) + EPS)
        mixed_ref[:, cut] = gated(output, wg_ref[:, cut], scale)

    tables = span_tables(inside_ref, start_ref, span, 1)
    queries = rotated_narrow(nq_ref[...], tables).astype(BF16)
    keys = (rotated_narrow(nk_ref[...], tables) * NARROW_SCALE).astype(BF16)
    values = nv_ref[...]
    low = low_lanes(square)
    none = jnp.zeros_like(queries)
    within = jnp.where(
        low,
        mm(weights(mm_nt(jnp.where(low, queries, none), keys), 3), values),
        mm(weights(mm_nt(jnp.where(low, none, queries), keys), 4), values),
    )
    fades = jnp.where(low_rows(square), earlier[3:4, :], earlier[4:5, :])
    entering = (prefix_ref[384:512, :].astype(F32) * fades + before_ref[0, 384:512, :]).astype(BF16)
    output = within + mm(queries, entering) * jnp.where(low, grown[:, 3:4], grown[:, 4:5])
    squares = output * output
    left = jnp.sum(jnp.where(low, squares, 0.0), axis=-1, keepdims=True)
    right = jnp.sum(jnp.where(low, 0.0, squares), axis=-1, keepdims=True)
    scale = lax.rsqrt(jnp.where(low, left, right) * (1.0 / 64.0) + EPS)
    mixed_ref[:, 384:512] = gated(output, ng_ref[...], scale)

    projected = (
        mm(mixed_ref[:, 0:384], wide_out_ref[...]) + mm(mixed_ref[:, 384:512], narrow_out_ref[...])
    ).astype(BF16)
    if len(out_refs) == 2:
        half = SPAN // 2
        out_refs[0][...] = projected[:half]
        out_refs[1][...] = projected[half:]
    else:
        out_refs[0][0] = projected


def join_kernel(minus_ref, plus_ref, from_below_ref, from_above_ref, minus_out_ref, plus_out_ref):
    part = pl.program_id(0)

    @pl.when(part == 0)
    def _():
        minus_out_ref[...] = minus_ref[...]
        plus_out_ref[...] = (plus_ref[...].astype(F32) + from_below_ref[...].astype(F32)).astype(BF16)

    @pl.when(part == 1)
    def _():
        minus_out_ref[...] = (minus_ref[...].astype(F32) + from_above_ref[...].astype(F32)).astype(BF16)
        plus_out_ref[...] = plus_ref[...]


def rms(values, gain):
    return values * lax.rsqrt(jnp.mean(values * values, axis=-1, keepdims=True) + EPS) * gain


def norms_kernel(
    own_ref, below_ref, above_ref, residual_ref, mix_ref, pre_ref, updated_ref, low_ref, high_ref
):
    projected = own_ref[...].astype(F32) + below_ref[...].astype(F32) + above_ref[...].astype(F32)
    updated = (residual_ref[...].astype(F32) + rms(projected, mix_ref[...])).astype(BF16)
    updated_ref[...] = updated
    normed = rms(updated.astype(F32), pre_ref[...]).astype(BF16)

    @pl.when(pl.program_id(0) == 0)
    def _():
        low_ref[...] = normed

    @pl.when(pl.program_id(0) == 1)
    def _():
        high_ref[...] = normed


def result_kernel(own_ref, below_ref, above_ref, updated_ref, gain_ref, out_ref):
    lowered = own_ref[...].astype(F32) + below_ref[...].astype(F32) + above_ref[...].astype(F32)
    out_ref[...] = (updated_ref[...].astype(F32) + rms(lowered.T, gain_ref[...])).astype(BF16)


def far_mixer_kernel(*refs, ups, downs):
    halves, refs = refs[:8], refs[8:]
    both_ref, hidden_ref, out_ref, low_ref, high_ref, down_ref, up_ref, x_ref, now_ref, sems = refs
    devices, share, units = up_ref.shape
    half = halves[0].shape[0]
    rows = 2 * half
    block = units // ups
    group = devices // downs
    lines = group * share

    def up_copy(k):
        at = pl.multiple_of(k * block, block)
        return pltpu.make_async_copy(
            both_ref.at[:, 0, :, pl.ds(at, block)], up_ref.at[:, :, pl.ds(at, block)], sems.at[k]
        )

    def down_copy(k):
        at = k * group
        return pltpu.make_async_copy(
            both_ref.at[pl.ds(at, group), 1], down_ref.at[pl.ds(at, group)], sems.at[ups + k]
        )

    for k in range(ups):
        up_copy(k).start()
    for k in range(downs):
        down_copy(k).start()
    for k, ref in enumerate(halves):
        x_ref[k * half : (k + 1) * half] = ref[...]

    @pl.loop(0, ups)
    def _(k):
        up_copy(k).wait()
        at = pl.multiple_of(k * block, block)
        weight = up_ref[:, :, pl.ds(at, block)].reshape(devices * share, block)
        rectified = jnp.maximum(mm(x_ref[...], weight), 0.0)
        hidden = (rectified * rectified).astype(BF16).T
        hidden_ref[pl.ds(at, block), :] = hidden[:, 2 * rows :]
        now_ref[pl.ds(at, block), :] = hidden[:, : 2 * rows]

    def lower(k, far_ref, base):
        down_copy(k).wait()
        weight = down_ref[pl.ds(k * group, group)].reshape(lines, units)
        lowered = mm(weight, now_ref[...]).astype(BF16)
        out_ref[pl.ds(pl.multiple_of(k * lines, lines), lines), :] = lowered[:, :rows]
        far_ref[pl.ds(pl.multiple_of((k - base) * lines, lines), lines), :] = lowered[:, rows:]

    @pl.loop(0, downs // 2)
    def _(k):
        lower(k, low_ref, 0)

    @pl.loop(downs // 2, downs)
    def _(k):
        lower(k, high_ref, downs // 2)


def near_mixer_kernel(hidden_ref, down_ref, minus_ref, plus_ref, *, parts):
    devices, share, units = down_ref.shape
    group = devices // parts
    lines = group * share
    rows = minus_ref.shape[1]

    @pl.loop(0, parts)
    def _(k):
        weight = down_ref[pl.ds(k * group, group)].reshape(lines, units)
        lowered = mm(weight, hidden_ref[...]).astype(BF16)
        at = pl.multiple_of(k * lines, lines)
        minus_ref[pl.ds(at, lines), :] = lowered[:, :rows]
        plus_ref[pl.ds(at, lines), :] = lowered[:, rows:]


SMALL = pltpu.CompilerParams(vmem_limit_bytes=16 * 1024 * 1024)
LARGE = pltpu.CompilerParams(vmem_limit_bytes=32 * 1024 * 1024)


def shifted(array, axis, by):
    size = lax.axis_size(axis)
    return lax.ppermute(array, axis, [(k, (k + by) % size) for k in range(size)])


def joined(minus, plus, from_below, from_above, picks=(None, None)):
    half, width = from_below.shape
    flat = pl.BlockSpec((half, width), lambda i: (i, 0))
    kept = pl.BlockSpec((half, width), lambda i: (0, 0))
    out = jax.ShapeDtypeStruct((2 * half, width), BF16)

    def source(pick):
        if pick is None:
            return flat
        return pl.BlockSpec((None, half, width), lambda i: (pick, i, 0))

    return pl.pallas_call(
        join_kernel,
        out_shape=(out, out),
        grid=(2,),
        in_specs=[source(picks[0]), source(picks[1]), kept, kept],
        out_specs=[flat, flat],
        compiler_params=SMALL,
        name="join",
        cost_estimate=pl.CostEstimate(flops=1_000_000, bytes_accessed=3_500_000, transcendentals=0),
    )(minus, plus, from_below, from_above)


def local(
    wide_query, wide_key, wide_value, wide_gate,
    narrow_query, narrow_key, narrow_value, narrow_gate,
    wide_decay, narrow_decay, residual, wide_out, narrow_out,
    up_weight, down_weight, gain_mix, gain_pre, gain_mlp,
):
    devices = lax.axis_size(SP)
    ranks = lax.axis_size("tp")
    length, width = wide_query.shape[0], residual.shape[1]
    rows = residual.shape[0]
    share = up_weight.shape[0]
    units = up_weight.shape[1]

    both = lax.all_gather(
        jnp.concatenate([up_weight, down_weight.T], axis=0), SP, axis=0, tiled=True
    ).reshape(devices, 2, share, units)

    inside, starts = (jnp.asarray(t) for t in position_tables(devices))
    scalars = [
        lax.axis_index(SP).astype(jnp.int32).reshape(1),
        lax.axis_index("tp").astype(jnp.int32).reshape(1),
    ]
    table_blocks = [
        pl.BlockSpec((4, SPAN, LANES), lambda s, i, t: (0, 0, 0)),
        pl.BlockSpec((1, 4 * SPANS, LANES), lambda s, i, t: (i[0], 0, 0)),
    ]

    def span_blocks(at):
        return (
            pl.BlockSpec((SPAN, 384), lambda s, i, t: (at(s, i, t), 0)),
            pl.BlockSpec((SPAN, 128), lambda s, i, t: (at(s, i, t), 0)),
            [
                pl.BlockSpec((3, SPAN), lambda s, i, t: (0, at(s, i, t))),
                pl.BlockSpec((2, SPAN), lambda s, i, t: (0, at(s, i, t))),
            ],
            [
                pl.BlockSpec((1, 512, LANES), lambda s, i, t: (at(s, i, t), 0, 0)),
                pl.BlockSpec((1, 8, LANES), lambda s, i, t: (at(s, i, t), 0, 0)),
            ],
        )

    wide_block, narrow_block, decay_blocks, state_blocks = span_blocks(lambda s, i, t: s)
    staged = (wide_gate, narrow_query, narrow_value, narrow_gate, narrow_out)
    before, earlier, message, *held = pl.pallas_call(
        functools.partial(states_kernel, staged=len(staged)),
        out_shape=(
            jax.ShapeDtypeStruct((SPANS, 512, LANES), F32),
            jax.ShapeDtypeStruct((SPANS, 8, LANES), F32),
            jax.ShapeDtypeStruct((devices, 16, LANES), BF16),
            *(pltpu.VMEM(x.shape, x.dtype) for x in staged),
        ),
        grid_spec=pltpu.PrefetchScalarGridSpec(
            num_scalar_prefetch=2,
            grid=(SPANS,),
            in_specs=[
                wide_block, wide_block, narrow_block, narrow_block, *decay_blocks, *table_blocks,
                *([pl.BlockSpec(memory_space=pltpu.HBM)] * len(staged)),
            ],
            out_specs=[
                *state_blocks,
                pl.BlockSpec((devices, 16, LANES), lambda s, i, t: (0, 0, 0)),
                *([pl.BlockSpec(memory_space=pltpu.VMEM)] * len(staged)),
            ],
            scratch_shapes=[
                pltpu.VMEM((8, LANES), F32),
                pltpu.VMEM((512, LANES), F32),
                pltpu.VMEM((8, LANES), F32),
                pltpu.SemaphoreType.DMA((len(staged),)),
            ],
        ),
        compiler_params=SMALL,
        name="states",
        cost_estimate=pl.CostEstimate(flops=60_000_000, bytes_accessed=2_500_000, transcendentals=20_000),
    )(
        *scalars,
        *(
            pltpu.with_memory_space_constraint(x, pltpu.HBM)
            for x in (
                wide_key, wide_value, narrow_key, narrow_value,
                wide_decay, narrow_decay, inside, starts, *staged,
            )
        ),
    )
    gate_held, query_held, value_held, narrow_gate_held, out_held = held

    arrived = lax.all_to_all(message, SP, 0, 0, tiled=True)
    prefixes = pl.pallas_call(
        prefix_kernel,
        out_shape=jax.ShapeDtypeStruct((devices, 8, LANES), BF16),
        compiler_params=SMALL,
        name="prefix",
        cost_estimate=pl.CostEstimate(flops=2_000_000, bytes_accessed=400_000, transcendentals=8_000),
    )(arrived)
    prefix = lax.all_to_all(prefixes, SP, 0, 0, tiled=True).reshape(512, LANES)

    def finish(first, count, out_shape, out_specs):
        wide, narrow, decays, states = span_blocks(lambda s, i, t: turned_span(first + s, t[0]))
        return pl.pallas_call(
            functools.partial(finish_kernel, first=first),
            out_shape=out_shape,
            grid_spec=pltpu.PrefetchScalarGridSpec(
                num_scalar_prefetch=2,
                grid=(count,),
                in_specs=[
                    wide, wide, wide, wide, narrow, narrow, narrow, narrow,
                    *decays, *table_blocks, *states,
                    pl.BlockSpec((512, LANES), lambda s, i, t: (0, 0)),
                    pl.BlockSpec((384, width), lambda s, i, t: (0, 0)),
                    pl.BlockSpec((128, width), lambda s, i, t: (0, 0)),
                ],
                out_specs=out_specs,
                scratch_shapes=[pltpu.VMEM((8, LANES), F32), pltpu.VMEM((SPAN, 512), BF16)],
            ),
            compiler_params=SMALL,
            name="finish" if first else "finish_far",
            cost_estimate=pl.CostEstimate(
                flops=350_000_000 * count,
                bytes_accessed=3_000_000 + 1_500_000 * count,
                transcendentals=150_000 * count,
            ),
        )(
            *scalars, wide_query, wide_key, wide_value, gate_held,
            query_held, narrow_key, value_held, narrow_gate_held,
            wide_decay, narrow_decay, inside, starts, before, earlier, prefix, wide_out, out_held,
        )

    half = rows // 2
    half_out = jax.ShapeDtypeStruct((half, width), BF16)
    near_out = jax.ShapeDtypeStruct((3, rows, width), BF16)
    low, high = finish(
        0, 1, (half_out, half_out), [pl.BlockSpec((half, width), lambda s, i, t: (0, 0))] * 2
    )
    low, high = shifted(low, "tp", 1), shifted(high, "tp", -1)
    (near,) = finish(
        1, 3, (near_out,), [pl.BlockSpec((1, rows, width), lambda s, i, t: (s, 0, 0))]
    )
    minus, plus = joined(near, near, low, high, (1, 2))
    below, above = shifted(plus, "tp", 1), shifted(minus, "tp", -1)
    flat = pl.BlockSpec((half, width), lambda i: (i, 0))
    kept = pl.BlockSpec((half, width), lambda i: (0, 0))
    gain = pl.BlockSpec((1, width), lambda i: (0, 0))
    updated, low, high = pl.pallas_call(
        norms_kernel,
        out_shape=[jax.ShapeDtypeStruct((rows, width), BF16), half_out, half_out],
        grid=(2,),
        in_specs=[
            pl.BlockSpec((None, half, width), lambda i: (0, i, 0)), flat, flat, flat, gain, gain,
        ],
        out_specs=[flat, kept, kept],
        compiler_params=SMALL,
        name="norms",
        cost_estimate=pl.CostEstimate(flops=4_000_000, bytes_accessed=3_500_000, transcendentals=300),
    )(near, below, above, residual, gain_mix.reshape(1, width), gain_pre.reshape(1, width))
    below_low, above_high = shifted(low, "tp", 1), shifted(high, "tp", -1)
    below_high, above_low = shifted(high, "tp", 1), shifted(low, "tp", -1)
    far_low, far_high = shifted(below_low, "tp", 1), shifted(above_high, "tp", -1)

    ups, downs = 4, 4
    whole = pl.BlockSpec(memory_space=pltpu.VMEM)
    turned_half = pltpu.VMEM((width // 2, rows), BF16)
    hidden, own, low, high, down = pl.pallas_call(
        functools.partial(far_mixer_kernel, ups=ups, downs=downs),
        out_shape=(
            pltpu.VMEM((units, 2 * rows), BF16),
            pltpu.VMEM((width, rows), BF16),
            turned_half,
            turned_half,
            pltpu.VMEM((devices, share, units), BF16),
        ),
        in_specs=[*([whole] * 8), pl.BlockSpec(memory_space=pltpu.HBM)],
        out_specs=[whole] * 5,
        scratch_shapes=[
            pltpu.VMEM((devices, share, units), BF16),
            pltpu.VMEM((4 * rows, width), BF16),
            pltpu.VMEM((units, 2 * rows), BF16),
            pltpu.SemaphoreType.DMA((ups + downs,)),
        ],
        compiler_params=LARGE,
        name="mixer_far",
        cost_estimate=pl.CostEstimate(
            flops=12 * rows * width * units, bytes_accessed=20_000_000, transcendentals=0
        ),
    )(low, high, far_low, far_high, below_low, below_high, above_low, above_high, both)
    low, high = shifted(low, "tp", 1), shifted(high, "tp", -1)
    minus, plus = pl.pallas_call(
        functools.partial(near_mixer_kernel, parts=2),
        out_shape=(jax.ShapeDtypeStruct((width, rows), BF16),) * 2,
        in_specs=[whole] * 2,
        out_specs=[whole] * 2,
        compiler_params=SMALL,
        name="mixer_near",
        cost_estimate=pl.CostEstimate(
            flops=4 * rows * width * units, bytes_accessed=2_000_000, transcendentals=0
        ),
    )(hidden, down)
    minus, plus = joined(minus, plus, low, high)
    below, above = shifted(plus, "tp", 1), shifted(minus, "tp", -1)
    return pl.pallas_call(
        result_kernel,
        out_shape=jax.ShapeDtypeStruct((rows, width), BF16),
        compiler_params=SMALL,
        name="result",
        cost_estimate=pl.CostEstimate(flops=4_000_000, bytes_accessed=3_500_000, transcendentals=300),
    )(own, below, above, updated, gain_mlp.reshape(1, width))


def solution(mesh):
    finer = Mesh(mesh.devices.reshape(8, 4, 2, mesh.shape["tp"]), ("sp_0", "sp_1", "sp_2", "tp"))
    in_specs = (
        *([P(SP, "tp")] * 8),
        P("tp", SP),
        P("tp", SP),
        P(SP_TP, None),
        P("tp", None),
        P("tp", None),
        P(SP, "tp"),
        P("tp", SP),
        P(),
        P(),
        P(),
    )
    return jax.shard_map(
        local, mesh=finer, in_specs=in_specs, out_specs=P(SP_TP, None), check_vma=False
    )
```

```python
import functools

import jax
import jax.numpy as jnp
import numpy as np
from jax import lax
from jax.experimental import pallas as pl
from jax.experimental.pallas import tpu as pltpu
from jax.sharding import Mesh
from jax.sharding import PartitionSpec as P

SPAN = 128
LANES = 128
SPANS = 4
SP = ("sp_0", "sp_1", "sp_2")
SP_TP = ("sp_0", "sp_1", "sp_2", "tp")
EPS = 1e-06
WIDE_SCALE = 128 ** (-0.5)
NARROW_SCALE = 64 ** (-0.5)
F32 = jnp.float32
BF16 = jnp.bfloat16


def position_tables(devices):
    lane = np.arange(LANES)

    def inverse(head_dim):
        half = head_dim // 2
        return 10000.0 ** (-2.0 * (lane % half) / head_dim), np.where(
            lane % head_dim < half, -1.0, 1.0
        )

    row = np.arange(SPAN)[:, None]
    first = (np.arange(devices * SPANS) * SPAN)[:, None]
    inside, starts = [], []
    for head_dim in (128, 64):
        rate, sign = inverse(head_dim)
        inside += [np.cos(row * rate), np.sin(row * rate) * sign]
        starts += [
            np.cos(first * rate).reshape(devices, SPANS, LANES),
            (np.sin(first * rate) * sign).reshape(devices, SPANS, LANES),
        ]
    return (
        np.stack(inside).astype(np.float32),
        np.concatenate(starts, axis=1).astype(np.float32),
    )


def span_tables(inside_ref, start_ref, span, group):
    cos_row, sin_row = inside_ref[2 * group], inside_ref[2 * group + 1]
    cos_start = start_ref[0, pl.ds(2 * group * SPANS + span, 1), :]
    sin_start = start_ref[0, pl.ds((2 * group + 1) * SPANS + span, 1), :]
    return (
        cos_row * cos_start - sin_row * sin_start,
        sin_row * cos_start + cos_row * sin_start,
    )


def rotated_wide(x, tables):
    x = x.astype(F32)
    return x * tables[0] + pltpu.roll(x, 64, 1) * tables[1]


def rotated_narrow(x, tables):
    x = x.astype(F32)
    lane = lax.broadcasted_iota(jnp.int32, x.shape, 1)
    partner = jnp.where((lane & 32) == 0, pltpu.roll(x, 96, 1), pltpu.roll(x, 32, 1))
    return x * tables[0] + partner * tables[1]


def running_decay(wide_decay_ref, narrow_decay_ref, rows_ref):
    rows_ref[...] = jnp.zeros_like(rows_ref)
    rows_ref[0:3, :] = wide_decay_ref[...]
    rows_ref[3:5, :] = narrow_decay_ref[...]
    x = rows_ref[...]
    lane = lax.broadcasted_iota(jnp.int32, x.shape, 1)
    step = 1
    while step < SPAN:
        x = x + jnp.where(lane >= step, pltpu.roll(x, step, 1), 0.0)
        step *= 2
    return x


def low_rows(shape):
    return lax.broadcasted_iota(jnp.int32, shape, 0) < 64


def low_lanes(shape):
    return lax.broadcasted_iota(jnp.int32, shape, 1) < 64


def mm(a, b):
    return jnp.dot(a, b, preferred_element_type=F32)


def mm_nt(a, b):
    return lax.dot_general(a, b, (((1,), (1,)), ((), ())), preferred_element_type=F32)


def mm_tn(a, b):
    return lax.dot_general(a, b, (((0,), (0,)), ((), ())), preferred_element_type=F32)


def turned_span(place, turn):
    return (turn + jnp.where(place == 0, 2, jnp.where(place == 3, 1, jnp.where(place == 2, 3, 0)))) & 3


def states_kernel(
    index_ref, _, wk_ref, wv_ref, nk_ref, nv_ref, wd_ref, nd_ref, inside_ref, start_ref, *refs, staged,
):
    sources, refs = refs[:staged], refs[staged:]
    before_ref, earlier_ref, message_ref = refs[:3]
    targets, refs = refs[3 : 3 + staged], refs[3 + staged :]
    rows_ref, state_ref, decay_ref, sems = refs
    span = pl.program_id(0)
    copies = [
        pltpu.make_async_copy(a.at[pl.ds(index_ref[0], 1)] if k == 0 else a, b, sems.at[k])
        for k, (a, b) in enumerate(zip(sources, targets))
    ]

    @pl.when(span == 0)
    def _():
        for copy in copies:
            copy.start()
        state_ref[...] = jnp.zeros_like(state_ref)
        decay_ref[...] = jnp.zeros_like(decay_ref)

    total = running_decay(wd_ref, nd_ref, rows_ref)
    last = total[:, SPAN - 1 : SPAN]
    tail = jnp.exp(last - total).T
    kept = jnp.exp(last)
    before_ref[0] = state_ref[...]
    earlier_ref[0] = decay_ref[...]
    tables = span_tables(inside_ref, start_ref, span, 0)
    for head in range(3):
        cut = slice(head * 128, head * 128 + 128)
        keys = rotated_wide(wk_ref[:, cut], tables) * WIDE_SCALE
        scaled = (keys * tail[:, head : head + 1]).astype(BF16)
        state_ref[cut, :] = state_ref[cut, :] * kept[head : head + 1, :] + mm_tn(scaled, wv_ref[:, cut])
    tables = span_tables(inside_ref, start_ref, span, 1)
    keys = rotated_narrow(nk_ref[...], tables) * NARROW_SCALE
    tails = jnp.where(low_lanes((SPAN, LANES)), tail[:, 3:4], tail[:, 4:5])
    own = mm_tn((keys * tails).astype(BF16), nv_ref[...])
    square = (LANES, LANES)
    own = jnp.where(low_rows(square) == low_lanes(square), own, 0.0)
    keeps = jnp.where(low_rows(square), kept[3:4, :], kept[4:5, :])
    state_ref[384:512, :] = state_ref[384:512, :] * keeps + own
    decay_ref[...] += jnp.broadcast_to(last, decay_ref.shape)

    @pl.when(span == SPANS - 1)
    def _():
        sums = decay_ref[...]
        high = sums.astype(BF16).astype(F32)
        low = sums - high
        sub = lax.broadcasted_iota(jnp.int32, (8, LANES), 0)
        at = 0
        for head, count in enumerate((16, 16, 16, 8, 8)):
            pair = jnp.where(
                sub == 0,
                high[head : head + 1, :],
                jnp.where(sub == 1, low[head : head + 1, :], 0.0),
            )
            body = state_ref[at * 8 : (at + count) * 8, :].reshape(count, 8, LANES)
            ends = jnp.broadcast_to(pair[None], (count, 8, LANES))
            message_ref[at : at + count] = jnp.concatenate([body, ends], axis=1).astype(BF16)
            at += count
        for copy in copies:
            copy.wait()


def prefix_kernel(message_ref, out_ref):
    devices = message_ref.shape[0]
    carried = jnp.zeros((8, LANES), F32)
    for k in range(devices):
        out_ref[k] = carried.astype(BF16)
        if k + 1 < devices:
            piece = message_ref[k].astype(F32)
            kept = jnp.exp(piece[8:9, :] + piece[9:10, :])
            carried = carried * kept + piece[0:8, :]


def gated(output, gate, scale):
    gate = gate.astype(F32)
    return (output * scale * (gate / (1.0 + jnp.exp(-gate)))).astype(BF16)


def finish_kernel(
    index_ref, turn_ref, wq_ref, wk_ref, wv_ref, wg_ref, nq_ref, nk_ref, nv_ref, ng_ref, wd_ref, nd_ref,
    inside_ref, start_ref, before_ref, earlier_ref, prefix_ref, wide_out_ref, narrow_out_ref,
    *out_refs, first,
):
    *out_refs, rows_ref, mixed_ref = out_refs
    span = turned_span(first + pl.program_id(0), turn_ref[0])
    total = running_decay(wd_ref, nd_ref, rows_ref)
    columns = total.T
    grown = jnp.exp(columns)
    earlier = jnp.exp(earlier_ref[0])
    square = (SPAN, SPAN)
    causal = lax.broadcasted_iota(jnp.int32, square, 0) >= lax.broadcasted_iota(jnp.int32, square, 1)

    def weights(scores, head):
        gaps = columns[:, head : head + 1] - total[head : head + 1, :]
        return (scores * jnp.exp(jnp.where(causal, gaps, -jnp.inf))).astype(BF16)

    tables = span_tables(inside_ref, start_ref, span, 0)
    for head in range(3):
        cut = slice(head * 128, head * 128 + 128)
        queries = rotated_wide(wq_ref[:, cut], tables).astype(BF16)
        keys = (rotated_wide(wk_ref[:, cut], tables) * WIDE_SCALE).astype(BF16)
        within = mm(weights(mm_nt(queries, keys), head), wv_ref[:, cut])
        entering = (
            prefix_ref[cut, :].astype(F32) * earlier[head : head + 1, :] + before_ref[0, cut, :]
        ).astype(BF16)
        output = within + mm(queries, entering) * grown[:, head : head + 1]
        scale = lax.rsqrt(jnp.mean(output * output, axis=-1, keepdims=True) + EPS)
        mixed_ref[:, cut] = gated(output, wg_ref[:, cut], scale)

    tables = span_tables(inside_ref, start_ref, span, 1)
    queries = rotated_narrow(nq_ref[...], tables).astype(BF16)
    keys = (rotated_narrow(nk_ref[...], tables) * NARROW_SCALE).astype(BF16)
    values = nv_ref[...]
    low = low_lanes(square)
    none = jnp.zeros_like(queries)
    within = jnp.where(
        low,
        mm(weights(mm_nt(jnp.where(low, queries, none), keys), 3), values),
        mm(weights(mm_nt(jnp.where(low, none, queries), keys), 4), values),
    )
    fades = jnp.where(low_rows(square), earlier[3:4, :], earlier[4:5, :])
    entering = (prefix_ref[384:512, :].astype(F32) * fades + before_ref[0, 384:512, :]).astype(BF16)
    output = within + mm(queries, entering) * jnp.where(low, grown[:, 3:4], grown[:, 4:5])
    squares = output * output
    left = jnp.sum(jnp.where(low, squares, 0.0), axis=-1, keepdims=True)
    right = jnp.sum(jnp.where(low, 0.0, squares), axis=-1, keepdims=True)
    scale = lax.rsqrt(jnp.where(low, left, right) * (1.0 / 64.0) + EPS)
    mixed_ref[:, 384:512] = gated(output, ng_ref[...], scale)

    projected = (
        mm(mixed_ref[:, 0:384], wide_out_ref[...]) + mm(mixed_ref[:, 384:512], narrow_out_ref[...])
    ).astype(BF16)
    if len(out_refs) == 2:
        half = SPAN // 2
        out_refs[0][...] = projected[:half]
        out_refs[1][...] = projected[half:]
    else:
        out_refs[0][0] = projected


def join_kernel(minus_ref, plus_ref, from_below_ref, from_above_ref, minus_out_ref, plus_out_ref):
    part = pl.program_id(0)

    @pl.when(part == 0)
    def _():
        minus_out_ref[...] = minus_ref[...]
        plus_out_ref[...] = (plus_ref[...].astype(F32) + from_below_ref[...].astype(F32)).astype(BF16)

    @pl.when(part == 1)
    def _():
        minus_out_ref[...] = (minus_ref[...].astype(F32) + from_above_ref[...].astype(F32)).astype(BF16)
        plus_out_ref[...] = plus_ref[...]


def rms(values, gain):
    return values * lax.rsqrt(jnp.mean(values * values, axis=-1, keepdims=True) + EPS) * gain


def norms_kernel(
    own_ref, below_ref, above_ref, residual_ref, mix_ref, pre_ref, updated_ref, low_ref, high_ref
):
    projected = own_ref[...].astype(F32) + below_ref[...].astype(F32) + above_ref[...].astype(F32)
    updated = (residual_ref[...].astype(F32) + rms(projected, mix_ref[...])).astype(BF16)
    updated_ref[...] = updated
    normed = rms(updated.astype(F32), pre_ref[...]).astype(BF16)

    @pl.when(pl.program_id(0) == 0)
    def _():
        low_ref[...] = normed

    @pl.when(pl.program_id(0) == 1)
    def _():
        high_ref[...] = normed


def tail_join_kernel(plus_ref, minus_ref, from_below_ref, from_above_ref, plus_out_ref, minus_out_ref):
    plus_out_ref[...] = (plus_ref[...].astype(F32) + from_below_ref[...].astype(F32)).astype(BF16)
    minus_out_ref[...] = (minus_ref[...].astype(F32) + from_above_ref[...].astype(F32)).astype(BF16)


def result_kernel(
    own_ref, below_low_ref, below_high_ref, above_low_ref, above_high_ref,
    updated_ref, gain_ref, out_ref,
):
    half = below_low_ref.shape[0]
    lowered = [
        own_ref[part].astype(F32) + below[...].astype(F32) + above[...].astype(F32)
        for part, below, above in (
            (slice(0, half), below_low_ref, above_low_ref),
            (slice(half, 2 * half), below_high_ref, above_high_ref),
        )
    ]
    lowered = jnp.concatenate(lowered, axis=0).T
    out_ref[...] = (updated_ref[...].astype(F32) + rms(lowered, gain_ref[...])).astype(BF16)


def up_block(x_ref, up_ref, at, block):
    weight = up_ref[:, :, pl.ds(at, block)].reshape(-1, block)
    rectified = jnp.maximum(mm(x_ref[...], weight), 0.0)
    return (rectified * rectified).astype(BF16).T


def down_block(down_ref, hidden_ref, k, group):
    weight = down_ref[pl.ds(k * group, group)].reshape(-1, hidden_ref.shape[0])
    return mm(weight, hidden_ref[...]).astype(BF16)


def far_mixer_kernel(*refs, ups, downs):
    halves, refs = refs[:4], refs[4:]
    both_ref, up_ref, down_ref, out_ref, low_ref, high_ref, x_ref, hidden_ref, sems = refs
    devices, share, units = up_ref.shape
    half = halves[0].shape[0]
    rows = 2 * half
    block = units // ups
    group = devices // downs
    lines = group * share

    def up_copy(k):
        at = pl.multiple_of(k * block, block)
        return pltpu.make_async_copy(
            both_ref.at[:, 0, :, pl.ds(at, block)], up_ref.at[:, :, pl.ds(at, block)], sems.at[k]
        )

    def down_copy(k):
        at = k * group
        return pltpu.make_async_copy(
            both_ref.at[pl.ds(at, group), 1], down_ref.at[pl.ds(at, group)], sems.at[ups + k]
        )

    for k in range(ups):
        up_copy(k).start()
    for k in range(downs):
        down_copy(k).start()
    for k, ref in enumerate(halves):
        x_ref[k * half : (k + 1) * half] = ref[...]

    @pl.loop(0, ups)
    def _(k):
        up_copy(k).wait()
        at = pl.multiple_of(k * block, block)
        hidden_ref[pl.ds(at, block), :] = up_block(x_ref, up_ref, at, block)

    def lower(k, far_ref, base):
        down_copy(k).wait()
        lowered = down_block(down_ref, hidden_ref, k, group)
        out_ref[pl.ds(pl.multiple_of(k * lines, lines), lines), :] = lowered[:, :rows]
        far_ref[pl.ds(pl.multiple_of((k - base) * lines, lines), lines), :] = lowered[:, rows:]

    @pl.loop(0, downs // 2)
    def _(k):
        lower(k, low_ref, 0)

    @pl.loop(downs // 2, downs)
    def _(k):
        lower(k, high_ref, downs // 2)


def near_mixer_kernel(*refs, ups, downs):
    halves, refs = refs[:4], refs[4:]
    up_ref, down_ref, minus_low_ref, minus_high_ref, plus_low_ref, plus_high_ref, x_ref, hidden_ref = refs
    devices, share, units = up_ref.shape
    half = halves[0].shape[0]
    rows = 2 * half
    block = units // ups
    group = devices // downs
    lines = group * share
    for k, ref in enumerate(halves):
        x_ref[k * half : (k + 1) * half] = ref[...]

    @pl.loop(0, ups)
    def _(k):
        at = pl.multiple_of(k * block, block)
        hidden_ref[pl.ds(at, block), :] = up_block(x_ref, up_ref, at, block)

    for first, minus_ref, plus_ref in (
        (0, minus_low_ref, plus_low_ref), (downs // 2, minus_high_ref, plus_high_ref)
    ):
        for k in range(downs // 2):
            lowered = down_block(down_ref, hidden_ref, first + k, group)
            at = slice(k * lines, (k + 1) * lines)
            minus_ref[at, :] = lowered[:, :rows]
            plus_ref[at, :] = lowered[:, rows:]


SMALL = pltpu.CompilerParams(vmem_limit_bytes=16 * 1024 * 1024)


def shifted(array, axis, by):
    size = lax.axis_size(axis)
    return lax.ppermute(array, axis, [(k, (k + by) % size) for k in range(size)])


def joined(minus, plus, from_below, from_above, picks=(None, None)):
    half, width = from_below.shape
    flat = pl.BlockSpec((half, width), lambda i: (i, 0))
    kept = pl.BlockSpec((half, width), lambda i: (0, 0))
    out = jax.ShapeDtypeStruct((2 * half, width), BF16)

    def source(pick):
        if pick is None:
            return flat
        return pl.BlockSpec((None, half, width), lambda i: (pick, i, 0))

    return pl.pallas_call(
        join_kernel,
        out_shape=(out, out),
        grid=(2,),
        in_specs=[source(picks[0]), source(picks[1]), kept, kept],
        out_specs=[flat, flat],
        compiler_params=SMALL,
        name="join",
        cost_estimate=pl.CostEstimate(flops=1_000_000, bytes_accessed=3_500_000, transcendentals=0),
    )(minus, plus, from_below, from_above)


def local(
    wide_query, wide_key, wide_value, wide_gate,
    narrow_query, narrow_key, narrow_value, narrow_gate,
    wide_decay, narrow_decay, residual, wide_out, narrow_out,
    up_weight, down_weight, gain_mix, gain_pre, gain_mlp,
):
    devices = lax.axis_size(SP)
    ranks = lax.axis_size("tp")
    length, width = wide_query.shape[0], residual.shape[1]
    rows = residual.shape[0]
    share = up_weight.shape[0]
    units = up_weight.shape[1]

    both = lax.all_gather(
        jnp.concatenate([up_weight, down_weight.T], axis=0), SP, axis=0, tiled=True
    ).reshape(devices, 2, share, units)

    inside, starts = (jnp.asarray(t) for t in position_tables(devices))
    scalars = [
        lax.axis_index(SP).astype(jnp.int32).reshape(1),
        lax.axis_index("tp").astype(jnp.int32).reshape(1),
    ]
    table_blocks = [
        pl.BlockSpec((4, SPAN, LANES), lambda s, i, t: (0, 0, 0)),
        pl.BlockSpec((1, 4 * SPANS, LANES), lambda s, i, t: (i[0], 0, 0)),
    ]

    def span_blocks(at):
        return (
            pl.BlockSpec((SPAN, 384), lambda s, i, t: (at(s, i, t), 0)),
            pl.BlockSpec((SPAN, 128), lambda s, i, t: (at(s, i, t), 0)),
            [
                pl.BlockSpec((3, SPAN), lambda s, i, t: (0, at(s, i, t))),
                pl.BlockSpec((2, SPAN), lambda s, i, t: (0, at(s, i, t))),
            ],
            [
                pl.BlockSpec((1, 512, LANES), lambda s, i, t: (at(s, i, t), 0, 0)),
                pl.BlockSpec((1, 8, LANES), lambda s, i, t: (at(s, i, t), 0, 0)),
            ],
        )

    wide_block, narrow_block, decay_blocks, state_blocks = span_blocks(lambda s, i, t: s)
    staged = (
        starts, inside, wide_decay, narrow_decay, wide_query, wide_key, wide_value, wide_gate,
        narrow_query, narrow_key, narrow_value, narrow_gate, wide_out, narrow_out,
    )
    before, earlier, message, *held = pl.pallas_call(
        functools.partial(states_kernel, staged=len(staged)),
        out_shape=(
            jax.ShapeDtypeStruct((SPANS, 512, LANES), F32),
            jax.ShapeDtypeStruct((SPANS, 8, LANES), F32),
            jax.ShapeDtypeStruct((devices, 16, LANES), BF16),
            pltpu.VMEM((1, *starts.shape[1:]), F32),
            *(pltpu.VMEM(x.shape, x.dtype) for x in staged[1:]),
        ),
        grid_spec=pltpu.PrefetchScalarGridSpec(
            num_scalar_prefetch=2,
            grid=(SPANS,),
            in_specs=[
                wide_block, wide_block, narrow_block, narrow_block, *decay_blocks, *table_blocks,
                *([pl.BlockSpec(memory_space=pltpu.HBM)] * len(staged)),
            ],
            out_specs=[
                *state_blocks,
                pl.BlockSpec((devices, 16, LANES), lambda s, i, t: (0, 0, 0)),
                *([pl.BlockSpec(memory_space=pltpu.VMEM)] * len(staged)),
            ],
            scratch_shapes=[
                pltpu.VMEM((8, LANES), F32),
                pltpu.VMEM((512, LANES), F32),
                pltpu.VMEM((8, LANES), F32),
                pltpu.SemaphoreType.DMA((len(staged),)),
            ],
        ),
        compiler_params=SMALL,
        name="states",
        cost_estimate=pl.CostEstimate(flops=60_000_000, bytes_accessed=2_500_000, transcendentals=20_000),
    )(
        *scalars,
        *(
            pltpu.with_memory_space_constraint(x, pltpu.HBM)
            for x in (
                wide_key, wide_value, narrow_key, narrow_value,
                wide_decay, narrow_decay, inside, starts, *staged,
            )
        ),
    )

    arrived = lax.all_to_all(message, SP, 0, 0, tiled=True)
    prefixes = pl.pallas_call(
        prefix_kernel,
        out_shape=jax.ShapeDtypeStruct((devices, 8, LANES), BF16),
        compiler_params=SMALL,
        name="prefix",
        cost_estimate=pl.CostEstimate(flops=2_000_000, bytes_accessed=400_000, transcendentals=8_000),
    )(arrived)
    prefix = lax.all_to_all(prefixes, SP, 0, 0, tiled=True).reshape(512, LANES)

    def finish(first, count, out_shape, out_specs):
        wide, narrow, decays, states = span_blocks(lambda s, i, t: turned_span(first + s, t[0]))
        return pl.pallas_call(
            functools.partial(finish_kernel, first=first),
            out_shape=out_shape,
            grid_spec=pltpu.PrefetchScalarGridSpec(
                num_scalar_prefetch=2,
                grid=(count,),
                in_specs=[
                    wide, wide, wide, wide, narrow, narrow, narrow, narrow,
                    *decays, table_blocks[0],
                    pl.BlockSpec((1, 4 * SPANS, LANES), lambda s, i, t: (0, 0, 0)), *states,
                    pl.BlockSpec((512, LANES), lambda s, i, t: (0, 0)),
                    pl.BlockSpec((384, width), lambda s, i, t: (0, 0)),
                    pl.BlockSpec((128, width), lambda s, i, t: (0, 0)),
                ],
                out_specs=out_specs,
                scratch_shapes=[pltpu.VMEM((8, LANES), F32), pltpu.VMEM((SPAN, 512), BF16)],
            ),
            compiler_params=SMALL,
            name="finish" if first else "finish_far",
            cost_estimate=pl.CostEstimate(
                flops=350_000_000 * count,
                bytes_accessed=3_000_000 + 1_500_000 * count,
                transcendentals=150_000 * count,
            ),
        )(
            *scalars, *held[4:12], held[2], held[3], held[1], held[0], before, earlier, prefix, *held[12:],
        )

    half = rows // 2
    half_out = jax.ShapeDtypeStruct((half, width), BF16)
    near_out = jax.ShapeDtypeStruct((3, rows, width), BF16)
    low, high = finish(
        0, 1, (half_out, half_out), [pl.BlockSpec((half, width), lambda s, i, t: (0, 0))] * 2
    )
    low, high = shifted(low, "tp", 1), shifted(high, "tp", -1)
    (near,) = finish(
        1, 3, (near_out,), [pl.BlockSpec((1, rows, width), lambda s, i, t: (s, 0, 0))]
    )
    minus, plus = joined(near, near, low, high, (1, 2))
    below, above = shifted(plus, "tp", 1), shifted(minus, "tp", -1)
    flat = pl.BlockSpec((half, width), lambda i: (i, 0))
    kept = pl.BlockSpec((half, width), lambda i: (0, 0))
    gain = pl.BlockSpec((1, width), lambda i: (0, 0))
    updated, low, high = pl.pallas_call(
        norms_kernel,
        out_shape=[jax.ShapeDtypeStruct((rows, width), BF16), half_out, half_out],
        grid=(2,),
        in_specs=[
            pl.BlockSpec((None, half, width), lambda i: (0, i, 0)), flat, flat, flat, gain, gain,
        ],
        out_specs=[flat, kept, kept],
        compiler_params=SMALL,
        name="norms",
        cost_estimate=pl.CostEstimate(flops=4_000_000, bytes_accessed=3_500_000, transcendentals=300),
    )(near, below, above, residual, gain_mix.reshape(1, width), gain_pre.reshape(1, width))
    below_low, above_high = shifted(low, "tp", 1), shifted(high, "tp", -1)
    below_high, above_low = shifted(high, "tp", 1), shifted(low, "tp", -1)
    far_low, far_high = shifted(below_low, "tp", 1), shifted(above_high, "tp", -1)

    ups, downs = 4, 4
    whole = pl.BlockSpec(memory_space=pltpu.VMEM)
    turned = pltpu.VMEM((width, rows), BF16)
    turned_half = pltpu.VMEM((width // 2, rows), BF16)
    weights = pltpu.VMEM((devices, share, units), BF16)
    scratch = [pltpu.VMEM((2 * rows, width), BF16), pltpu.VMEM((units, 2 * rows), BF16)]
    up, down, own, low, high = pl.pallas_call(
        functools.partial(far_mixer_kernel, ups=ups, downs=downs),
        out_shape=(weights, weights, turned, turned_half, turned_half),
        in_specs=[*([whole] * 4), pl.BlockSpec(memory_space=pltpu.HBM)],
        out_specs=[whole] * 5,
        scratch_shapes=[*scratch, pltpu.SemaphoreType.DMA((ups + downs,))],
        compiler_params=SMALL,
        name="mixer_far",
        cost_estimate=pl.CostEstimate(
            flops=8 * rows * width * units, bytes_accessed=20_000_000, transcendentals=0
        ),
    )(low, high, far_low, far_high, pltpu.with_memory_space_constraint(both, pltpu.HBM))
    low, high = shifted(low, "tp", 1), shifted(high, "tp", -1)
    minus_low, minus_high, plus_low, plus_high = pl.pallas_call(
        functools.partial(near_mixer_kernel, ups=2, downs=2),
        out_shape=(turned_half,) * 4,
        in_specs=[whole] * 6,
        out_specs=[whole] * 4,
        scratch_shapes=scratch,
        compiler_params=SMALL,
        name="mixer_near",
        cost_estimate=pl.CostEstimate(
            flops=8 * rows * width * units, bytes_accessed=2_000_000, transcendentals=0
        ),
    )(below_low, below_high, above_low, above_high, up, down)
    below_high, above_low = shifted(plus_high, "tp", 1), shifted(minus_low, "tp", -1)
    plus_low, minus_high = pl.pallas_call(
        tail_join_kernel,
        out_shape=(turned_half,) * 2,
        in_specs=[whole] * 4,
        out_specs=[whole] * 2,
        compiler_params=SMALL,
        name="tail_join",
        cost_estimate=pl.CostEstimate(flops=500_000, bytes_accessed=1_500_000, transcendentals=0),
    )(plus_low, minus_high, low, high)
    below_low, above_high = shifted(plus_low, "tp", 1), shifted(minus_high, "tp", -1)
    return pl.pallas_call(
        result_kernel,
        out_shape=jax.ShapeDtypeStruct((rows, width), BF16),
        compiler_params=SMALL,
        name="result",
        cost_estimate=pl.CostEstimate(flops=4_000_000, bytes_accessed=3_500_000, transcendentals=300),
    )(
        own, below_low, below_high, above_low, above_high, updated, gain_mlp.reshape(1, width)
    )


def solution(mesh):
    finer = Mesh(mesh.devices.reshape(8, 4, 2, mesh.shape["tp"]), ("sp_0", "sp_1", "sp_2", "tp"))
    in_specs = (
        *([P(SP, "tp")] * 8),
        P("tp", SP),
        P("tp", SP),
        P(SP_TP, None),
        P("tp", None),
        P("tp", None),
        P(SP, "tp"),
        P("tp", SP),
        P(),
        P(),
        P(),
    )
    return jax.shard_map(
        local, mesh=finer, in_specs=in_specs, out_specs=P(SP_TP, None), check_vma=False
    )
```

```python
import functools

import jax
import jax.numpy as jnp
import numpy as np
from jax import lax
from jax.experimental import pallas as pl
from jax.experimental.pallas import tpu as pltpu
from jax.sharding import Mesh
from jax.sharding import PartitionSpec as P

SPAN = 128
LANES = 128
SPANS = 4
SPAN_PART = 16
SP = ("sp_0", "sp_1", "sp_2")
SP_TP = ("sp_0", "sp_1", "sp_2", "tp")
EPS = 1e-06
WIDE_SCALE = 128 ** (-0.5)
NARROW_SCALE = 64 ** (-0.5)
F32 = jnp.float32
BF16 = jnp.bfloat16


def position_tables(devices):
    lane = np.arange(LANES)
    inside, upper, lower = [], [], []
    for head_dim in (128, 64):
        half = head_dim // 2
        rate = 10000.0 ** (-2.0 * (lane % half) / head_dim)
        sign = np.where(lane % head_dim < half, -1.0, 1.0)
        for table, positions in (
            (inside, np.arange(SPAN)),
            (upper, np.arange(devices * SPANS // SPAN_PART) * SPAN_PART * SPAN),
            (lower, np.arange(SPAN_PART) * SPAN),
        ):
            angles = positions[:, None] * rate
            table += [np.cos(angles), np.sin(angles) * sign]
    return [np.stack(t).astype(np.float32) for t in (inside, upper, lower)]


def turned_by(first, second):
    return (
        first[0] * second[0] - first[1] * second[1],
        first[1] * second[0] + first[0] * second[1],
    )


def span_tables(table_refs, block, group):
    inside_ref, upper_ref, lower_ref = table_refs
    start = turned_by(
        *(
            [ref[2 * group + k, pl.ds(at, 1), :] for k in range(2)]
            for ref, at in ((upper_ref, block // SPAN_PART), (lower_ref, block % SPAN_PART))
        )
    )
    return turned_by((inside_ref[2 * group], inside_ref[2 * group + 1]), start)


def rotated_wide(x, tables):
    x = x.astype(F32)
    return x * tables[0] + pltpu.roll(x, 64, 1) * tables[1]


def rotated_narrow(x, tables):
    x = x.astype(F32)
    lane = lax.broadcasted_iota(jnp.int32, x.shape, 1)
    partner = jnp.where((lane & 32) == 0, pltpu.roll(x, 96, 1), pltpu.roll(x, 32, 1))
    return x * tables[0] + partner * tables[1]


def running_decay(wide_decay_ref, narrow_decay_ref, rows_ref):
    rows_ref[...] = jnp.zeros_like(rows_ref)
    rows_ref[0:3, :] = wide_decay_ref[...]
    rows_ref[3:5, :] = narrow_decay_ref[...]
    x = rows_ref[...]
    lane = lax.broadcasted_iota(jnp.int32, x.shape, 1)
    step = 1
    while step < SPAN:
        x = x + jnp.where(lane >= step, pltpu.roll(x, step, 1), 0.0)
        step *= 2
    return x


def low_rows(shape):
    return lax.broadcasted_iota(jnp.int32, shape, 0) < 64


def low_lanes(shape):
    return lax.broadcasted_iota(jnp.int32, shape, 1) < 64


def mm(a, b):
    return jnp.dot(a, b, preferred_element_type=F32)


def mm_nt(a, b):
    return lax.dot_general(a, b, (((1,), (1,)), ((), ())), preferred_element_type=F32)


def mm_tn(a, b):
    return lax.dot_general(a, b, (((0,), (0,)), ((), ())), preferred_element_type=F32)


def turned_span(place, turn):
    return (turn + jnp.where(place == 0, 2, jnp.where(place == 3, 1, jnp.where(place == 2, 3, 0)))) & 3


def states_kernel(
    index_ref, _, wk_ref, wv_ref, nk_ref, nv_ref, wd_ref, nd_ref, *refs, staged,
):
    table_refs, refs = refs[:3], refs[3:]
    sources, refs = refs[:staged], refs[staged:]
    before_ref, earlier_ref, message_ref = refs[:3]
    targets, refs = refs[3 : 3 + staged], refs[3 + staged :]
    rows_ref, state_ref, decay_ref, sems = refs
    span = pl.program_id(0)
    place = index_ref[0] * SPANS + span
    copies = [pltpu.make_async_copy(a, b, sems.at[k]) for k, (a, b) in enumerate(zip(sources, targets))]

    @pl.when(span == 0)
    def _():
        for copy in copies:
            copy.start()
        state_ref[...] = jnp.zeros_like(state_ref)
        decay_ref[...] = jnp.zeros_like(decay_ref)

    total = running_decay(wd_ref, nd_ref, rows_ref)
    last = total[:, SPAN - 1 : SPAN]
    tail = jnp.exp(last - total).T
    kept = jnp.exp(last)
    before_ref[0] = state_ref[...]
    earlier_ref[0] = decay_ref[...]
    tables = span_tables(table_refs, place, 0)
    for head in range(3):
        cut = slice(head * 128, head * 128 + 128)
        keys = rotated_wide(wk_ref[:, cut], tables) * WIDE_SCALE
        scaled = (keys * tail[:, head : head + 1]).astype(BF16)
        state_ref[cut, :] = state_ref[cut, :] * kept[head : head + 1, :] + mm_tn(scaled, wv_ref[:, cut])
    tables = span_tables(table_refs, place, 1)
    keys = rotated_narrow(nk_ref[...], tables) * NARROW_SCALE
    tails = jnp.where(low_lanes((SPAN, LANES)), tail[:, 3:4], tail[:, 4:5])
    own = mm_tn((keys * tails).astype(BF16), nv_ref[...])
    square = (LANES, LANES)
    own = jnp.where(low_rows(square) == low_lanes(square), own, 0.0)
    keeps = jnp.where(low_rows(square), kept[3:4, :], kept[4:5, :])
    state_ref[384:512, :] = state_ref[384:512, :] * keeps + own
    decay_ref[...] += jnp.broadcast_to(last, decay_ref.shape)

    @pl.when(span == SPANS - 1)
    def _():
        sums = decay_ref[...]
        high = sums.astype(BF16).astype(F32)
        low = sums - high
        sub = lax.broadcasted_iota(jnp.int32, (8, LANES), 0)
        at = 0
        for head, count in enumerate((16, 16, 16, 8, 8)):
            pair = jnp.where(
                sub == 0,
                high[head : head + 1, :],
                jnp.where(sub == 1, low[head : head + 1, :], 0.0),
            )
            body = state_ref[at * 8 : (at + count) * 8, :].reshape(count, 8, LANES)
            ends = jnp.broadcast_to(pair[None], (count, 8, LANES))
            message_ref[at : at + count] = jnp.concatenate([body, ends], axis=1).astype(BF16)
            at += count
        for copy in copies:
            copy.wait()


def prefix_kernel(message_ref, out_ref):
    devices = message_ref.shape[0]
    carried = jnp.zeros((8, LANES), F32)
    for k in range(devices):
        out_ref[k] = carried.astype(BF16)
        if k + 1 < devices:
            piece = message_ref[k].astype(F32)
            kept = jnp.exp(piece[8:9, :] + piece[9:10, :])
            carried = carried * kept + piece[0:8, :]


def gated(output, gate, scale):
    gate = gate.astype(F32)
    return (output * scale * (gate / (1.0 + jnp.exp(-gate)))).astype(BF16)


def finish_kernel(
    index_ref, turn_ref, wq_ref, wk_ref, wv_ref, wg_ref, nq_ref, nk_ref, nv_ref, ng_ref, wd_ref, nd_ref,
    inside_ref, upper_ref, lower_ref, before_ref, earlier_ref, prefix_ref, wide_out_ref, narrow_out_ref,
    *out_refs, first,
):
    *out_refs, rows_ref, mixed_ref = out_refs
    span = turned_span(first + pl.program_id(0), turn_ref[0])
    place = index_ref[0] * SPANS + span
    table_refs = (inside_ref, upper_ref, lower_ref)
    total = running_decay(wd_ref, nd_ref, rows_ref)
    columns = total.T
    grown = jnp.exp(columns)
    earlier = jnp.exp(earlier_ref[0])
    square = (SPAN, SPAN)
    causal = lax.broadcasted_iota(jnp.int32, square, 0) >= lax.broadcasted_iota(jnp.int32, square, 1)

    def weights(scores, head):
        gaps = columns[:, head : head + 1] - total[head : head + 1, :]
        return (scores * jnp.exp(jnp.where(causal, gaps, -jnp.inf))).astype(BF16)

    tables = span_tables(table_refs, place, 0)
    for head in range(3):
        cut = slice(head * 128, head * 128 + 128)
        queries = rotated_wide(wq_ref[:, cut], tables).astype(BF16)
        keys = (rotated_wide(wk_ref[:, cut], tables) * WIDE_SCALE).astype(BF16)
        within = mm(weights(mm_nt(queries, keys), head), wv_ref[:, cut])
        entering = (
            prefix_ref[cut, :].astype(F32) * earlier[head : head + 1, :] + before_ref[0, cut, :]
        ).astype(BF16)
        output = within + mm(queries, entering) * grown[:, head : head + 1]
        scale = lax.rsqrt(jnp.mean(output * output, axis=-1, keepdims=True) + EPS)
        mixed_ref[:, cut] = gated(output, wg_ref[:, cut], scale)

    tables = span_tables(table_refs, place, 1)
    queries = rotated_narrow(nq_ref[...], tables).astype(BF16)
    keys = (rotated_narrow(nk_ref[...], tables) * NARROW_SCALE).astype(BF16)
    values = nv_ref[...]
    low = low_lanes(square)
    none = jnp.zeros_like(queries)
    within = jnp.where(
        low,
        mm(weights(mm_nt(jnp.where(low, queries, none), keys), 3), values),
        mm(weights(mm_nt(jnp.where(low, none, queries), keys), 4), values),
    )
    fades = jnp.where(low_rows(square), earlier[3:4, :], earlier[4:5, :])
    entering = (prefix_ref[384:512, :].astype(F32) * fades + before_ref[0, 384:512, :]).astype(BF16)
    output = within + mm(queries, entering) * jnp.where(low, grown[:, 3:4], grown[:, 4:5])
    squares = output * output
    left = jnp.sum(jnp.where(low, squares, 0.0), axis=-1, keepdims=True)
    right = jnp.sum(jnp.where(low, 0.0, squares), axis=-1, keepdims=True)
    scale = lax.rsqrt(jnp.where(low, left, right) * (1.0 / 64.0) + EPS)
    mixed_ref[:, 384:512] = gated(output, ng_ref[...], scale)

    projected = (
        mm(mixed_ref[:, 0:384], wide_out_ref[...]) + mm(mixed_ref[:, 384:512], narrow_out_ref[...])
    ).astype(BF16)
    if len(out_refs) == 2:
        half = SPAN // 2
        out_refs[0][...] = projected[:half]
        out_refs[1][...] = projected[half:]
    else:
        out_refs[0][0] = projected


def join_kernel(minus_ref, plus_ref, from_below_ref, from_above_ref, minus_out_ref, plus_out_ref):
    part = pl.program_id(0)

    @pl.when(part == 0)
    def _():
        minus_out_ref[...] = minus_ref[...]
        plus_out_ref[...] = (plus_ref[...].astype(F32) + from_below_ref[...].astype(F32)).astype(BF16)

    @pl.when(part == 1)
    def _():
        minus_out_ref[...] = (minus_ref[...].astype(F32) + from_above_ref[...].astype(F32)).astype(BF16)
        plus_out_ref[...] = plus_ref[...]


def rms(values, gain):
    return values * lax.rsqrt(jnp.mean(values * values, axis=-1, keepdims=True) + EPS) * gain


def norms_kernel(
    own_ref, below_ref, above_ref, residual_ref, mix_ref, pre_ref, updated_ref, low_ref, high_ref
):
    projected = own_ref[...].astype(F32) + below_ref[...].astype(F32) + above_ref[...].astype(F32)
    updated = (residual_ref[...].astype(F32) + rms(projected, mix_ref[...])).astype(BF16)
    updated_ref[...] = updated
    normed = rms(updated.astype(F32), pre_ref[...]).astype(BF16)

    @pl.when(pl.program_id(0) == 0)
    def _():
        low_ref[...] = normed

    @pl.when(pl.program_id(0) == 1)
    def _():
        high_ref[...] = normed


def tail_join_kernel(plus_ref, minus_ref, from_below_ref, from_above_ref, plus_out_ref, minus_out_ref):
    plus_out_ref[...] = (plus_ref[...].astype(F32) + from_below_ref[...].astype(F32)).astype(BF16)
    minus_out_ref[...] = (minus_ref[...].astype(F32) + from_above_ref[...].astype(F32)).astype(BF16)


def result_kernel(
    own_ref, below_low_ref, below_high_ref, above_low_ref, above_high_ref,
    updated_ref, gain_ref, out_ref,
):
    half = below_low_ref.shape[0]
    lowered = [
        own_ref[part].astype(F32) + below[...].astype(F32) + above[...].astype(F32)
        for part, below, above in (
            (slice(0, half), below_low_ref, above_low_ref),
            (slice(half, 2 * half), below_high_ref, above_high_ref),
        )
    ]
    lowered = jnp.concatenate(lowered, axis=0).T
    out_ref[...] = (updated_ref[...].astype(F32) + rms(lowered, gain_ref[...])).astype(BF16)


def up_block(x_ref, up_ref, at, block):
    weight = up_ref[:, :, pl.ds(at, block)].reshape(-1, block)
    rectified = jnp.maximum(mm(x_ref[...], weight), 0.0)
    return (rectified * rectified).astype(BF16).T


def down_block(down_ref, hidden_ref, k, group):
    weight = down_ref[pl.ds(k * group, group)].reshape(-1, hidden_ref.shape[0])
    return mm(weight, hidden_ref[...]).astype(BF16)


def far_mixer_kernel(*refs, ups, downs):
    halves, refs = refs[:2], refs[2:]
    both_ref, up_ref, down_ref, low_ref, high_ref, x_ref, hidden_ref, sems = refs
    devices, share, units = up_ref.shape
    half = halves[0].shape[0]
    block = units // ups
    group = devices // downs
    lines = group * share

    def up_copy(k):
        at = pl.multiple_of(k * block, block)
        return pltpu.make_async_copy(
            both_ref.at[:, 0, :, pl.ds(at, block)], up_ref.at[:, :, pl.ds(at, block)], sems.at[k]
        )

    def down_copy(k):
        at = k * group
        return pltpu.make_async_copy(
            both_ref.at[pl.ds(at, group), 1], down_ref.at[pl.ds(at, group)], sems.at[ups + k]
        )

    for k in range(ups):
        up_copy(k).start()
    for k in range(downs):
        down_copy(k).start()
    for k, ref in enumerate(halves):
        x_ref[k * half : (k + 1) * half] = ref[...]

    @pl.loop(0, ups)
    def _(k):
        up_copy(k).wait()
        at = pl.multiple_of(k * block, block)
        hidden_ref[pl.ds(at, block), :] = up_block(x_ref, up_ref, at, block)

    def lower(k, far_ref, base):
        down_copy(k).wait()
        lowered = down_block(down_ref, hidden_ref, k, group)
        far_ref[pl.ds(pl.multiple_of((k - base) * lines, lines), lines), :] = lowered

    @pl.loop(0, downs // 2)
    def _(k):
        lower(k, low_ref, 0)

    @pl.loop(downs // 2, downs)
    def _(k):
        lower(k, high_ref, downs // 2)


def near_mixer_kernel(*refs, ups, downs):
    halves, refs = refs[:4], refs[4:]
    up_ref, down_ref, minus_low_ref, minus_high_ref, plus_low_ref, plus_high_ref, x_ref, hidden_ref = refs
    devices, share, units = up_ref.shape
    half = halves[0].shape[0]
    rows = 2 * half
    block = units // ups
    group = devices // downs
    lines = group * share
    for k, ref in enumerate(halves):
        x_ref[k * half : (k + 1) * half] = ref[...]

    @pl.loop(0, ups)
    def _(k):
        at = pl.multiple_of(k * block, block)
        hidden_ref[pl.ds(at, block), :] = up_block(x_ref, up_ref, at, block)

    for first, minus_ref, plus_ref in (
        (0, minus_low_ref, plus_low_ref), (downs // 2, minus_high_ref, plus_high_ref)
    ):
        for k in range(downs // 2):
            lowered = down_block(down_ref, hidden_ref, first + k, group)
            at = slice(k * lines, (k + 1) * lines)
            minus_ref[at, :] = lowered[:, :rows]
            plus_ref[at, :] = lowered[:, rows:]


def own_mixer_kernel(first_ref, second_ref, up_ref, down_ref, out_ref, x_ref, hidden_ref, *, parts):
    devices, share, units = up_ref.shape
    half = first_ref.shape[0]
    x_ref[:half] = first_ref[...]
    x_ref[half:] = second_ref[...]
    hidden_ref[...] = up_block(x_ref, up_ref, 0, units)
    group = devices // parts
    lines = group * share
    for k in range(parts):
        out_ref[k * lines : (k + 1) * lines, :] = down_block(down_ref, hidden_ref, k, group)


SMALL = pltpu.CompilerParams(vmem_limit_bytes=16 * 1024 * 1024)


def shifted(array, axis, by):
    size = lax.axis_size(axis)
    return lax.ppermute(array, axis, [(k, (k + by) % size) for k in range(size)])


def joined(minus, plus, from_below, from_above, picks=(None, None)):
    half, width = from_below.shape
    flat = pl.BlockSpec((half, width), lambda i: (i, 0))
    kept = pl.BlockSpec((half, width), lambda i: (0, 0))
    out = jax.ShapeDtypeStruct((2 * half, width), BF16)

    def source(pick):
        if pick is None:
            return flat
        return pl.BlockSpec((None, half, width), lambda i: (pick, i, 0))

    return pl.pallas_call(
        join_kernel,
        out_shape=(out, out),
        grid=(2,),
        in_specs=[source(picks[0]), source(picks[1]), kept, kept],
        out_specs=[flat, flat],
        compiler_params=SMALL,
        name="join",
        cost_estimate=pl.CostEstimate(flops=1_000_000, bytes_accessed=3_500_000, transcendentals=0),
    )(minus, plus, from_below, from_above)


def local(
    wide_query, wide_key, wide_value, wide_gate,
    narrow_query, narrow_key, narrow_value, narrow_gate,
    wide_decay, narrow_decay, residual, wide_out, narrow_out,
    up_weight, down_weight, gain_mix, gain_pre, gain_mlp,
):
    devices = lax.axis_size(SP)
    ranks = lax.axis_size("tp")
    length, width = wide_query.shape[0], residual.shape[1]
    rows = residual.shape[0]
    share = up_weight.shape[0]
    units = up_weight.shape[1]

    both = lax.all_gather(
        jnp.concatenate([up_weight, down_weight.T], axis=0), SP, axis=0, tiled=True
    ).reshape(devices, 2, share, units)

    tables = [jnp.asarray(t) for t in position_tables(devices)]
    scalars = [
        lax.axis_index(SP).astype(jnp.int32).reshape(1),
        lax.axis_index("tp").astype(jnp.int32).reshape(1),
    ]
    table_blocks = [pl.BlockSpec(t.shape, lambda s, i, t: (0, 0, 0)) for t in tables]

    def span_blocks(at):
        return (
            pl.BlockSpec((SPAN, 384), lambda s, i, t: (at(s, i, t), 0)),
            pl.BlockSpec((SPAN, 128), lambda s, i, t: (at(s, i, t), 0)),
            [
                pl.BlockSpec((3, SPAN), lambda s, i, t: (0, at(s, i, t))),
                pl.BlockSpec((2, SPAN), lambda s, i, t: (0, at(s, i, t))),
            ],
            [
                pl.BlockSpec((1, 512, LANES), lambda s, i, t: (at(s, i, t), 0, 0)),
                pl.BlockSpec((1, 8, LANES), lambda s, i, t: (at(s, i, t), 0, 0)),
            ],
        )

    wide_block, narrow_block, decay_blocks, state_blocks = span_blocks(lambda s, i, t: s)
    staged = (
        *tables, wide_decay, narrow_decay, wide_query, wide_key, wide_value, wide_gate,
        narrow_query, narrow_key, narrow_value, narrow_gate, wide_out, narrow_out,
    )
    before, earlier, message, *held = pl.pallas_call(
        functools.partial(states_kernel, staged=len(staged)),
        out_shape=(
            jax.ShapeDtypeStruct((SPANS, 512, LANES), F32),
            jax.ShapeDtypeStruct((SPANS, 8, LANES), F32),
            jax.ShapeDtypeStruct((devices, 16, LANES), BF16),
            *(pltpu.VMEM(x.shape, x.dtype) for x in staged),
        ),
        grid_spec=pltpu.PrefetchScalarGridSpec(
            num_scalar_prefetch=2,
            grid=(SPANS,),
            in_specs=[
                wide_block, wide_block, narrow_block, narrow_block, *decay_blocks, *table_blocks,
                *([pl.BlockSpec(memory_space=pltpu.HBM)] * len(staged)),
            ],
            out_specs=[
                *state_blocks,
                pl.BlockSpec((devices, 16, LANES), lambda s, i, t: (0, 0, 0)),
                *([pl.BlockSpec(memory_space=pltpu.VMEM)] * len(staged)),
            ],
            scratch_shapes=[
                pltpu.VMEM((8, LANES), F32),
                pltpu.VMEM((512, LANES), F32),
                pltpu.VMEM((8, LANES), F32),
                pltpu.SemaphoreType.DMA((len(staged),)),
            ],
        ),
        compiler_params=SMALL,
        name="states",
        cost_estimate=pl.CostEstimate(flops=60_000_000, bytes_accessed=2_500_000, transcendentals=20_000),
    )(
        *scalars,
        *(
            pltpu.with_memory_space_constraint(x, pltpu.HBM)
            for x in (
                wide_key, wide_value, narrow_key, narrow_value,
                wide_decay, narrow_decay, *tables, *staged,
            )
        ),
    )

    arrived = lax.all_to_all(message, SP, 0, 0, tiled=True)
    prefixes = pl.pallas_call(
        prefix_kernel,
        out_shape=jax.ShapeDtypeStruct((devices, 8, LANES), BF16),
        compiler_params=SMALL,
        name="prefix",
        cost_estimate=pl.CostEstimate(flops=2_000_000, bytes_accessed=400_000, transcendentals=8_000),
    )(arrived)
    prefix = lax.all_to_all(prefixes, SP, 0, 0, tiled=True).reshape(512, LANES)

    def finish(first, count, out_shape, out_specs):
        wide, narrow, decays, states = span_blocks(lambda s, i, t: turned_span(first + s, t[0]))
        return pl.pallas_call(
            functools.partial(finish_kernel, first=first),
            out_shape=out_shape,
            grid_spec=pltpu.PrefetchScalarGridSpec(
                num_scalar_prefetch=2,
                grid=(count,),
                in_specs=[
                    wide, wide, wide, wide, narrow, narrow, narrow, narrow,
                    *decays, *table_blocks, *states,
                    pl.BlockSpec((512, LANES), lambda s, i, t: (0, 0)),
                    pl.BlockSpec((384, width), lambda s, i, t: (0, 0)),
                    pl.BlockSpec((128, width), lambda s, i, t: (0, 0)),
                ],
                out_specs=out_specs,
                scratch_shapes=[pltpu.VMEM((8, LANES), F32), pltpu.VMEM((SPAN, 512), BF16)],
            ),
            compiler_params=SMALL,
            name="finish" if first else "finish_far",
            cost_estimate=pl.CostEstimate(
                flops=350_000_000 * count,
                bytes_accessed=3_000_000 + 1_500_000 * count,
                transcendentals=150_000 * count,
            ),
        )(
            *scalars, *held[5:13], *held[3:5], *held[:3], before, earlier, prefix, *held[13:],
        )

    half = rows // 2
    half_out = jax.ShapeDtypeStruct((half, width), BF16)
    near_out = jax.ShapeDtypeStruct((3, rows, width), BF16)
    low, high = finish(
        0, 1, (half_out, half_out), [pl.BlockSpec((half, width), lambda s, i, t: (0, 0))] * 2
    )
    low, high = shifted(low, "tp", 1), shifted(high, "tp", -1)
    (near,) = finish(
        1, 3, (near_out,), [pl.BlockSpec((1, rows, width), lambda s, i, t: (s, 0, 0))]
    )
    minus, plus = joined(near, near, low, high, (1, 2))
    below, above = shifted(plus, "tp", 1), shifted(minus, "tp", -1)
    flat = pl.BlockSpec((half, width), lambda i: (i, 0))
    kept = pl.BlockSpec((half, width), lambda i: (0, 0))
    gain = pl.BlockSpec((1, width), lambda i: (0, 0))
    updated, low, high = pl.pallas_call(
        norms_kernel,
        out_shape=[jax.ShapeDtypeStruct((rows, width), BF16), half_out, half_out],
        grid=(2,),
        in_specs=[
            pl.BlockSpec((None, half, width), lambda i: (0, i, 0)), flat, flat, flat, gain, gain,
        ],
        out_specs=[flat, kept, kept],
        compiler_params=SMALL,
        name="norms",
        cost_estimate=pl.CostEstimate(flops=4_000_000, bytes_accessed=3_500_000, transcendentals=300),
    )(near, below, above, residual, gain_mix.reshape(1, width), gain_pre.reshape(1, width))
    below_low, above_high = shifted(low, "tp", 1), shifted(high, "tp", -1)
    below_high, above_low = shifted(high, "tp", 1), shifted(low, "tp", -1)
    far_low, far_high = shifted(below_low, "tp", 1), shifted(above_high, "tp", -1)

    ups, downs = 4, 4
    whole = pl.BlockSpec(memory_space=pltpu.VMEM)
    turned = pltpu.VMEM((width, rows), BF16)
    turned_half = pltpu.VMEM((width // 2, rows), BF16)
    weights = pltpu.VMEM((devices, share, units), BF16)
    scratch = [pltpu.VMEM((2 * rows, width), BF16), pltpu.VMEM((units, 2 * rows), BF16)]
    scratch_half = [pltpu.VMEM((rows, width), BF16), pltpu.VMEM((units, rows), BF16)]
    own_low, own_high = low, high
    up, down, low, high = pl.pallas_call(
        functools.partial(far_mixer_kernel, ups=ups, downs=downs),
        out_shape=(weights, weights, turned_half, turned_half),
        in_specs=[*([whole] * 2), pl.BlockSpec(memory_space=pltpu.HBM)],
        out_specs=[whole] * 4,
        scratch_shapes=[*scratch_half, pltpu.SemaphoreType.DMA((ups + downs,))],
        compiler_params=SMALL,
        name="mixer_far",
        cost_estimate=pl.CostEstimate(
            flops=4 * rows * width * units, bytes_accessed=20_000_000, transcendentals=0
        ),
    )(far_low, far_high, pltpu.with_memory_space_constraint(both, pltpu.HBM))
    low, high = shifted(low, "tp", 1), shifted(high, "tp", -1)
    minus_low, minus_high, plus_low, plus_high = pl.pallas_call(
        functools.partial(near_mixer_kernel, ups=1, downs=2),
        out_shape=(turned_half,) * 4,
        in_specs=[whole] * 6,
        out_specs=[whole] * 4,
        scratch_shapes=scratch,
        compiler_params=SMALL,
        name="mixer_near",
        cost_estimate=pl.CostEstimate(
            flops=8 * rows * width * units, bytes_accessed=2_000_000, transcendentals=0
        ),
    )(below_low, below_high, above_low, above_high, up, down)
    below_high, above_low = shifted(plus_high, "tp", 1), shifted(minus_low, "tp", -1)
    plus_low, minus_high = pl.pallas_call(
        tail_join_kernel,
        out_shape=(turned_half,) * 2,
        in_specs=[whole] * 4,
        out_specs=[whole] * 2,
        compiler_params=SMALL,
        name="tail_join",
        cost_estimate=pl.CostEstimate(flops=500_000, bytes_accessed=1_500_000, transcendentals=0),
    )(plus_low, minus_high, low, high)
    below_low, above_high = shifted(plus_low, "tp", 1), shifted(minus_high, "tp", -1)
    own_low, _ = lax.optimization_barrier((own_low, plus_low))
    own = pl.pallas_call(
        functools.partial(own_mixer_kernel, parts=2),
        out_shape=turned,
        in_specs=[whole] * 4,
        out_specs=whole,
        scratch_shapes=scratch_half,
        compiler_params=SMALL,
        name="mixer_own",
        cost_estimate=pl.CostEstimate(
            flops=4 * rows * width * units, bytes_accessed=2_000_000, transcendentals=0
        ),
    )(own_low, own_high, up, down)
    return pl.pallas_call(
        result_kernel,
        out_shape=jax.ShapeDtypeStruct((rows, width), BF16),
        compiler_params=SMALL,
        name="result",
        cost_estimate=pl.CostEstimate(flops=4_000_000, bytes_accessed=3_500_000, transcendentals=300),
    )(
        own, below_low, below_high, above_low, above_high, updated, gain_mlp.reshape(1, width)
    )


def solution(mesh):
    finer = Mesh(mesh.devices.reshape(8, 4, 2, mesh.shape["tp"]), ("sp_0", "sp_1", "sp_2", "tp"))
    in_specs = (
        *([P(SP, "tp")] * 8),
        P("tp", SP),
        P("tp", SP),
        P(SP_TP, None),
        P("tp", None),
        P("tp", None),
        P(SP, "tp"),
        P("tp", SP),
        P(),
        P(),
        P(),
    )
    return jax.shard_map(
        local, mesh=finer, in_specs=in_specs, out_specs=P(SP_TP, None), check_vma=False
    )
```

```python
import functools

import jax
import jax.numpy as jnp
import numpy as np
from jax import lax
from jax.experimental import pallas as pl
from jax.experimental.pallas import tpu as pltpu
from jax.sharding import Mesh
from jax.sharding import PartitionSpec as P

SPAN = 128
LANES = 128
SPANS = 4
SPAN_PART = 16
SLICE_HEADS = (0, 0, 1, 1, 2, 2, 3, 4)
SP = ("sp_0", "sp_1", "sp_2")
SP_TP = ("sp_0", "sp_1", "sp_2", "tp")
EPS = 1e-06
WIDE_SCALE = 128 ** (-0.5)
NARROW_SCALE = 64 ** (-0.5)
F32 = jnp.float32
BF16 = jnp.bfloat16


def position_tables(devices):
    lane = np.arange(LANES)
    inside, upper, lower = [], [], []
    for head_dim in (128, 64):
        half = head_dim // 2
        rate = 10000.0 ** (-2.0 * (lane % half) / head_dim)
        sign = np.where(lane % head_dim < half, -1.0, 1.0)
        for table, positions in (
            (inside, np.arange(SPAN)),
            (upper, np.arange(devices * SPANS // SPAN_PART) * SPAN_PART * SPAN),
            (lower, np.arange(SPAN_PART) * SPAN),
        ):
            angles = positions[:, None] * rate
            table += [np.cos(angles), np.sin(angles) * sign]
    return [np.stack(t).astype(np.float32) for t in (inside, upper, lower)]


def turned_by(first, second):
    return (
        first[0] * second[0] - first[1] * second[1],
        first[1] * second[0] + first[0] * second[1],
    )


def span_tables(table_refs, block, group):
    inside_ref, upper_ref, lower_ref = table_refs
    start = turned_by(
        *(
            [ref[2 * group + k, pl.ds(at, 1), :] for k in range(2)]
            for ref, at in ((upper_ref, block // SPAN_PART), (lower_ref, block % SPAN_PART))
        )
    )
    return turned_by((inside_ref[2 * group], inside_ref[2 * group + 1]), start)


def rotated_wide(x, tables):
    x = x.astype(F32)
    return x * tables[0] + pltpu.roll(x, 64, 1) * tables[1]


def rotated_narrow(x, tables):
    x = x.astype(F32)
    lane = lax.broadcasted_iota(jnp.int32, x.shape, 1)
    partner = jnp.where((lane & 32) == 0, pltpu.roll(x, 96, 1), pltpu.roll(x, 32, 1))
    return x * tables[0] + partner * tables[1]


def running_decay(wide_decay_ref, narrow_decay_ref, rows_ref):
    rows_ref[...] = jnp.zeros_like(rows_ref)
    rows_ref[0:3, :] = wide_decay_ref[...]
    rows_ref[3:5, :] = narrow_decay_ref[...]
    x = rows_ref[...]
    lane = lax.broadcasted_iota(jnp.int32, x.shape, 1)
    step = 1
    while step < SPAN:
        x = x + jnp.where(lane >= step, pltpu.roll(x, step, 1), 0.0)
        step *= 2
    return x


def low_rows(shape):
    return lax.broadcasted_iota(jnp.int32, shape, 0) < 64


def low_lanes(shape):
    return lax.broadcasted_iota(jnp.int32, shape, 1) < 64


def mm(a, b):
    return jnp.dot(a, b, preferred_element_type=F32)


def mm_nt(a, b):
    return lax.dot_general(a, b, (((1,), (1,)), ((), ())), preferred_element_type=F32)


def mm_tn(a, b):
    return lax.dot_general(a, b, (((0,), (0,)), ((), ())), preferred_element_type=F32)


def in_two(values):
    high = values.astype(BF16).astype(F32)
    return high, values - high


def log_rows(high, low):
    sub = lax.broadcasted_iota(jnp.int32, (16, LANES), 0)
    return jnp.where(sub == 0, high, jnp.where(sub == 1, low, 0.0)).astype(BF16)


def turned_span(place, turn):
    return (turn + jnp.where(place == 0, 2, jnp.where(place == 3, 1, jnp.where(place == 2, 3, 0)))) & 3


def states_kernel(
    index_ref, _, wk_ref, wv_ref, nk_ref, nv_ref, wd_ref, nd_ref, *refs, staged,
):
    table_refs, refs = refs[:3], refs[3:]
    sources, refs = refs[:staged], refs[staged:]
    before_ref, earlier_ref, message_ref = refs[:3]
    targets, refs = refs[3 : 3 + staged], refs[3 + staged :]
    rows_ref, state_ref, decay_ref, sems = refs
    span = pl.program_id(0)
    place = index_ref[0] * SPANS + span
    copies = [pltpu.make_async_copy(a, b, sems.at[k]) for k, (a, b) in enumerate(zip(sources, targets))]

    @pl.when(span == 0)
    def _():
        for copy in copies:
            copy.start()
        state_ref[...] = jnp.zeros_like(state_ref)
        decay_ref[...] = jnp.zeros_like(decay_ref)

    total = running_decay(wd_ref, nd_ref, rows_ref)
    last = total[:, SPAN - 1 : SPAN]
    tail = jnp.exp(last - total).T
    kept = jnp.exp(last)
    before_ref[0] = state_ref[...]
    earlier_ref[0] = decay_ref[...]
    tables = span_tables(table_refs, place, 0)
    for head in range(3):
        cut = slice(head * 128, head * 128 + 128)
        keys = rotated_wide(wk_ref[:, cut], tables) * WIDE_SCALE
        scaled = (keys * tail[:, head : head + 1]).astype(BF16)
        state_ref[cut, :] = state_ref[cut, :] * kept[head : head + 1, :] + mm_tn(scaled, wv_ref[:, cut])
    tables = span_tables(table_refs, place, 1)
    keys = rotated_narrow(nk_ref[...], tables) * NARROW_SCALE
    tails = jnp.where(low_lanes((SPAN, LANES)), tail[:, 3:4], tail[:, 4:5])
    own = mm_tn((keys * tails).astype(BF16), nv_ref[...])
    square = (LANES, LANES)
    own = jnp.where(low_rows(square) == low_lanes(square), own, 0.0)
    keeps = jnp.where(low_rows(square), kept[3:4, :], kept[4:5, :])
    state_ref[384:512, :] = state_ref[384:512, :] * keeps + own
    decay_ref[...] += jnp.broadcast_to(last, decay_ref.shape)

    @pl.when(span == SPANS - 1)
    def _():
        sums = decay_ref[...]
        high, low = in_two(sums)
        for part, head in enumerate(SLICE_HEADS):
            message_ref[part, 0:64] = state_ref[part * 64 : part * 64 + 64, :].astype(BF16)
            message_ref[part, 64:80] = log_rows(high[head : head + 1, :], low[head : head + 1, :])
        for copy in copies:
            copy.wait()


def plane_kernel(message_ref, out_ref, within_ref, logs_ref):
    carried = jnp.zeros((64, LANES), F32)
    logs = jnp.zeros((1, LANES), F32)
    for k in range(8):
        within_ref[k] = carried
        logs_ref[k] = jnp.broadcast_to(logs, (8, LANES))
        piece = message_ref[k].astype(F32)
        log = piece[64:65, :] + piece[65:66, :]
        carried = carried * jnp.exp(log) + piece[0:64, :]
        logs = logs + log
    ends = log_rows(*in_two(logs))
    for k in range(8):
        out_ref[k, 0:64] = carried.astype(BF16)
        out_ref[k, 64:80] = ends


def prefix_kernel(index_ref, planes_ref, within_ref, logs_ref, out_ref):
    plane = index_ref[0] // 8
    carried = jnp.zeros((64, LANES), F32)
    for k in range(7):
        piece = planes_ref[k].astype(F32)
        log = piece[64:65, :] + piece[65:66, :]
        carried = jnp.where(k < plane, carried * jnp.exp(log) + piece[0:64, :], carried)
    for k in range(8):
        out_ref[k] = (carried * jnp.exp(logs_ref[k, 0:1, :]) + within_ref[k]).astype(BF16)


def gated(output, gate, scale):
    gate = gate.astype(F32)
    return (output * scale * (gate / (1.0 + jnp.exp(-gate)))).astype(BF16)


def finish_kernel(
    index_ref, turn_ref, wq_ref, wk_ref, wv_ref, wg_ref, nq_ref, nk_ref, nv_ref, ng_ref, wd_ref, nd_ref,
    inside_ref, upper_ref, lower_ref, before_ref, earlier_ref, prefix_ref, wide_out_ref, narrow_out_ref,
    *out_refs, first,
):
    *out_refs, rows_ref, mixed_ref = out_refs
    span = turned_span(first + pl.program_id(0), turn_ref[0])
    place = index_ref[0] * SPANS + span
    table_refs = (inside_ref, upper_ref, lower_ref)
    total = running_decay(wd_ref, nd_ref, rows_ref)
    columns = total.T
    grown = jnp.exp(columns)
    earlier = jnp.exp(earlier_ref[0])
    square = (SPAN, SPAN)
    causal = lax.broadcasted_iota(jnp.int32, square, 0) >= lax.broadcasted_iota(jnp.int32, square, 1)

    def weights(scores, head):
        gaps = columns[:, head : head + 1] - total[head : head + 1, :]
        return (scores * jnp.exp(jnp.where(causal, gaps, -jnp.inf))).astype(BF16)

    tables = span_tables(table_refs, place, 0)
    for head in range(3):
        cut = slice(head * 128, head * 128 + 128)
        queries = rotated_wide(wq_ref[:, cut], tables).astype(BF16)
        keys = (rotated_wide(wk_ref[:, cut], tables) * WIDE_SCALE).astype(BF16)
        within = mm(weights(mm_nt(queries, keys), head), wv_ref[:, cut])
        entering = (
            prefix_ref[cut, :].astype(F32) * earlier[head : head + 1, :] + before_ref[0, cut, :]
        ).astype(BF16)
        output = within + mm(queries, entering) * grown[:, head : head + 1]
        scale = lax.rsqrt(jnp.mean(output * output, axis=-1, keepdims=True) + EPS)
        mixed_ref[:, cut] = gated(output, wg_ref[:, cut], scale)

    tables = span_tables(table_refs, place, 1)
    queries = rotated_narrow(nq_ref[...], tables).astype(BF16)
    keys = (rotated_narrow(nk_ref[...], tables) * NARROW_SCALE).astype(BF16)
    values = nv_ref[...]
    low = low_lanes(square)
    none = jnp.zeros_like(queries)
    within = jnp.where(
        low,
        mm(weights(mm_nt(jnp.where(low, queries, none), keys), 3), values),
        mm(weights(mm_nt(jnp.where(low, none, queries), keys), 4), values),
    )
    fades = jnp.where(low_rows(square), earlier[3:4, :], earlier[4:5, :])
    entering = (prefix_ref[384:512, :].astype(F32) * fades + before_ref[0, 384:512, :]).astype(BF16)
    output = within + mm(queries, entering) * jnp.where(low, grown[:, 3:4], grown[:, 4:5])
    squares = output * output
    left = jnp.sum(jnp.where(low, squares, 0.0), axis=-1, keepdims=True)
    right = jnp.sum(jnp.where(low, 0.0, squares), axis=-1, keepdims=True)
    scale = lax.rsqrt(jnp.where(low, left, right) * (1.0 / 64.0) + EPS)
    mixed_ref[:, 384:512] = gated(output, ng_ref[...], scale)

    projected = (
        mm(mixed_ref[:, 0:384], wide_out_ref[...]) + mm(mixed_ref[:, 384:512], narrow_out_ref[...])
    ).astype(BF16)
    if len(out_refs) == 2:
        half = SPAN // 2
        out_refs[0][...] = projected[:half]
        out_refs[1][...] = projected[half:]
    else:
        out_refs[0][0] = projected


def join_kernel(minus_ref, plus_ref, from_below_ref, from_above_ref, minus_out_ref, plus_out_ref):
    part = pl.program_id(0)

    @pl.when(part == 0)
    def _():
        minus_out_ref[...] = minus_ref[...]
        plus_out_ref[...] = (plus_ref[...].astype(F32) + from_below_ref[...].astype(F32)).astype(BF16)

    @pl.when(part == 1)
    def _():
        minus_out_ref[...] = (minus_ref[...].astype(F32) + from_above_ref[...].astype(F32)).astype(BF16)
        plus_out_ref[...] = plus_ref[...]


def rms(values, gain):
    return values * lax.rsqrt(jnp.mean(values * values, axis=-1, keepdims=True) + EPS) * gain


def norms_kernel(
    own_ref, below_ref, above_ref, residual_ref, mix_ref, pre_ref, updated_ref, low_ref, high_ref
):
    projected = own_ref[...].astype(F32) + below_ref[...].astype(F32) + above_ref[...].astype(F32)
    updated = (residual_ref[...].astype(F32) + rms(projected, mix_ref[...])).astype(BF16)
    updated_ref[...] = updated
    normed = rms(updated.astype(F32), pre_ref[...]).astype(BF16)

    @pl.when(pl.program_id(0) == 0)
    def _():
        low_ref[...] = normed

    @pl.when(pl.program_id(0) == 1)
    def _():
        high_ref[...] = normed


def tail_join_kernel(plus_ref, minus_ref, from_below_ref, from_above_ref, plus_out_ref, minus_out_ref):
    plus_out_ref[...] = (plus_ref[...].astype(F32) + from_below_ref[...].astype(F32)).astype(BF16)
    minus_out_ref[...] = (minus_ref[...].astype(F32) + from_above_ref[...].astype(F32)).astype(BF16)


def result_kernel(
    own_ref, below_low_ref, below_high_ref, above_low_ref, above_high_ref,
    updated_ref, gain_ref, out_ref,
):
    half = below_low_ref.shape[0]
    lowered = [
        own_ref[part].astype(F32) + below[...].astype(F32) + above[...].astype(F32)
        for part, below, above in (
            (slice(0, half), below_low_ref, above_low_ref),
            (slice(half, 2 * half), below_high_ref, above_high_ref),
        )
    ]
    lowered = jnp.concatenate(lowered, axis=0).T
    out_ref[...] = (updated_ref[...].astype(F32) + rms(lowered, gain_ref[...])).astype(BF16)


def up_block(x_ref, up_ref, at, block):
    weight = up_ref[:, :, pl.ds(at, block)].reshape(-1, block)
    rectified = jnp.maximum(mm(x_ref[...], weight), 0.0)
    return (rectified * rectified).astype(BF16).T


def down_block(down_ref, hidden_ref, k, group):
    weight = down_ref[pl.ds(k * group, group)].reshape(-1, hidden_ref.shape[0])
    return mm(weight, hidden_ref[...]).astype(BF16)


def far_mixer_kernel(*refs, ups, downs):
    halves, refs = refs[:2], refs[2:]
    both_ref, up_ref, down_ref, low_ref, high_ref, x_ref, hidden_ref, sems = refs
    devices, share, units = up_ref.shape
    half = halves[0].shape[0]
    block = units // ups
    group = devices // downs
    lines = group * share

    def up_copy(k):
        at = pl.multiple_of(k * block, block)
        return pltpu.make_async_copy(
            both_ref.at[:, 0, :, pl.ds(at, block)], up_ref.at[:, :, pl.ds(at, block)], sems.at[k]
        )

    def down_copy(k):
        at = k * group
        return pltpu.make_async_copy(
            both_ref.at[pl.ds(at, group), 1], down_ref.at[pl.ds(at, group)], sems.at[ups + k]
        )

    for k in range(ups):
        up_copy(k).start()
    for k in range(downs):
        down_copy(k).start()
    for k, ref in enumerate(halves):
        x_ref[k * half : (k + 1) * half] = ref[...]

    @pl.loop(0, ups)
    def _(k):
        up_copy(k).wait()
        at = pl.multiple_of(k * block, block)
        hidden_ref[pl.ds(at, block), :] = up_block(x_ref, up_ref, at, block)

    def lower(k, far_ref, base):
        down_copy(k).wait()
        lowered = down_block(down_ref, hidden_ref, k, group)
        far_ref[pl.ds(pl.multiple_of((k - base) * lines, lines), lines), :] = lowered

    @pl.loop(0, downs // 2)
    def _(k):
        lower(k, low_ref, 0)

    @pl.loop(downs // 2, downs)
    def _(k):
        lower(k, high_ref, downs // 2)


def near_mixer_kernel(*refs, ups, downs):
    halves, refs = refs[:4], refs[4:]
    up_ref, down_ref, minus_low_ref, minus_high_ref, plus_low_ref, plus_high_ref, x_ref, hidden_ref = refs
    devices, share, units = up_ref.shape
    half = halves[0].shape[0]
    rows = 2 * half
    block = units // ups
    group = devices // downs
    lines = group * share
    for k, ref in enumerate(halves):
        x_ref[k * half : (k + 1) * half] = ref[...]

    @pl.loop(0, ups)
    def _(k):
        at = pl.multiple_of(k * block, block)
        hidden_ref[pl.ds(at, block), :] = up_block(x_ref, up_ref, at, block)

    for first, minus_ref, plus_ref in (
        (0, minus_low_ref, plus_low_ref), (downs // 2, minus_high_ref, plus_high_ref)
    ):
        for k in range(downs // 2):
            lowered = down_block(down_ref, hidden_ref, first + k, group)
            at = slice(k * lines, (k + 1) * lines)
            minus_ref[at, :] = lowered[:, :rows]
            plus_ref[at, :] = lowered[:, rows:]


def own_mixer_kernel(first_ref, second_ref, up_ref, down_ref, out_ref, x_ref, hidden_ref, *, parts):
    devices, share, units = up_ref.shape
    half = first_ref.shape[0]
    x_ref[:half] = first_ref[...]
    x_ref[half:] = second_ref[...]
    hidden_ref[...] = up_block(x_ref, up_ref, 0, units)
    group = devices // parts
    lines = group * share
    for k in range(parts):
        out_ref[k * lines : (k + 1) * lines, :] = down_block(down_ref, hidden_ref, k, group)


SMALL = pltpu.CompilerParams(vmem_limit_bytes=16 * 1024 * 1024)


def shifted(array, axis, by):
    size = lax.axis_size(axis)
    return lax.ppermute(array, axis, [(k, (k + by) % size) for k in range(size)])


def joined(minus, plus, from_below, from_above, picks=(None, None)):
    half, width = from_below.shape
    flat = pl.BlockSpec((half, width), lambda i: (i, 0))
    kept = pl.BlockSpec((half, width), lambda i: (0, 0))
    out = jax.ShapeDtypeStruct((2 * half, width), BF16)

    def source(pick):
        if pick is None:
            return flat
        return pl.BlockSpec((None, half, width), lambda i: (pick, i, 0))

    return pl.pallas_call(
        join_kernel,
        out_shape=(out, out),
        grid=(2,),
        in_specs=[source(picks[0]), source(picks[1]), kept, kept],
        out_specs=[flat, flat],
        compiler_params=SMALL,
        name="join",
        cost_estimate=pl.CostEstimate(flops=1_000_000, bytes_accessed=3_500_000, transcendentals=0),
    )(minus, plus, from_below, from_above)


def local(
    wide_query, wide_key, wide_value, wide_gate,
    narrow_query, narrow_key, narrow_value, narrow_gate,
    wide_decay, narrow_decay, residual, wide_out, narrow_out,
    up_weight, down_weight, gain_mix, gain_pre, gain_mlp,
):
    devices = lax.axis_size(SP)
    ranks = lax.axis_size("tp")
    length, width = wide_query.shape[0], residual.shape[1]
    rows = residual.shape[0]
    share = up_weight.shape[0]
    units = up_weight.shape[1]

    both = lax.all_gather(
        jnp.concatenate([up_weight, down_weight.T], axis=0), SP, axis=0, tiled=True
    ).reshape(devices, 2, share, units)

    tables = [jnp.asarray(t) for t in position_tables(devices)]
    scalars = [
        lax.axis_index(SP).astype(jnp.int32).reshape(1),
        lax.axis_index("tp").astype(jnp.int32).reshape(1),
    ]
    table_blocks = [pl.BlockSpec(t.shape, lambda s, i, t: (0, 0, 0)) for t in tables]

    def span_blocks(at):
        return (
            pl.BlockSpec((SPAN, 384), lambda s, i, t: (at(s, i, t), 0)),
            pl.BlockSpec((SPAN, 128), lambda s, i, t: (at(s, i, t), 0)),
            [
                pl.BlockSpec((3, SPAN), lambda s, i, t: (0, at(s, i, t))),
                pl.BlockSpec((2, SPAN), lambda s, i, t: (0, at(s, i, t))),
            ],
            [
                pl.BlockSpec((1, 512, LANES), lambda s, i, t: (at(s, i, t), 0, 0)),
                pl.BlockSpec((1, 8, LANES), lambda s, i, t: (at(s, i, t), 0, 0)),
            ],
        )

    wide_block, narrow_block, decay_blocks, state_blocks = span_blocks(lambda s, i, t: s)
    staged = (
        *tables, wide_decay, narrow_decay, wide_query, wide_key, wide_value, wide_gate,
        narrow_query, narrow_key, narrow_value, narrow_gate, wide_out, narrow_out,
    )
    before, earlier, message, *held = pl.pallas_call(
        functools.partial(states_kernel, staged=len(staged)),
        out_shape=(
            jax.ShapeDtypeStruct((SPANS, 512, LANES), F32),
            jax.ShapeDtypeStruct((SPANS, 8, LANES), F32),
            jax.ShapeDtypeStruct((8, 80, LANES), BF16),
            *(pltpu.VMEM(x.shape, x.dtype) for x in staged),
        ),
        grid_spec=pltpu.PrefetchScalarGridSpec(
            num_scalar_prefetch=2,
            grid=(SPANS,),
            in_specs=[
                wide_block, wide_block, narrow_block, narrow_block, *decay_blocks, *table_blocks,
                *([pl.BlockSpec(memory_space=pltpu.HBM)] * len(staged)),
            ],
            out_specs=[
                *state_blocks,
                pl.BlockSpec((8, 80, LANES), lambda s, i, t: (0, 0, 0)),
                *([pl.BlockSpec(memory_space=pltpu.VMEM)] * len(staged)),
            ],
            scratch_shapes=[
                pltpu.VMEM((8, LANES), F32),
                pltpu.VMEM((512, LANES), F32),
                pltpu.VMEM((8, LANES), F32),
                pltpu.SemaphoreType.DMA((len(staged),)),
            ],
        ),
        compiler_params=SMALL,
        name="states",
        cost_estimate=pl.CostEstimate(flops=60_000_000, bytes_accessed=2_500_000, transcendentals=20_000),
    )(
        *scalars,
        *(
            pltpu.with_memory_space_constraint(x, pltpu.HBM)
            for x in (
                wide_key, wide_value, narrow_key, narrow_value,
                wide_decay, narrow_decay, *tables, *staged,
            )
        ),
    )

    arrived = lax.all_to_all(message, SP[1:], 0, 0, tiled=True)
    planes, within, logs = pl.pallas_call(
        plane_kernel,
        out_shape=(
            jax.ShapeDtypeStruct((8, 80, LANES), BF16),
            jax.ShapeDtypeStruct((8, 64, LANES), F32),
            jax.ShapeDtypeStruct((8, 8, LANES), F32),
        ),
        compiler_params=SMALL,
        name="plane",
        cost_estimate=pl.CostEstimate(flops=300_000, bytes_accessed=600_000, transcendentals=8_000),
    )(arrived)
    planes = lax.all_to_all(planes, SP[0], 0, 0, tiled=True)
    whole = pl.BlockSpec(memory_space=pltpu.VMEM)
    prefixes = pl.pallas_call(
        prefix_kernel,
        out_shape=jax.ShapeDtypeStruct((8, 64, LANES), BF16),
        in_specs=[pl.BlockSpec(memory_space=pltpu.SMEM), whole, whole, whole],
        out_specs=whole,
        compiler_params=SMALL,
        name="prefix",
        cost_estimate=pl.CostEstimate(flops=300_000, bytes_accessed=600_000, transcendentals=8_000),
    )(scalars[0], planes, within, logs)
    prefix = lax.all_to_all(prefixes, SP[1:], 0, 0, tiled=True).reshape(512, LANES)

    def finish(first, count, out_shape, out_specs):
        wide, narrow, decays, states = span_blocks(lambda s, i, t: turned_span(first + s, t[0]))
        return pl.pallas_call(
            functools.partial(finish_kernel, first=first),
            out_shape=out_shape,
            grid_spec=pltpu.PrefetchScalarGridSpec(
                num_scalar_prefetch=2,
                grid=(count,),
                in_specs=[
                    wide, wide, wide, wide, narrow, narrow, narrow, narrow,
                    *decays, *table_blocks, *states,
                    pl.BlockSpec((512, LANES), lambda s, i, t: (0, 0)),
                    pl.BlockSpec((384, width), lambda s, i, t: (0, 0)),
                    pl.BlockSpec((128, width), lambda s, i, t: (0, 0)),
                ],
                out_specs=out_specs,
                scratch_shapes=[pltpu.VMEM((8, LANES), F32), pltpu.VMEM((SPAN, 512), BF16)],
            ),
            compiler_params=SMALL,
            name="finish" if first else "finish_far",
            cost_estimate=pl.CostEstimate(
                flops=350_000_000 * count,
                bytes_accessed=3_000_000 + 1_500_000 * count,
                transcendentals=150_000 * count,
            ),
        )(
            *scalars, *held[5:13], *held[3:5], *held[:3], before, earlier, prefix, *held[13:],
        )

    half = rows // 2
    half_out = jax.ShapeDtypeStruct((half, width), BF16)
    near_out = jax.ShapeDtypeStruct((3, rows, width), BF16)
    low, high = finish(
        0, 1, (half_out, half_out), [pl.BlockSpec((half, width), lambda s, i, t: (0, 0))] * 2
    )
    low, high = shifted(low, "tp", 1), shifted(high, "tp", -1)
    (near,) = finish(
        1, 3, (near_out,), [pl.BlockSpec((1, rows, width), lambda s, i, t: (s, 0, 0))]
    )
    minus, plus = joined(near, near, low, high, (1, 2))
    below, above = shifted(plus, "tp", 1), shifted(minus, "tp", -1)
    flat = pl.BlockSpec((half, width), lambda i: (i, 0))
    kept = pl.BlockSpec((half, width), lambda i: (0, 0))
    gain = pl.BlockSpec((1, width), lambda i: (0, 0))
    updated, low, high = pl.pallas_call(
        norms_kernel,
        out_shape=[jax.ShapeDtypeStruct((rows, width), BF16), half_out, half_out],
        grid=(2,),
        in_specs=[
            pl.BlockSpec((None, half, width), lambda i: (0, i, 0)), flat, flat, flat, gain, gain,
        ],
        out_specs=[flat, kept, kept],
        compiler_params=SMALL,
        name="norms",
        cost_estimate=pl.CostEstimate(flops=4_000_000, bytes_accessed=3_500_000, transcendentals=300),
    )(near, below, above, residual, gain_mix.reshape(1, width), gain_pre.reshape(1, width))
    below_low, above_high = shifted(low, "tp", 1), shifted(high, "tp", -1)
    below_high, above_low = shifted(high, "tp", 1), shifted(low, "tp", -1)
    far_low, far_high = shifted(below_low, "tp", 1), shifted(above_high, "tp", -1)

    ups, downs = 4, 4
    turned = pltpu.VMEM((width, rows), BF16)
    turned_half = pltpu.VMEM((width // 2, rows), BF16)
    weights = pltpu.VMEM((devices, share, units), BF16)
    scratch = [pltpu.VMEM((2 * rows, width), BF16), pltpu.VMEM((units, 2 * rows), BF16)]
    scratch_half = [pltpu.VMEM((rows, width), BF16), pltpu.VMEM((units, rows), BF16)]
    own_low, own_high = low, high
    up, down, low, high = pl.pallas_call(
        functools.partial(far_mixer_kernel, ups=ups, downs=downs),
        out_shape=(weights, weights, turned_half, turned_half),
        in_specs=[*([whole] * 2), pl.BlockSpec(memory_space=pltpu.HBM)],
        out_specs=[whole] * 4,
        scratch_shapes=[*scratch_half, pltpu.SemaphoreType.DMA((ups + downs,))],
        compiler_params=SMALL,
        name="mixer_far",
        cost_estimate=pl.CostEstimate(
            flops=4 * rows * width * units, bytes_accessed=20_000_000, transcendentals=0
        ),
    )(far_low, far_high, pltpu.with_memory_space_constraint(both, pltpu.HBM))
    low, high = shifted(low, "tp", 1), shifted(high, "tp", -1)
    minus_low, minus_high, plus_low, plus_high = pl.pallas_call(
        functools.partial(near_mixer_kernel, ups=1, downs=2),
        out_shape=(turned_half,) * 4,
        in_specs=[whole] * 6,
        out_specs=[whole] * 4,
        scratch_shapes=scratch,
        compiler_params=SMALL,
        name="mixer_near",
        cost_estimate=pl.CostEstimate(
            flops=8 * rows * width * units, bytes_accessed=2_000_000, transcendentals=0
        ),
    )(below_low, below_high, above_low, above_high, up, down)
    below_high, above_low = shifted(plus_high, "tp", 1), shifted(minus_low, "tp", -1)
    plus_low, minus_high = pl.pallas_call(
        tail_join_kernel,
        out_shape=(turned_half,) * 2,
        in_specs=[whole] * 4,
        out_specs=[whole] * 2,
        compiler_params=SMALL,
        name="tail_join",
        cost_estimate=pl.CostEstimate(flops=500_000, bytes_accessed=1_500_000, transcendentals=0),
    )(plus_low, minus_high, low, high)
    below_low, above_high = shifted(plus_low, "tp", 1), shifted(minus_high, "tp", -1)
    own_low, _ = lax.optimization_barrier((own_low, plus_low))
    own = pl.pallas_call(
        functools.partial(own_mixer_kernel, parts=2),
        out_shape=turned,
        in_specs=[whole] * 4,
        out_specs=whole,
        scratch_shapes=scratch_half,
        compiler_params=SMALL,
        name="mixer_own",
        cost_estimate=pl.CostEstimate(
            flops=4 * rows * width * units, bytes_accessed=2_000_000, transcendentals=0
        ),
    )(own_low, own_high, up, down)
    return pl.pallas_call(
        result_kernel,
        out_shape=jax.ShapeDtypeStruct((rows, width), BF16),
        compiler_params=SMALL,
        name="result",
        cost_estimate=pl.CostEstimate(flops=4_000_000, bytes_accessed=3_500_000, transcendentals=300),
    )(
        own, below_low, below_high, above_low, above_high, updated, gain_mlp.reshape(1, width)
    )


def solution(mesh):
    finer = Mesh(mesh.devices.reshape(8, 4, 2, mesh.shape["tp"]), ("sp_0", "sp_1", "sp_2", "tp"))
    in_specs = (
        *([P(SP, "tp")] * 8),
        P("tp", SP),
        P("tp", SP),
        P(SP_TP, None),
        P("tp", None),
        P("tp", None),
        P(SP, "tp"),
        P("tp", SP),
        P(),
        P(),
        P(),
    )
    return jax.shard_map(
        local, mesh=finer, in_specs=in_specs, out_specs=P(SP_TP, None), check_vma=False
    )
```

```python
import functools

import jax
import jax.numpy as jnp
import numpy as np
from jax import lax
from jax.experimental import pallas as pl
from jax.experimental.pallas import tpu as pltpu
from jax.sharding import Mesh
from jax.sharding import PartitionSpec as P

SPAN = 128
LANES = 128
SPANS = 4
SPAN_PART = 16
SLICE_HEADS = (0, 0, 1, 1, 2, 2, 3, 4)
SP = ("sp_0", "sp_1", "sp_2")
SP_TP = ("sp_0", "sp_1", "sp_2", "tp")
EPS = 1e-06
WIDE_SCALE = 128 ** (-0.5)
NARROW_SCALE = 64 ** (-0.5)
F32 = jnp.float32
BF16 = jnp.bfloat16


def position_tables(devices):
    lane = np.arange(LANES)
    inside, upper, lower = [], [], []
    for head_dim in (128, 64):
        half = head_dim // 2
        rate = 10000.0 ** (-2.0 * (lane % half) / head_dim)
        sign = np.where(lane % head_dim < half, -1.0, 1.0)
        for table, positions in (
            (inside, np.arange(SPAN)),
            (upper, np.arange(devices * SPANS // SPAN_PART) * SPAN_PART * SPAN),
            (lower, np.arange(SPAN_PART) * SPAN),
        ):
            angles = positions[:, None] * rate
            table += [np.cos(angles), np.sin(angles) * sign]
    return [np.stack(t).astype(np.float32) for t in (inside, upper, lower)]


def turned_by(first, second):
    return (
        first[0] * second[0] - first[1] * second[1],
        first[1] * second[0] + first[0] * second[1],
    )


def span_tables(table_refs, block, group):
    inside_ref, upper_ref, lower_ref = table_refs
    start = turned_by(
        *(
            [ref[2 * group + k, pl.ds(at, 1), :] for k in range(2)]
            for ref, at in ((upper_ref, block // SPAN_PART), (lower_ref, block % SPAN_PART))
        )
    )
    return turned_by((inside_ref[2 * group], inside_ref[2 * group + 1]), start)


def rotated_wide(x, tables):
    x = x.astype(F32)
    return x * tables[0] + pltpu.roll(x, 64, 1) * tables[1]


def rotated_narrow(x, tables):
    x = x.astype(F32)
    lane = lax.broadcasted_iota(jnp.int32, x.shape, 1)
    partner = jnp.where((lane & 32) == 0, pltpu.roll(x, 96, 1), pltpu.roll(x, 32, 1))
    return x * tables[0] + partner * tables[1]


def running_decay(wide_decay_ref, narrow_decay_ref, rows_ref):
    rows_ref[...] = jnp.zeros_like(rows_ref)
    rows_ref[0:3, :] = wide_decay_ref[...]
    rows_ref[3:5, :] = narrow_decay_ref[...]
    x = rows_ref[...]
    lane = lax.broadcasted_iota(jnp.int32, x.shape, 1)
    step = 1
    while step < SPAN:
        x = x + jnp.where(lane >= step, pltpu.roll(x, step, 1), 0.0)
        step *= 2
    return x


def low_rows(shape):
    return lax.broadcasted_iota(jnp.int32, shape, 0) < 64


def low_lanes(shape):
    return lax.broadcasted_iota(jnp.int32, shape, 1) < 64


def mm(a, b):
    return jnp.dot(a, b, preferred_element_type=F32)


def mm_nt(a, b):
    return lax.dot_general(a, b, (((1,), (1,)), ((), ())), preferred_element_type=F32)


def mm_tn(a, b):
    return lax.dot_general(a, b, (((0,), (0,)), ((), ())), preferred_element_type=F32)


def in_two(values):
    high = values.astype(BF16).astype(F32)
    return high, values - high


def log_rows(high, low):
    sub = lax.broadcasted_iota(jnp.int32, (16, LANES), 0)
    return jnp.where(sub == 0, high, jnp.where(sub == 1, low, 0.0)).astype(BF16)


def turned_span(place, turn):
    return (turn + jnp.where(place == 0, 2, jnp.where(place == 3, 1, jnp.where(place == 2, 3, 0)))) & 3


def states_kernel(
    index_ref, _, wk_ref, wv_ref, nk_ref, nv_ref, wd_ref, nd_ref, *refs, staged,
):
    table_refs, refs = refs[:3], refs[3:]
    sources, refs = refs[:staged], refs[staged:]
    before_ref, earlier_ref, message_ref = refs[:3]
    targets, refs = refs[3 : 3 + staged], refs[3 + staged :]
    rows_ref, state_ref, decay_ref, sems = refs
    span = pl.program_id(0)
    place = index_ref[0] * SPANS + span
    copies = [pltpu.make_async_copy(a, b, sems.at[k]) for k, (a, b) in enumerate(zip(sources, targets))]

    @pl.when(span == 0)
    def _():
        for copy in copies:
            copy.start()
        state_ref[...] = jnp.zeros_like(state_ref)
        decay_ref[...] = jnp.zeros_like(decay_ref)

    total = running_decay(wd_ref, nd_ref, rows_ref)
    last = total[:, SPAN - 1 : SPAN]
    tail = jnp.exp(last - total).T
    kept = jnp.exp(last)
    before_ref[0] = state_ref[...]
    earlier_ref[0] = decay_ref[...]
    tables = span_tables(table_refs, place, 0)
    for head in range(3):
        cut = slice(head * 128, head * 128 + 128)
        keys = rotated_wide(wk_ref[:, cut], tables) * WIDE_SCALE
        scaled = (keys * tail[:, head : head + 1]).astype(BF16)
        state_ref[cut, :] = state_ref[cut, :] * kept[head : head + 1, :] + mm_tn(scaled, wv_ref[:, cut])
    tables = span_tables(table_refs, place, 1)
    keys = rotated_narrow(nk_ref[...], tables) * NARROW_SCALE
    tails = jnp.where(low_lanes((SPAN, LANES)), tail[:, 3:4], tail[:, 4:5])
    own = mm_tn((keys * tails).astype(BF16), nv_ref[...])
    square = (LANES, LANES)
    own = jnp.where(low_rows(square) == low_lanes(square), own, 0.0)
    keeps = jnp.where(low_rows(square), kept[3:4, :], kept[4:5, :])
    state_ref[384:512, :] = state_ref[384:512, :] * keeps + own
    decay_ref[...] += jnp.broadcast_to(last, decay_ref.shape)

    @pl.when(span == SPANS - 1)
    def _():
        sums = decay_ref[...]
        high, low = in_two(sums)
        for part, head in enumerate(SLICE_HEADS):
            message_ref[part, 0:64] = state_ref[part * 64 : part * 64 + 64, :].astype(BF16)
            message_ref[part, 64:80] = log_rows(high[head : head + 1, :], low[head : head + 1, :])
        for copy in copies:
            copy.wait()


def plane_kernel(message_ref, out_ref, within_ref, logs_ref):
    carried = jnp.zeros((64, LANES), F32)
    logs = jnp.zeros((1, LANES), F32)
    for k in range(8):
        within_ref[k] = carried
        logs_ref[k] = jnp.broadcast_to(logs, (8, LANES))
        piece = message_ref[k].astype(F32)
        log = piece[64:65, :] + piece[65:66, :]
        carried = carried * jnp.exp(log) + piece[0:64, :]
        logs = logs + log
    ends = log_rows(*in_two(logs))
    for k in range(8):
        out_ref[k, 0:64] = carried.astype(BF16)
        out_ref[k, 64:80] = ends


def prefix_kernel(index_ref, planes_ref, within_ref, logs_ref, out_ref):
    plane = index_ref[0] // 8
    carried = jnp.zeros((64, LANES), F32)
    for k in range(7):
        piece = planes_ref[k].astype(F32)
        log = piece[64:65, :] + piece[65:66, :]
        carried = jnp.where(k < plane, carried * jnp.exp(log) + piece[0:64, :], carried)
    for k in range(8):
        out_ref[k] = (carried * jnp.exp(logs_ref[k, 0:1, :]) + within_ref[k]).astype(BF16)


def gated(output, gate, scale):
    gate = gate.astype(F32)
    return (output * scale * (gate / (1.0 + jnp.exp(-gate)))).astype(BF16)


def finish_kernel(
    index_ref, turn_ref, wq_ref, wk_ref, wv_ref, wg_ref, nq_ref, nk_ref, nv_ref, ng_ref, wd_ref, nd_ref,
    inside_ref, upper_ref, lower_ref, before_ref, earlier_ref, prefix_ref, wide_out_ref, narrow_out_ref,
    *out_refs, first,
):
    *out_refs, rows_ref, mixed_ref = out_refs
    span = turned_span(first + pl.program_id(0), turn_ref[0])
    place = index_ref[0] * SPANS + span
    table_refs = (inside_ref, upper_ref, lower_ref)
    total = running_decay(wd_ref, nd_ref, rows_ref)
    columns = total.T
    grown = jnp.exp(columns)
    earlier = jnp.exp(earlier_ref[0])
    square = (SPAN, SPAN)
    causal = lax.broadcasted_iota(jnp.int32, square, 0) >= lax.broadcasted_iota(jnp.int32, square, 1)

    def weights(scores, head):
        gaps = columns[:, head : head + 1] - total[head : head + 1, :]
        return (scores * jnp.exp(jnp.where(causal, gaps, -jnp.inf))).astype(BF16)

    tables = span_tables(table_refs, place, 0)
    for head in range(3):
        cut = slice(head * 128, head * 128 + 128)
        queries = rotated_wide(wq_ref[:, cut], tables).astype(BF16)
        keys = (rotated_wide(wk_ref[:, cut], tables) * WIDE_SCALE).astype(BF16)
        within = mm(weights(mm_nt(queries, keys), head), wv_ref[:, cut])
        entering = (
            prefix_ref[cut, :].astype(F32) * earlier[head : head + 1, :] + before_ref[0, cut, :]
        ).astype(BF16)
        output = within + mm(queries, entering) * grown[:, head : head + 1]
        scale = lax.rsqrt(jnp.mean(output * output, axis=-1, keepdims=True) + EPS)
        mixed_ref[:, cut] = gated(output, wg_ref[:, cut], scale)

    tables = span_tables(table_refs, place, 1)
    queries = rotated_narrow(nq_ref[...], tables).astype(BF16)
    keys = (rotated_narrow(nk_ref[...], tables) * NARROW_SCALE).astype(BF16)
    values = nv_ref[...]
    low = low_lanes(square)
    none = jnp.zeros_like(queries)
    within = jnp.where(
        low,
        mm(weights(mm_nt(jnp.where(low, queries, none), keys), 3), values),
        mm(weights(mm_nt(jnp.where(low, none, queries), keys), 4), values),
    )
    fades = jnp.where(low_rows(square), earlier[3:4, :], earlier[4:5, :])
    entering = (prefix_ref[384:512, :].astype(F32) * fades + before_ref[0, 384:512, :]).astype(BF16)
    output = within + mm(queries, entering) * jnp.where(low, grown[:, 3:4], grown[:, 4:5])
    squares = output * output
    left = jnp.sum(jnp.where(low, squares, 0.0), axis=-1, keepdims=True)
    right = jnp.sum(jnp.where(low, 0.0, squares), axis=-1, keepdims=True)
    scale = lax.rsqrt(jnp.where(low, left, right) * (1.0 / 64.0) + EPS)
    mixed_ref[:, 384:512] = gated(output, ng_ref[...], scale)

    projected = (
        mm(mixed_ref[:, 0:384], wide_out_ref[...]) + mm(mixed_ref[:, 384:512], narrow_out_ref[...])
    ).astype(BF16)
    if len(out_refs) == 2:
        half = SPAN // 2
        out_refs[0][...] = projected[:half]
        out_refs[1][...] = projected[half:]
    else:
        out_refs[0][0] = projected


def join_kernel(minus_ref, plus_ref, from_below_ref, from_above_ref, minus_out_ref, plus_out_ref):
    part = pl.program_id(0)

    @pl.when(part == 0)
    def _():
        minus_out_ref[...] = minus_ref[...]
        plus_out_ref[...] = (plus_ref[...].astype(F32) + from_below_ref[...].astype(F32)).astype(BF16)

    @pl.when(part == 1)
    def _():
        minus_out_ref[...] = (minus_ref[...].astype(F32) + from_above_ref[...].astype(F32)).astype(BF16)
        plus_out_ref[...] = plus_ref[...]


def rms(values, gain):
    return values * lax.rsqrt(jnp.mean(values * values, axis=-1, keepdims=True) + EPS) * gain


def norms_kernel(
    own_ref, below_ref, above_ref, residual_ref, mix_ref, pre_ref, updated_ref, low_ref, high_ref
):
    projected = own_ref[...].astype(F32) + below_ref[...].astype(F32) + above_ref[...].astype(F32)
    updated = (residual_ref[...].astype(F32) + rms(projected, mix_ref[...])).astype(BF16)
    updated_ref[...] = updated
    normed = rms(updated.astype(F32), pre_ref[...]).astype(BF16)

    @pl.when(pl.program_id(0) == 0)
    def _():
        low_ref[...] = normed

    @pl.when(pl.program_id(0) == 1)
    def _():
        high_ref[...] = normed


def tail_join_kernel(plus_ref, minus_ref, from_below_ref, from_above_ref, plus_out_ref, minus_out_ref):
    plus_out_ref[...] = (plus_ref[...].astype(F32) + from_below_ref[...].astype(F32)).astype(BF16)
    minus_out_ref[...] = (minus_ref[...].astype(F32) + from_above_ref[...].astype(F32)).astype(BF16)


def result_kernel(
    own_ref, below_low_ref, below_high_ref, above_low_ref, above_high_ref,
    updated_ref, gain_ref, out_ref,
):
    half = below_low_ref.shape[0]
    lowered = [
        own_ref[part].astype(F32) + below[...].astype(F32) + above[...].astype(F32)
        for part, below, above in (
            (slice(0, half), below_low_ref, above_low_ref),
            (slice(half, 2 * half), below_high_ref, above_high_ref),
        )
    ]
    lowered = jnp.concatenate(lowered, axis=0)
    scale = lax.rsqrt(jnp.mean(lowered * lowered, axis=0, keepdims=True) + EPS)
    scaled = (lowered * scale).astype(BF16).T.astype(F32)
    out_ref[...] = (updated_ref[...].astype(F32) + scaled * gain_ref[...]).astype(BF16)


def up_block(x_ref, up_ref, at, block):
    weight = up_ref[:, :, pl.ds(at, block)].reshape(-1, block)
    rectified = jnp.maximum(mm(x_ref[...], weight), 0.0)
    return (rectified * rectified).astype(BF16).T


def down_block(down_ref, hidden_ref, k, group):
    weight = down_ref[pl.ds(k * group, group)].reshape(-1, hidden_ref.shape[0])
    return mm(weight, hidden_ref[...]).astype(BF16)


def far_mixer_kernel(*refs, ups, downs):
    halves, refs = refs[:2], refs[2:]
    both_ref, up_ref, down_ref, low_ref, high_ref, x_ref, hidden_ref, total_ref, sems = refs
    devices, share, units = up_ref.shape
    half = halves[0].shape[0]
    band = devices // ups
    block = band * share
    group = devices // downs
    lines = group * share

    def up_copy(k):
        at = k * band
        return pltpu.make_async_copy(
            both_ref.at[pl.ds(at, band), 0], up_ref.at[pl.ds(at, band)], sems.at[k]
        )

    def down_copy(k):
        at = k * group
        return pltpu.make_async_copy(
            both_ref.at[pl.ds(at, group), 1], down_ref.at[pl.ds(at, group)], sems.at[ups + k]
        )

    for k in range(ups):
        up_copy(k).start()
    for k in range(downs):
        down_copy(k).start()
    for k, ref in enumerate(halves):
        x_ref[k * half : (k + 1) * half] = ref[...]

    for k in range(ups):
        up_copy(k).wait()
        weight = up_ref[k * band : (k + 1) * band].reshape(block, units)
        part = mm(x_ref[:, k * block : (k + 1) * block], weight)
        total_ref[...] = part if k == 0 else total_ref[...] + part
    rectified = jnp.maximum(total_ref[...], 0.0)
    hidden_ref[...] = (rectified * rectified).astype(BF16).T

    def lower(k, far_ref, base):
        down_copy(k).wait()
        lowered = down_block(down_ref, hidden_ref, k, group)
        far_ref[pl.ds(pl.multiple_of((k - base) * lines, lines), lines), :] = lowered

    @pl.loop(0, downs // 2)
    def _(k):
        lower(k, low_ref, 0)

    @pl.loop(downs // 2, downs)
    def _(k):
        lower(k, high_ref, downs // 2)


def near_mixer_kernel(*refs, ups, downs):
    halves, refs = refs[:4], refs[4:]
    up_ref, down_ref, minus_low_ref, minus_high_ref, plus_low_ref, plus_high_ref, x_ref, hidden_ref = refs
    devices, share, units = up_ref.shape
    half = halves[0].shape[0]
    rows = 2 * half
    block = units // ups
    group = devices // downs
    lines = group * share
    for k, ref in enumerate(halves):
        x_ref[k * half : (k + 1) * half] = ref[...]

    @pl.loop(0, ups)
    def _(k):
        at = pl.multiple_of(k * block, block)
        hidden_ref[pl.ds(at, block), :] = up_block(x_ref, up_ref, at, block)

    for first, minus_ref, plus_ref in (
        (0, minus_low_ref, plus_low_ref), (downs // 2, minus_high_ref, plus_high_ref)
    ):
        for k in range(downs // 2):
            lowered = down_block(down_ref, hidden_ref, first + k, group)
            at = slice(k * lines, (k + 1) * lines)
            minus_ref[at, :] = lowered[:, :rows]
            plus_ref[at, :] = lowered[:, rows:]


def own_mixer_kernel(first_ref, second_ref, up_ref, down_ref, out_ref, x_ref, hidden_ref, *, parts):
    devices, share, units = up_ref.shape
    half = first_ref.shape[0]
    x_ref[:half] = first_ref[...]
    x_ref[half:] = second_ref[...]
    hidden_ref[...] = up_block(x_ref, up_ref, 0, units)
    group = devices // parts
    lines = group * share
    for k in range(parts):
        out_ref[k * lines : (k + 1) * lines, :] = down_block(down_ref, hidden_ref, k, group)


SMALL = pltpu.CompilerParams(vmem_limit_bytes=16 * 1024 * 1024)


def shifted(array, axis, by):
    size = lax.axis_size(axis)
    return lax.ppermute(array, axis, [(k, (k + by) % size) for k in range(size)])


def joined(minus, plus, from_below, from_above, picks=(None, None)):
    half, width = from_below.shape
    flat = pl.BlockSpec((half, width), lambda i: (i, 0))
    kept = pl.BlockSpec((half, width), lambda i: (0, 0))
    out = jax.ShapeDtypeStruct((2 * half, width), BF16)

    def source(pick):
        if pick is None:
            return flat
        return pl.BlockSpec((None, half, width), lambda i: (pick, i, 0))

    return pl.pallas_call(
        join_kernel,
        out_shape=(out, out),
        grid=(2,),
        in_specs=[source(picks[0]), source(picks[1]), kept, kept],
        out_specs=[flat, flat],
        compiler_params=SMALL,
        name="join",
        cost_estimate=pl.CostEstimate(flops=1_000_000, bytes_accessed=3_500_000, transcendentals=0),
    )(minus, plus, from_below, from_above)


def local(
    wide_query, wide_key, wide_value, wide_gate,
    narrow_query, narrow_key, narrow_value, narrow_gate,
    wide_decay, narrow_decay, residual, wide_out, narrow_out,
    up_weight, down_weight, gain_mix, gain_pre, gain_mlp,
):
    devices = lax.axis_size(SP)
    ranks = lax.axis_size("tp")
    length, width = wide_query.shape[0], residual.shape[1]
    rows = residual.shape[0]
    share = up_weight.shape[0]
    units = up_weight.shape[1]

    both = lax.all_gather(
        jnp.concatenate([up_weight, down_weight.T], axis=0), SP, axis=0, tiled=True
    ).reshape(devices, 2, share, units)

    tables = [jnp.asarray(t) for t in position_tables(devices)]
    scalars = [
        lax.axis_index(SP).astype(jnp.int32).reshape(1),
        lax.axis_index("tp").astype(jnp.int32).reshape(1),
    ]
    table_blocks = [pl.BlockSpec(t.shape, lambda s, i, t: (0, 0, 0)) for t in tables]

    def span_blocks(at):
        return (
            pl.BlockSpec((SPAN, 384), lambda s, i, t: (at(s, i, t), 0)),
            pl.BlockSpec((SPAN, 128), lambda s, i, t: (at(s, i, t), 0)),
            [
                pl.BlockSpec((3, SPAN), lambda s, i, t: (0, at(s, i, t))),
                pl.BlockSpec((2, SPAN), lambda s, i, t: (0, at(s, i, t))),
            ],
            [
                pl.BlockSpec((1, 512, LANES), lambda s, i, t: (at(s, i, t), 0, 0)),
                pl.BlockSpec((1, 8, LANES), lambda s, i, t: (at(s, i, t), 0, 0)),
            ],
        )

    wide_block, narrow_block, decay_blocks, state_blocks = span_blocks(lambda s, i, t: s)
    staged = (
        *tables, wide_decay, narrow_decay, wide_query, wide_key, wide_value, wide_gate,
        narrow_query, narrow_key, narrow_value, narrow_gate, wide_out, narrow_out,
    )
    before, earlier, message, *held = pl.pallas_call(
        functools.partial(states_kernel, staged=len(staged)),
        out_shape=(
            jax.ShapeDtypeStruct((SPANS, 512, LANES), F32),
            jax.ShapeDtypeStruct((SPANS, 8, LANES), F32),
            jax.ShapeDtypeStruct((8, 80, LANES), BF16),
            *(pltpu.VMEM(x.shape, x.dtype) for x in staged),
        ),
        grid_spec=pltpu.PrefetchScalarGridSpec(
            num_scalar_prefetch=2,
            grid=(SPANS,),
            in_specs=[
                wide_block, wide_block, narrow_block, narrow_block, *decay_blocks, *table_blocks,
                *([pl.BlockSpec(memory_space=pltpu.HBM)] * len(staged)),
            ],
            out_specs=[
                *state_blocks,
                pl.BlockSpec((8, 80, LANES), lambda s, i, t: (0, 0, 0)),
                *([pl.BlockSpec(memory_space=pltpu.VMEM)] * len(staged)),
            ],
            scratch_shapes=[
                pltpu.VMEM((8, LANES), F32),
                pltpu.VMEM((512, LANES), F32),
                pltpu.VMEM((8, LANES), F32),
                pltpu.SemaphoreType.DMA((len(staged),)),
            ],
        ),
        compiler_params=SMALL,
        name="states",
        cost_estimate=pl.CostEstimate(flops=60_000_000, bytes_accessed=2_500_000, transcendentals=20_000),
    )(
        *scalars,
        *(
            pltpu.with_memory_space_constraint(x, pltpu.HBM)
            for x in (
                wide_key, wide_value, narrow_key, narrow_value,
                wide_decay, narrow_decay, *tables, *staged,
            )
        ),
    )

    arrived = lax.all_to_all(message, SP[1:], 0, 0, tiled=True)
    planes, within, logs = pl.pallas_call(
        plane_kernel,
        out_shape=(
            jax.ShapeDtypeStruct((8, 80, LANES), BF16),
            jax.ShapeDtypeStruct((8, 64, LANES), F32),
            jax.ShapeDtypeStruct((8, 8, LANES), F32),
        ),
        compiler_params=SMALL,
        name="plane",
        cost_estimate=pl.CostEstimate(flops=300_000, bytes_accessed=600_000, transcendentals=8_000),
    )(arrived)
    planes = lax.all_to_all(planes, SP[0], 0, 0, tiled=True)
    whole = pl.BlockSpec(memory_space=pltpu.VMEM)
    prefixes = pl.pallas_call(
        prefix_kernel,
        out_shape=jax.ShapeDtypeStruct((8, 64, LANES), BF16),
        in_specs=[pl.BlockSpec(memory_space=pltpu.SMEM), whole, whole, whole],
        out_specs=whole,
        compiler_params=SMALL,
        name="prefix",
        cost_estimate=pl.CostEstimate(flops=300_000, bytes_accessed=600_000, transcendentals=8_000),
    )(scalars[0], planes, within, logs)
    prefix = lax.all_to_all(prefixes, SP[1:], 0, 0, tiled=True).reshape(512, LANES)

    def finish(first, count, out_shape, out_specs):
        wide, narrow, decays, states = span_blocks(lambda s, i, t: turned_span(first + s, t[0]))
        return pl.pallas_call(
            functools.partial(finish_kernel, first=first),
            out_shape=out_shape,
            grid_spec=pltpu.PrefetchScalarGridSpec(
                num_scalar_prefetch=2,
                grid=(count,),
                in_specs=[
                    wide, wide, wide, wide, narrow, narrow, narrow, narrow,
                    *decays, *table_blocks, *states,
                    pl.BlockSpec((512, LANES), lambda s, i, t: (0, 0)),
                    pl.BlockSpec((384, width), lambda s, i, t: (0, 0)),
                    pl.BlockSpec((128, width), lambda s, i, t: (0, 0)),
                ],
                out_specs=out_specs,
                scratch_shapes=[pltpu.VMEM((8, LANES), F32), pltpu.VMEM((SPAN, 512), BF16)],
            ),
            compiler_params=SMALL,
            name="finish" if first else "finish_far",
            cost_estimate=pl.CostEstimate(
                flops=350_000_000 * count,
                bytes_accessed=3_000_000 + 1_500_000 * count,
                transcendentals=150_000 * count,
            ),
        )(
            *scalars, *held[5:13], *held[3:5], *held[:3], before, earlier, prefix, *held[13:],
        )

    half = rows // 2
    half_out = jax.ShapeDtypeStruct((half, width), BF16)
    near_out = jax.ShapeDtypeStruct((3, rows, width), BF16)
    low, high = finish(
        0, 1, (half_out, half_out), [pl.BlockSpec((half, width), lambda s, i, t: (0, 0))] * 2
    )
    low, high = shifted(low, "tp", 1), shifted(high, "tp", -1)
    (near,) = finish(
        1, 3, (near_out,), [pl.BlockSpec((1, rows, width), lambda s, i, t: (s, 0, 0))]
    )
    minus, plus = joined(near, near, low, high, (1, 2))
    below, above = shifted(plus, "tp", 1), shifted(minus, "tp", -1)
    flat = pl.BlockSpec((half, width), lambda i: (i, 0))
    kept = pl.BlockSpec((half, width), lambda i: (0, 0))
    gain = pl.BlockSpec((1, width), lambda i: (0, 0))
    updated, low, high = pl.pallas_call(
        norms_kernel,
        out_shape=[jax.ShapeDtypeStruct((rows, width), BF16), half_out, half_out],
        grid=(2,),
        in_specs=[
            pl.BlockSpec((None, half, width), lambda i: (0, i, 0)), flat, flat, flat, gain, gain,
        ],
        out_specs=[flat, kept, kept],
        compiler_params=SMALL,
        name="norms",
        cost_estimate=pl.CostEstimate(flops=4_000_000, bytes_accessed=3_500_000, transcendentals=300),
    )(near, below, above, residual, gain_mix.reshape(1, width), gain_pre.reshape(1, width))
    below_low, above_high = shifted(low, "tp", 1), shifted(high, "tp", -1)
    below_high, above_low = shifted(high, "tp", 1), shifted(low, "tp", -1)
    far_low, far_high = shifted(below_low, "tp", 1), shifted(above_high, "tp", -1)

    ups, downs = 4, 4
    turned = pltpu.VMEM((width, rows), BF16)
    turned_half = pltpu.VMEM((width // 2, rows), BF16)
    weights = pltpu.VMEM((devices, share, units), BF16)
    scratch = [pltpu.VMEM((2 * rows, width), BF16), pltpu.VMEM((units, 2 * rows), BF16)]
    scratch_half = [pltpu.VMEM((rows, width), BF16), pltpu.VMEM((units, rows), BF16)]
    own_low, own_high = low, high
    up, down, low, high = pl.pallas_call(
        functools.partial(far_mixer_kernel, ups=ups, downs=downs),
        out_shape=(weights, weights, turned_half, turned_half),
        in_specs=[*([whole] * 2), pl.BlockSpec(memory_space=pltpu.HBM)],
        out_specs=[whole] * 4,
        scratch_shapes=[
            *scratch_half, pltpu.VMEM((rows, units), F32), pltpu.SemaphoreType.DMA((ups + downs,)),
        ],
        compiler_params=SMALL,
        name="mixer_far",
        cost_estimate=pl.CostEstimate(
            flops=4 * rows * width * units, bytes_accessed=20_000_000, transcendentals=0
        ),
    )(far_low, far_high, pltpu.with_memory_space_constraint(both, pltpu.HBM))
    low, high = shifted(low, "tp", 1), shifted(high, "tp", -1)
    minus_low, minus_high, plus_low, plus_high = pl.pallas_call(
        functools.partial(near_mixer_kernel, ups=1, downs=2),
        out_shape=(turned_half,) * 4,
        in_specs=[whole] * 6,
        out_specs=[whole] * 4,
        scratch_shapes=scratch,
        compiler_params=SMALL,
        name="mixer_near",
        cost_estimate=pl.CostEstimate(
            flops=8 * rows * width * units, bytes_accessed=2_000_000, transcendentals=0
        ),
    )(below_low, below_high, above_low, above_high, up, down)
    below_high, above_low = shifted(plus_high, "tp", 1), shifted(minus_low, "tp", -1)
    plus_low, minus_high = pl.pallas_call(
        tail_join_kernel,
        out_shape=(turned_half,) * 2,
        in_specs=[whole] * 4,
        out_specs=[whole] * 2,
        compiler_params=SMALL,
        name="tail_join",
        cost_estimate=pl.CostEstimate(flops=500_000, bytes_accessed=1_500_000, transcendentals=0),
    )(plus_low, minus_high, low, high)
    below_low, above_high = shifted(plus_low, "tp", 1), shifted(minus_high, "tp", -1)
    own_low, _ = lax.optimization_barrier((own_low, plus_low))
    own = pl.pallas_call(
        functools.partial(own_mixer_kernel, parts=2),
        out_shape=turned,
        in_specs=[whole] * 4,
        out_specs=whole,
        scratch_shapes=scratch_half,
        compiler_params=SMALL,
        name="mixer_own",
        cost_estimate=pl.CostEstimate(
            flops=4 * rows * width * units, bytes_accessed=2_000_000, transcendentals=0
        ),
    )(own_low, own_high, up, down)
    return pl.pallas_call(
        result_kernel,
        out_shape=jax.ShapeDtypeStruct((rows, width), BF16),
        compiler_params=SMALL,
        name="result",
        cost_estimate=pl.CostEstimate(flops=4_000_000, bytes_accessed=3_500_000, transcendentals=300),
    )(
        own, below_low, below_high, above_low, above_high, updated, gain_mlp.reshape(1, width)
    )


def solution(mesh):
    finer = Mesh(mesh.devices.reshape(8, 4, 2, mesh.shape["tp"]), ("sp_0", "sp_1", "sp_2", "tp"))
    in_specs = (
        *([P(SP, "tp")] * 8),
        P("tp", SP),
        P("tp", SP),
        P(SP_TP, None),
        P("tp", None),
        P("tp", None),
        P(SP, "tp"),
        P("tp", SP),
        P(),
        P(),
        P(),
    )
    return jax.shard_map(
        local, mesh=finer, in_specs=in_specs, out_specs=P(SP_TP, None), check_vma=False
    )
```

```python
import functools

import jax
import jax.numpy as jnp
import numpy as np
from jax import lax
from jax.experimental import pallas as pl
from jax.experimental.pallas import tpu as pltpu
from jax.sharding import Mesh
from jax.sharding import PartitionSpec as P

SPAN = 128
LANES = 128
SPANS = 4
SPAN_PART = 16
SLICE_HEADS = (0, 0, 1, 1, 2, 2, 3, 4)
SP = ("sp_0", "sp_1", "sp_2")
SP_TP = ("sp_0", "sp_1", "sp_2", "tp")
EPS = 1e-06
WIDE_SCALE = 128 ** (-0.5)
NARROW_SCALE = 64 ** (-0.5)
F32 = jnp.float32
BF16 = jnp.bfloat16


def position_tables(devices):
    lane = np.arange(LANES)
    inside, upper, lower = [], [], []
    for head_dim in (128, 64):
        half = head_dim // 2
        rate = 10000.0 ** (-2.0 * (lane % half) / head_dim)
        sign = np.where(lane % head_dim < half, -1.0, 1.0)
        for table, positions in (
            (inside, np.arange(SPAN)),
            (upper, np.arange(devices * SPANS // SPAN_PART) * SPAN_PART * SPAN),
            (lower, np.arange(SPAN_PART) * SPAN),
        ):
            angles = positions[:, None] * rate
            table += [np.cos(angles), np.sin(angles) * sign]
    return [np.stack(t).astype(np.float32) for t in (inside, upper, lower)]


def turned_by(first, second):
    return (
        first[0] * second[0] - first[1] * second[1],
        first[1] * second[0] + first[0] * second[1],
    )


def span_tables(table_refs, block, group):
    inside_ref, upper_ref, lower_ref = table_refs
    start = turned_by(
        *(
            [ref[2 * group + k, pl.ds(at, 1), :] for k in range(2)]
            for ref, at in ((upper_ref, block // SPAN_PART), (lower_ref, block % SPAN_PART))
        )
    )
    return turned_by((inside_ref[2 * group], inside_ref[2 * group + 1]), start)


def rotated_wide(x, tables):
    x = x.astype(F32)
    return x * tables[0] + pltpu.roll(x, 64, 1) * tables[1]


def rotated_narrow(x, tables):
    x = x.astype(F32)
    lane = lax.broadcasted_iota(jnp.int32, x.shape, 1)
    partner = jnp.where((lane & 32) == 0, pltpu.roll(x, 96, 1), pltpu.roll(x, 32, 1))
    return x * tables[0] + partner * tables[1]


def running_decay(wide_decay_ref, narrow_decay_ref, rows_ref):
    rows_ref[...] = jnp.zeros_like(rows_ref)
    rows_ref[0:3, :] = wide_decay_ref[...]
    rows_ref[3:5, :] = narrow_decay_ref[...]
    x = rows_ref[...]
    lane = lax.broadcasted_iota(jnp.int32, x.shape, 1)
    step = 1
    while step < SPAN:
        x = x + jnp.where(lane >= step, pltpu.roll(x, step, 1), 0.0)
        step *= 2
    return x


def low_rows(shape):
    return lax.broadcasted_iota(jnp.int32, shape, 0) < 64


def low_lanes(shape):
    return lax.broadcasted_iota(jnp.int32, shape, 1) < 64


def mm(a, b):
    return jnp.dot(a, b, preferred_element_type=F32)


def mm_nt(a, b):
    return lax.dot_general(a, b, (((1,), (1,)), ((), ())), preferred_element_type=F32)


def mm_tn(a, b):
    return lax.dot_general(a, b, (((0,), (0,)), ((), ())), preferred_element_type=F32)


def in_two(values):
    high = values.astype(BF16).astype(F32)
    return high, values - high


def log_rows(high, low):
    sub = lax.broadcasted_iota(jnp.int32, (8, LANES), 0)
    return jnp.where(sub == 0, high, jnp.where(sub == 1, low, 0.0)).astype(BF16)


def turned_span(place, turn):
    return (turn + jnp.where(place == 0, 2, jnp.where(place == 3, 1, jnp.where(place == 2, 3, 0)))) & 3


def states_kernel(
    index_ref, _, wk_ref, wv_ref, nk_ref, nv_ref, wd_ref, nd_ref, *refs, staged,
):
    table_refs, refs = refs[:3], refs[3:]
    sources, refs = refs[:staged], refs[staged:]
    before_ref, earlier_ref, message_ref = refs[:3]
    targets, refs = refs[3 : 3 + staged], refs[3 + staged :]
    rows_ref, state_ref, decay_ref, sems = refs
    span = pl.program_id(0)
    place = index_ref[0] * SPANS + span
    copies = [pltpu.make_async_copy(a, b, sems.at[k]) for k, (a, b) in enumerate(zip(sources, targets))]

    @pl.when(span == 0)
    def _():
        for copy in copies:
            copy.start()
        state_ref[...] = jnp.zeros_like(state_ref)
        decay_ref[...] = jnp.zeros_like(decay_ref)

    total = running_decay(wd_ref, nd_ref, rows_ref)
    last = total[:, SPAN - 1 : SPAN]
    tail = jnp.exp(last - total).T
    kept = jnp.exp(last)
    before_ref[0] = state_ref[...]
    earlier_ref[0] = decay_ref[...]
    tables = span_tables(table_refs, place, 0)
    for head in range(3):
        cut = slice(head * 128, head * 128 + 128)
        keys = rotated_wide(wk_ref[:, cut], tables) * WIDE_SCALE
        scaled = (keys * tail[:, head : head + 1]).astype(BF16)
        state_ref[cut, :] = state_ref[cut, :] * kept[head : head + 1, :] + mm_tn(scaled, wv_ref[:, cut])
    tables = span_tables(table_refs, place, 1)
    keys = rotated_narrow(nk_ref[...], tables) * NARROW_SCALE
    tails = jnp.where(low_lanes((SPAN, LANES)), tail[:, 3:4], tail[:, 4:5])
    own = mm_tn((keys * tails).astype(BF16), nv_ref[...])
    square = (LANES, LANES)
    own = jnp.where(low_rows(square) == low_lanes(square), own, 0.0)
    keeps = jnp.where(low_rows(square), kept[3:4, :], kept[4:5, :])
    state_ref[384:512, :] = state_ref[384:512, :] * keeps + own
    decay_ref[...] += jnp.broadcast_to(last, decay_ref.shape)

    @pl.when(span == SPANS - 1)
    def _():
        sums = decay_ref[...]
        high, low = in_two(sums)
        for part, head in enumerate(SLICE_HEADS):
            message_ref[part, 0:64] = state_ref[part * 64 : part * 64 + 64, :].astype(BF16)
            message_ref[part, 64:72] = log_rows(high[head : head + 1, :], low[head : head + 1, :])
        for copy in copies:
            copy.wait()


def plane_kernel(message_ref, out_ref, within_ref, logs_ref):
    carried = jnp.zeros((64, LANES), F32)
    logs = jnp.zeros((1, LANES), F32)
    for k in range(8):
        within_ref[k] = carried
        logs_ref[k] = jnp.broadcast_to(logs, (8, LANES))
        piece = message_ref[k].astype(F32)
        log = piece[64:65, :] + piece[65:66, :]
        carried = carried * jnp.exp(log) + piece[0:64, :]
        logs = logs + log
    ends = log_rows(*in_two(logs))
    for k in range(8):
        out_ref[k, 0:64] = carried.astype(BF16)
        out_ref[k, 64:72] = ends


def prefix_kernel(index_ref, planes_ref, within_ref, logs_ref, out_ref):
    plane = index_ref[0] // 8
    carried = jnp.zeros((64, LANES), F32)
    for k in range(7):
        piece = planes_ref[k].astype(F32)
        log = piece[64:65, :] + piece[65:66, :]
        carried = jnp.where(k < plane, carried * jnp.exp(log) + piece[0:64, :], carried)
    for k in range(8):
        out_ref[k] = (carried * jnp.exp(logs_ref[k, 0:1, :]) + within_ref[k]).astype(BF16)


def gated(output, gate, scale):
    gate = gate.astype(F32)
    return (output * scale * (gate / (1.0 + jnp.exp(-gate)))).astype(BF16)


def finish_kernel(
    index_ref, turn_ref, wq_ref, wk_ref, wv_ref, wg_ref, nq_ref, nk_ref, nv_ref, ng_ref, wd_ref, nd_ref,
    inside_ref, upper_ref, lower_ref, before_ref, earlier_ref, prefix_ref, wide_out_ref, narrow_out_ref,
    *out_refs, first,
):
    *out_refs, rows_ref, mixed_ref = out_refs
    span = turned_span(first + pl.program_id(0), turn_ref[0])
    place = index_ref[0] * SPANS + span
    table_refs = (inside_ref, upper_ref, lower_ref)
    total = running_decay(wd_ref, nd_ref, rows_ref)
    columns = total.T
    grown = jnp.exp(columns)
    earlier = jnp.exp(earlier_ref[0])
    square = (SPAN, SPAN)
    causal = lax.broadcasted_iota(jnp.int32, square, 0) >= lax.broadcasted_iota(jnp.int32, square, 1)

    def weights(scores, head):
        gaps = columns[:, head : head + 1] - total[head : head + 1, :]
        return (scores * jnp.exp(jnp.where(causal, gaps, -jnp.inf))).astype(BF16)

    tables = span_tables(table_refs, place, 0)
    for head in range(3):
        cut = slice(head * 128, head * 128 + 128)
        queries = rotated_wide(wq_ref[:, cut], tables).astype(BF16)
        keys = (rotated_wide(wk_ref[:, cut], tables) * WIDE_SCALE).astype(BF16)
        within = mm(weights(mm_nt(queries, keys), head), wv_ref[:, cut])
        entering = (
            prefix_ref[cut, :].astype(F32) * earlier[head : head + 1, :] + before_ref[0, cut, :]
        ).astype(BF16)
        output = within + mm(queries, entering) * grown[:, head : head + 1]
        scale = lax.rsqrt(jnp.mean(output * output, axis=-1, keepdims=True) + EPS)
        mixed_ref[:, cut] = gated(output, wg_ref[:, cut], scale)

    tables = span_tables(table_refs, place, 1)
    queries = rotated_narrow(nq_ref[...], tables).astype(BF16)
    keys = (rotated_narrow(nk_ref[...], tables) * NARROW_SCALE).astype(BF16)
    values = nv_ref[...]
    low = low_lanes(square)
    none = jnp.zeros_like(queries)
    within = jnp.where(
        low,
        mm(weights(mm_nt(jnp.where(low, queries, none), keys), 3), values),
        mm(weights(mm_nt(jnp.where(low, none, queries), keys), 4), values),
    )
    fades = jnp.where(low_rows(square), earlier[3:4, :], earlier[4:5, :])
    entering = (prefix_ref[384:512, :].astype(F32) * fades + before_ref[0, 384:512, :]).astype(BF16)
    output = within + mm(queries, entering) * jnp.where(low, grown[:, 3:4], grown[:, 4:5])
    squares = output * output
    left = jnp.sum(jnp.where(low, squares, 0.0), axis=-1, keepdims=True)
    right = jnp.sum(jnp.where(low, 0.0, squares), axis=-1, keepdims=True)
    scale = lax.rsqrt(jnp.where(low, left, right) * (1.0 / 64.0) + EPS)
    mixed_ref[:, 384:512] = gated(output, ng_ref[...], scale)

    projected = (
        mm(mixed_ref[:, 0:384], wide_out_ref[...]) + mm(mixed_ref[:, 384:512], narrow_out_ref[...])
    ).astype(BF16)
    if len(out_refs) == 2:
        half = SPAN // 2
        out_refs[0][...] = projected[:half]
        out_refs[1][...] = projected[half:]
    else:
        out_refs[0][0] = projected


def join_kernel(minus_ref, plus_ref, from_below_ref, from_above_ref, minus_out_ref, plus_out_ref):
    part = pl.program_id(0)

    @pl.when(part == 0)
    def _():
        minus_out_ref[...] = minus_ref[...]
        plus_out_ref[...] = (plus_ref[...].astype(F32) + from_below_ref[...].astype(F32)).astype(BF16)

    @pl.when(part == 1)
    def _():
        minus_out_ref[...] = (minus_ref[...].astype(F32) + from_above_ref[...].astype(F32)).astype(BF16)
        plus_out_ref[...] = plus_ref[...]


def rms(values, gain):
    return values * lax.rsqrt(jnp.mean(values * values, axis=-1, keepdims=True) + EPS) * gain


def norms_kernel(
    own_ref, below_ref, above_ref, residual_ref, mix_ref, pre_ref, updated_ref, low_ref, high_ref
):
    projected = own_ref[...].astype(F32) + below_ref[...].astype(F32) + above_ref[...].astype(F32)
    updated = (residual_ref[...].astype(F32) + rms(projected, mix_ref[...])).astype(BF16)
    updated_ref[...] = updated
    normed = rms(updated.astype(F32), pre_ref[...]).astype(BF16)

    @pl.when(pl.program_id(0) == 0)
    def _():
        low_ref[...] = normed

    @pl.when(pl.program_id(0) == 1)
    def _():
        high_ref[...] = normed


def tail_join_kernel(plus_ref, minus_ref, from_below_ref, from_above_ref, plus_out_ref, minus_out_ref):
    plus_out_ref[...] = (plus_ref[...].astype(F32) + from_below_ref[...].astype(F32)).astype(BF16)
    minus_out_ref[...] = (minus_ref[...].astype(F32) + from_above_ref[...].astype(F32)).astype(BF16)


def result_kernel(
    own_ref, below_low_ref, below_high_ref, above_low_ref, above_high_ref,
    updated_ref, gain_ref, out_ref,
):
    half = below_low_ref.shape[0]
    lowered = [
        own_ref[part].astype(F32) + below[...].astype(F32) + above[...].astype(F32)
        for part, below, above in (
            (slice(0, half), below_low_ref, above_low_ref),
            (slice(half, 2 * half), below_high_ref, above_high_ref),
        )
    ]
    lowered = jnp.concatenate(lowered, axis=0).T
    out_ref[...] = (updated_ref[...].astype(F32) + rms(lowered, gain_ref[...])).astype(BF16)


def up_block(x_ref, up_ref, at, block):
    weight = up_ref[:, :, pl.ds(at, block)].reshape(-1, block)
    rectified = jnp.maximum(mm(x_ref[...], weight), 0.0)
    return (rectified * rectified).astype(BF16).T


def down_block(down_ref, hidden_ref, k, group):
    weight = down_ref[pl.ds(k * group, group)].reshape(-1, hidden_ref.shape[0])
    return mm(weight, hidden_ref[...]).astype(BF16)


def far_mixer_kernel(*refs, ups, downs):
    halves, refs = refs[:2], refs[2:]
    both_ref, up_ref, down_ref, low_ref, high_ref, x_ref, hidden_ref, sems = refs
    devices, share, units = up_ref.shape
    half = halves[0].shape[0]
    block = units // ups
    group = devices // downs
    lines = group * share

    def up_copy(k):
        at = pl.multiple_of(k * block, block)
        return pltpu.make_async_copy(
            both_ref.at[:, 0, :, pl.ds(at, block)], up_ref.at[:, :, pl.ds(at, block)], sems.at[k]
        )

    def down_copy(k):
        at = k * group
        return pltpu.make_async_copy(
            both_ref.at[pl.ds(at, group), 1], down_ref.at[pl.ds(at, group)], sems.at[ups + k]
        )

    for k in range(ups):
        up_copy(k).start()
    for k in range(downs):
        down_copy(k).start()
    for k, ref in enumerate(halves):
        x_ref[k * half : (k + 1) * half] = ref[...]

    @pl.loop(0, ups)
    def _(k):
        up_copy(k).wait()
        at = pl.multiple_of(k * block, block)
        hidden_ref[pl.ds(at, block), :] = up_block(x_ref, up_ref, at, block)

    def lower(k, far_ref, base):
        down_copy(k).wait()
        lowered = down_block(down_ref, hidden_ref, k, group)
        far_ref[pl.ds(pl.multiple_of((k - base) * lines, lines), lines), :] = lowered

    @pl.loop(0, downs // 2)
    def _(k):
        lower(k, low_ref, 0)

    @pl.loop(downs // 2, downs)
    def _(k):
        lower(k, high_ref, downs // 2)


def near_mixer_kernel(*refs, ups, downs):
    halves, refs = refs[:4], refs[4:]
    up_ref, down_ref, minus_low_ref, minus_high_ref, plus_low_ref, plus_high_ref, x_ref, hidden_ref = refs
    devices, share, units = up_ref.shape
    half = halves[0].shape[0]
    rows = 2 * half
    block = units // ups
    group = devices // downs
    lines = group * share
    for k, ref in enumerate(halves):
        x_ref[k * half : (k + 1) * half] = ref[...]

    @pl.loop(0, ups)
    def _(k):
        at = pl.multiple_of(k * block, block)
        hidden_ref[pl.ds(at, block), :] = up_block(x_ref, up_ref, at, block)

    for first, minus_ref, plus_ref in (
        (0, minus_low_ref, plus_low_ref), (downs // 2, minus_high_ref, plus_high_ref)
    ):
        for k in range(downs // 2):
            lowered = down_block(down_ref, hidden_ref, first + k, group)
            at = slice(k * lines, (k + 1) * lines)
            minus_ref[at, :] = lowered[:, :rows]
            plus_ref[at, :] = lowered[:, rows:]


def own_mixer_kernel(first_ref, second_ref, up_ref, down_ref, out_ref, x_ref, hidden_ref, *, parts):
    devices, share, units = up_ref.shape
    half = first_ref.shape[0]
    x_ref[:half] = first_ref[...]
    x_ref[half:] = second_ref[...]
    hidden_ref[...] = up_block(x_ref, up_ref, 0, units)
    group = devices // parts
    lines = group * share
    for k in range(parts):
        out_ref[k * lines : (k + 1) * lines, :] = down_block(down_ref, hidden_ref, k, group)


SMALL = pltpu.CompilerParams(vmem_limit_bytes=16 * 1024 * 1024)


def shifted(array, axis, by):
    size = lax.axis_size(axis)
    return lax.ppermute(array, axis, [(k, (k + by) % size) for k in range(size)])


def joined(minus, plus, from_below, from_above, picks=(None, None)):
    half, width = from_below.shape
    flat = pl.BlockSpec((half, width), lambda i: (i, 0))
    kept = pl.BlockSpec((half, width), lambda i: (0, 0))
    out = jax.ShapeDtypeStruct((2 * half, width), BF16)

    def source(pick):
        if pick is None:
            return flat
        return pl.BlockSpec((None, half, width), lambda i: (pick, i, 0))

    return pl.pallas_call(
        join_kernel,
        out_shape=(out, out),
        grid=(2,),
        in_specs=[source(picks[0]), source(picks[1]), kept, kept],
        out_specs=[flat, flat],
        compiler_params=SMALL,
        name="join",
        cost_estimate=pl.CostEstimate(flops=1_000_000, bytes_accessed=3_500_000, transcendentals=0),
    )(minus, plus, from_below, from_above)


def local(
    wide_query, wide_key, wide_value, wide_gate,
    narrow_query, narrow_key, narrow_value, narrow_gate,
    wide_decay, narrow_decay, residual, wide_out, narrow_out,
    up_weight, down_weight, gain_mix, gain_pre, gain_mlp,
):
    devices = lax.axis_size(SP)
    ranks = lax.axis_size("tp")
    length, width = wide_query.shape[0], residual.shape[1]
    rows = residual.shape[0]
    share = up_weight.shape[0]
    units = up_weight.shape[1]

    both = lax.all_gather(
        jnp.concatenate([up_weight, down_weight.T], axis=0), SP, axis=0, tiled=True
    ).reshape(devices, 2, share, units)

    tables = [jnp.asarray(t) for t in position_tables(devices)]
    scalars = [
        lax.axis_index(SP).astype(jnp.int32).reshape(1),
        lax.axis_index("tp").astype(jnp.int32).reshape(1),
    ]
    table_blocks = [pl.BlockSpec(t.shape, lambda s, i, t: (0, 0, 0)) for t in tables]

    def span_blocks(at):
        return (
            pl.BlockSpec((SPAN, 384), lambda s, i, t: (at(s, i, t), 0)),
            pl.BlockSpec((SPAN, 128), lambda s, i, t: (at(s, i, t), 0)),
            [
                pl.BlockSpec((3, SPAN), lambda s, i, t: (0, at(s, i, t))),
                pl.BlockSpec((2, SPAN), lambda s, i, t: (0, at(s, i, t))),
            ],
            [
                pl.BlockSpec((1, 512, LANES), lambda s, i, t: (at(s, i, t), 0, 0)),
                pl.BlockSpec((1, 8, LANES), lambda s, i, t: (at(s, i, t), 0, 0)),
            ],
        )

    wide_block, narrow_block, decay_blocks, state_blocks = span_blocks(lambda s, i, t: s)
    staged = (
        *tables, wide_decay, narrow_decay, wide_query, wide_key, wide_value, wide_gate,
        narrow_query, narrow_key, narrow_value, narrow_gate, wide_out, narrow_out,
    )
    before, earlier, message, *held = pl.pallas_call(
        functools.partial(states_kernel, staged=len(staged)),
        out_shape=(
            jax.ShapeDtypeStruct((SPANS, 512, LANES), F32),
            jax.ShapeDtypeStruct((SPANS, 8, LANES), F32),
            jax.ShapeDtypeStruct((8, 72, LANES), BF16),
            *(pltpu.VMEM(x.shape, x.dtype) for x in staged),
        ),
        grid_spec=pltpu.PrefetchScalarGridSpec(
            num_scalar_prefetch=2,
            grid=(SPANS,),
            in_specs=[
                wide_block, wide_block, narrow_block, narrow_block, *decay_blocks, *table_blocks,
                *([pl.BlockSpec(memory_space=pltpu.HBM)] * len(staged)),
            ],
            out_specs=[
                *state_blocks,
                pl.BlockSpec((8, 72, LANES), lambda s, i, t: (0, 0, 0)),
                *([pl.BlockSpec(memory_space=pltpu.VMEM)] * len(staged)),
            ],
            scratch_shapes=[
                pltpu.VMEM((8, LANES), F32),
                pltpu.VMEM((512, LANES), F32),
                pltpu.VMEM((8, LANES), F32),
                pltpu.SemaphoreType.DMA((len(staged),)),
            ],
        ),
        compiler_params=SMALL,
        name="states",
        cost_estimate=pl.CostEstimate(flops=60_000_000, bytes_accessed=2_500_000, transcendentals=20_000),
    )(
        *scalars,
        *(
            pltpu.with_memory_space_constraint(x, pltpu.HBM)
            for x in (
                wide_key, wide_value, narrow_key, narrow_value,
                wide_decay, narrow_decay, *tables, *staged,
            )
        ),
    )

    arrived = lax.all_to_all(message, SP[1:], 0, 0, tiled=True)
    planes, within, logs = pl.pallas_call(
        plane_kernel,
        out_shape=(
            jax.ShapeDtypeStruct((8, 72, LANES), BF16),
            jax.ShapeDtypeStruct((8, 64, LANES), F32),
            jax.ShapeDtypeStruct((8, 8, LANES), F32),
        ),
        compiler_params=SMALL,
        name="plane",
        cost_estimate=pl.CostEstimate(flops=300_000, bytes_accessed=600_000, transcendentals=8_000),
    )(arrived)
    planes = lax.all_to_all(planes, SP[0], 0, 0, tiled=True)
    whole = pl.BlockSpec(memory_space=pltpu.VMEM)
    prefixes = pl.pallas_call(
        prefix_kernel,
        out_shape=jax.ShapeDtypeStruct((8, 64, LANES), BF16),
        in_specs=[pl.BlockSpec(memory_space=pltpu.SMEM), whole, whole, whole],
        out_specs=whole,
        compiler_params=SMALL,
        name="prefix",
        cost_estimate=pl.CostEstimate(flops=300_000, bytes_accessed=600_000, transcendentals=8_000),
    )(scalars[0], planes, within, logs)
    prefix = lax.all_to_all(prefixes, SP[1:], 0, 0, tiled=True).reshape(512, LANES)

    def finish(first, count, out_shape, out_specs):
        wide, narrow, decays, states = span_blocks(lambda s, i, t: turned_span(first + s, t[0]))
        return pl.pallas_call(
            functools.partial(finish_kernel, first=first),
            out_shape=out_shape,
            grid_spec=pltpu.PrefetchScalarGridSpec(
                num_scalar_prefetch=2,
                grid=(count,),
                in_specs=[
                    wide, wide, wide, wide, narrow, narrow, narrow, narrow,
                    *decays, *table_blocks, *states,
                    pl.BlockSpec((512, LANES), lambda s, i, t: (0, 0)),
                    pl.BlockSpec((384, width), lambda s, i, t: (0, 0)),
                    pl.BlockSpec((128, width), lambda s, i, t: (0, 0)),
                ],
                out_specs=out_specs,
                scratch_shapes=[pltpu.VMEM((8, LANES), F32), pltpu.VMEM((SPAN, 512), BF16)],
            ),
            compiler_params=SMALL,
            name="finish" if first else "finish_far",
            cost_estimate=pl.CostEstimate(
                flops=350_000_000 * count,
                bytes_accessed=3_000_000 + 1_500_000 * count,
                transcendentals=150_000 * count,
            ),
        )(
            *scalars, *held[5:13], *held[3:5], *held[:3], before, earlier, prefix, *held[13:],
        )

    half = rows // 2
    half_out = jax.ShapeDtypeStruct((half, width), BF16)
    near_out = jax.ShapeDtypeStruct((3, rows, width), BF16)
    low, high = finish(
        0, 1, (half_out, half_out), [pl.BlockSpec((half, width), lambda s, i, t: (0, 0))] * 2
    )
    low, high = shifted(low, "tp", 1), shifted(high, "tp", -1)
    (near,) = finish(
        1, 3, (near_out,), [pl.BlockSpec((1, rows, width), lambda s, i, t: (s, 0, 0))]
    )
    minus, plus = joined(near, near, low, high, (1, 2))
    below, above = shifted(plus, "tp", 1), shifted(minus, "tp", -1)
    flat = pl.BlockSpec((half, width), lambda i: (i, 0))
    kept = pl.BlockSpec((half, width), lambda i: (0, 0))
    gain = pl.BlockSpec((1, width), lambda i: (0, 0))
    updated, low, high = pl.pallas_call(
        norms_kernel,
        out_shape=[jax.ShapeDtypeStruct((rows, width), BF16), half_out, half_out],
        grid=(2,),
        in_specs=[
            pl.BlockSpec((None, half, width), lambda i: (0, i, 0)), flat, flat, flat, gain, gain,
        ],
        out_specs=[flat, kept, kept],
        compiler_params=SMALL,
        name="norms",
        cost_estimate=pl.CostEstimate(flops=4_000_000, bytes_accessed=3_500_000, transcendentals=300),
    )(near, below, above, residual, gain_mix.reshape(1, width), gain_pre.reshape(1, width))
    below_low, above_high = shifted(low, "tp", 1), shifted(high, "tp", -1)
    below_high, above_low = shifted(high, "tp", 1), shifted(low, "tp", -1)
    far_low, far_high = shifted(below_low, "tp", 1), shifted(above_high, "tp", -1)

    ups, downs = 4, 4
    turned = pltpu.VMEM((width, rows), BF16)
    turned_half = pltpu.VMEM((width // 2, rows), BF16)
    weights = pltpu.VMEM((devices, share, units), BF16)
    scratch = [pltpu.VMEM((2 * rows, width), BF16), pltpu.VMEM((units, 2 * rows), BF16)]
    scratch_half = [pltpu.VMEM((rows, width), BF16), pltpu.VMEM((units, rows), BF16)]
    own_low, own_high = low, high
    up, down, low, high = pl.pallas_call(
        functools.partial(far_mixer_kernel, ups=ups, downs=downs),
        out_shape=(weights, weights, turned_half, turned_half),
        in_specs=[*([whole] * 2), pl.BlockSpec(memory_space=pltpu.HBM)],
        out_specs=[whole] * 4,
        scratch_shapes=[*scratch_half, pltpu.SemaphoreType.DMA((ups + downs,))],
        compiler_params=SMALL,
        name="mixer_far",
        cost_estimate=pl.CostEstimate(
            flops=4 * rows * width * units, bytes_accessed=20_000_000, transcendentals=0
        ),
    )(far_low, far_high, pltpu.with_memory_space_constraint(both, pltpu.HBM))
    low, high = shifted(low, "tp", 1), shifted(high, "tp", -1)
    minus_low, minus_high, plus_low, plus_high = pl.pallas_call(
        functools.partial(near_mixer_kernel, ups=1, downs=2),
        out_shape=(turned_half,) * 4,
        in_specs=[whole] * 6,
        out_specs=[whole] * 4,
        scratch_shapes=scratch,
        compiler_params=SMALL,
        name="mixer_near",
        cost_estimate=pl.CostEstimate(
            flops=8 * rows * width * units, bytes_accessed=2_000_000, transcendentals=0
        ),
    )(below_low, below_high, above_low, above_high, up, down)
    below_high, above_low = shifted(plus_high, "tp", 1), shifted(minus_low, "tp", -1)
    plus_low, minus_high = pl.pallas_call(
        tail_join_kernel,
        out_shape=(turned_half,) * 2,
        in_specs=[whole] * 4,
        out_specs=[whole] * 2,
        compiler_params=SMALL,
        name="tail_join",
        cost_estimate=pl.CostEstimate(flops=500_000, bytes_accessed=1_500_000, transcendentals=0),
    )(plus_low, minus_high, low, high)
    below_low, above_high = shifted(plus_low, "tp", 1), shifted(minus_high, "tp", -1)
    own_low, _ = lax.optimization_barrier((own_low, plus_low))
    own = pl.pallas_call(
        functools.partial(own_mixer_kernel, parts=2),
        out_shape=turned,
        in_specs=[whole] * 4,
        out_specs=whole,
        scratch_shapes=scratch_half,
        compiler_params=SMALL,
        name="mixer_own",
        cost_estimate=pl.CostEstimate(
            flops=4 * rows * width * units, bytes_accessed=2_000_000, transcendentals=0
        ),
    )(own_low, own_high, up, down)
    return pl.pallas_call(
        result_kernel,
        out_shape=jax.ShapeDtypeStruct((rows, width), BF16),
        compiler_params=SMALL,
        name="result",
        cost_estimate=pl.CostEstimate(flops=4_000_000, bytes_accessed=3_500_000, transcendentals=300),
    )(
        own, below_low, below_high, above_low, above_high, updated, gain_mlp.reshape(1, width)
    )


def solution(mesh):
    finer = Mesh(mesh.devices.reshape(8, 4, 2, mesh.shape["tp"]), ("sp_0", "sp_1", "sp_2", "tp"))
    in_specs = (
        *([P(SP, "tp")] * 8),
        P("tp", SP),
        P("tp", SP),
        P(SP_TP, None),
        P("tp", None),
        P("tp", None),
        P(SP, "tp"),
        P("tp", SP),
        P(),
        P(),
        P(),
    )
    return jax.shard_map(
        local, mesh=finer, in_specs=in_specs, out_specs=P(SP_TP, None), check_vma=False
    )
```
